256 devices in a mesh: sp: 64 (over z, x, core), tp: 4 (over y).
Axes of the slice: x: 4, y: 4, z: 8, core: 2. Of those that a mesh axis runs over, the one named last changes fastest.
Arguments:
- tokens: bfloat16 [16384, 2048], P(('sp', 'tp')), may hold values from -6 to 6
- input_gain: float32 [2048], replicated, may hold values from 0.1 to 1.9
- memory_query: bfloat16 [2048, 512], P(None, 'tp'), may hold values from -0.125 to 0.125
- memory_key: bfloat16 [2048, 512], P(None, 'tp'), may hold values from -0.125 to 0.125
- memory_value: bfloat16 [2048, 512], P(None, 'tp'), may hold values from -0.125 to 0.125
- memory_outgate: bfloat16 [2048, 512], P(None, 'tp'), may hold values from -0.125 to 0.125
- memory_gates: bfloat16 [2048, 4, 8], replicated, may hold values from -0.0625 to 0.0625
- gate_offset: float32 [4, 16384, 8], P(None, 'sp', 'tp'), may hold values from -1 to 150
- memory_norm_gain: float32 [512], replicated, may hold values from 0.1 to 1.9
- query_down: bfloat16 [2048, 384], replicated, may hold values from -0.125 to 0.125
- query_down_gain: float32 [384], replicated, may hold values from 0.1 to 1.9
- latent_down: bfloat16 [2048, 256], replicated, may hold values from -0.125 to 0.125
- latent_gain: float32 [256], replicated, may hold values from 0.1 to 1.9
- rotary_down: bfloat16 [2048, 32], replicated, may hold values from -0.125 to 0.125
- query_up: bfloat16 [384, 8, 96], replicated, may hold values from -0.3125 to 0.3125
- latent_up: bfloat16 [256, 8, 128], replicated, may hold values from -0.375 to 0.375
- query_gain: float32 [96], replicated, may hold values from 1.2 to 8
- key_gain: float32 [96], replicated, may hold values from 1.2 to 8
- memory_output: bfloat16 [512, 2048], replicated, may hold values from -0.25 to 0.25
- attention_output: bfloat16 [512, 2048], replicated, may hold values from -0.75 to 0.75
Outputs:
- mixed: bfloat16 [16384, 2048], P(('sp', 'tp'))
The draws below stay inside these ranges and needn't reach their ends.
All inputs are finite; a program needn't handle non-finite values.
Results may differ from the reference program's by a relative error of at most 0.019.
The reference program's roundings to bfloat16 on the way count: a program that leaves them out, or rounds other values in their place, can miss the bound.
Values may be sent and summed in bfloat16 or wider, within the bound.
A program may use at most 128 MiB of HBM per device.

```python
import jax
import jax.numpy as jnp
from jax import lax

D = 2048
MEMORY_HEADS = 8
ML_DH = 64
ML_BLOCK = 128
MLA_HEADS = 8
Q_RANK = 384
KV_RANK = 256
NOPE = 64
ROPE = 32
VDIM = 64
TOK_DEV = 256
SEQUENCE_TOKENS = 16384


def draw_gate_offset(key, part):
    key_sequence = jax.random.split(jax.random.fold_in(key, 17), 7)
    blocks = SEQUENCE_TOKENS // TOK_DEV
    inputs = jax.random.uniform(key_sequence[0], (2, SEQUENCE_TOKENS, MEMORY_HEADS), jnp.float32, -1.0, 1.0)
    slow_level = jnp.log(jnp.float32(SEQUENCE_TOKENS)) + 0.4 + jax.random.uniform(key_sequence[1], (2, blocks, MEMORY_HEADS), jnp.float32, -1.6, 1.6)
    fast_level = jnp.log(jnp.float32(ML_BLOCK / 4.0)) + jax.random.uniform(key_sequence[2], (2, blocks, MEMORY_HEADS), jnp.float32, 0.0, 0.7)
    fast_heads = jax.random.bernoulli(key_sequence[3], 0.5, (2, 1, MEMORY_HEADS))
    memory_levels = jnp.repeat(jnp.where(fast_heads, fast_level, slow_level), TOK_DEV, axis=1)
    token_places = jnp.arange(SEQUENCE_TOKENS, dtype=jnp.int32)
    outlier_positions = jax.random.randint(key_sequence[5], (2, 4, 1, MEMORY_HEADS), 0, SEQUENCE_TOKENS)
    outlier_tokens = jnp.any(token_places[None, None, :, None] == outlier_positions, axis=1)
    forget_gate = jnp.where(outlier_tokens, jax.random.uniform(key_sequence[6], (2, SEQUENCE_TOKENS, MEMORY_HEADS), jnp.float32, -0.5, 1.4), memory_levels)
    return jnp.stack([inputs[0], forget_gate[0], inputs[1], forget_gate[1]], axis=0)


def draw_query_gain(key, part):
    subkey = jax.random.fold_in(key, 29)
    return jax.random.uniform(subkey, (NOPE + ROPE,), jnp.float32, 1.2, 2.0)


def draw_key_gain(key, part):
    subkey = jax.random.fold_in(key, 31)
    return jax.random.uniform(subkey, (NOPE + ROPE,), jnp.float32, 1.2, 2.0)


def shard_levels(stream_key, extent, shards, low, high):
    factor_of, own = 1.0, jax.random.fold_in(stream_key, 6)
    for dim, parts in shards:
        draws = jnp.exp(jax.random.uniform(jax.random.fold_in(own, dim), (parts,), jnp.float32, low / len(shards), high / len(shards)))
        factor_of = factor_of * jnp.repeat(draws, extent[dim] // parts).reshape([-1 if axis == dim else 1 for axis in range(len(extent))])
    return factor_of


def centred(rng, extent, deviation, limit, cuts=(), kind=jnp.bfloat16):
    level = shard_levels(rng, extent, cuts, -0.22, 0.18) if cuts else 1.0
    values = jax.random.normal(rng, extent, jnp.float32) * deviation * level
    return jnp.minimum(jnp.maximum(values, -limit), limit).astype(kind)


def setup_inputs(seed: int = 0) -> dict:
    key_of = jax.random.split(jax.random.key(seed), 21)
    tokens = centred(key_of[0], (SEQUENCE_TOKENS, D), 1.0, 6.0, ((0, 256),))
    input_gain = jnp.clip(1.0 + 0.18 * jax.random.normal(key_of[1], (D,), jnp.float32), 0.1, 1.9)
    memory_query = centred(key_of[2], (D, MEMORY_HEADS * ML_DH), D ** -0.5, 0.125, ((1, 4),))
    memory_key = centred(key_of[3], (D, MEMORY_HEADS * ML_DH), D ** -0.5, 0.125, ((1, 4),))
    memory_value = centred(key_of[4], (D, MEMORY_HEADS * ML_DH), D ** -0.5, 0.125, ((1, 4),))
    memory_outgate = centred(key_of[5], (D, MEMORY_HEADS * ML_DH), D ** -0.5, 0.125, ((1, 4),))
    memory_gates = centred(key_of[6], (D, 4, MEMORY_HEADS), (4 * D) ** -0.5, 0.0625)
    gate_offset = draw_gate_offset(jax.random.fold_in(key_of[20], 71), 0)
    memory_norm_gain = jnp.clip(1.0 + 0.18 * jax.random.normal(key_of[8], (MEMORY_HEADS * ML_DH,), jnp.float32), 0.1, 1.9)
    query_down = centred(key_of[9], (D, Q_RANK), D ** -0.5, 0.125)
    query_down_gain = jnp.clip(1.0 + 0.18 * jax.random.normal(key_of[10], (Q_RANK,), jnp.float32), 0.1, 1.9)
    latent_down = centred(key_of[11], (D, KV_RANK), D ** -0.5, 0.125)
    latent_gain = jnp.clip(1.0 + 0.18 * jax.random.normal(key_of[12], (KV_RANK,), jnp.float32), 0.1, 1.9)
    rotary_down = centred(key_of[13], (D, ROPE), D ** -0.5, 0.125)
    query_up = centred(key_of[14], (Q_RANK, MLA_HEADS, NOPE + ROPE), Q_RANK ** -0.5, 0.3125)
    latent_up = centred(key_of[15], (KV_RANK, MLA_HEADS, NOPE + VDIM), KV_RANK ** -0.5, 0.375)
    query_gain = draw_query_gain(jax.random.fold_in(key_of[20], 71), 0)
    key_gain = draw_key_gain(jax.random.fold_in(key_of[20], 71), 0)
    memory_output = centred(key_of[18], (MEMORY_HEADS * ML_DH, D), (MEMORY_HEADS * ML_DH) ** -0.5, 0.25)
    attention_output = centred(key_of[19], (MLA_HEADS * VDIM, D), (MLA_HEADS * VDIM // 9) ** -0.5, 0.75)
    return {"tokens": tokens, "input_gain": input_gain, "memory_query": memory_query, "memory_key": memory_key, "memory_value": memory_value, "memory_outgate": memory_outgate, "memory_gates": memory_gates, "gate_offset": gate_offset, "memory_norm_gain": memory_norm_gain, "query_down": query_down, "query_down_gain": query_down_gain, "latent_down": latent_down, "latent_gain": latent_gain, "rotary_down": rotary_down, "query_up": query_up, "latent_up": latent_up, "query_gain": query_gain, "key_gain": key_gain, "memory_output": memory_output, "attention_output": attention_output}


EPSILON = 1e-06
ROPE_BASE = 10000.0
FLOOR_LOG = -1e+30

def rounded(vectors):
    return lax.optimization_barrier(vectors.astype(jnp.bfloat16))

def rms_scale(vectors, scaling):
    mean_square = lax.optimization_barrier(jnp.mean(vectors * vectors, axis=-1, keepdims=True))
    return vectors * lax.rsqrt(mean_square + EPSILON) * scaling

def rotate_half(vectors, positions):
    half_width = vectors.shape[-1] // 2
    frequency = ROPE_BASE ** (-jnp.arange(half_width, dtype=jnp.float32) / half_width)
    angles = positions.astype(jnp.float32)[:, None] * frequency[None, :]
    shaped = (positions.shape[0],) + (1,) * (vectors.ndim - 2) + (half_width,)
    cosine = jnp.cos(angles).reshape(shaped)
    sine_part = jnp.sin(angles).reshape(shaped)
    first_half = vectors[..., :half_width]
    second_half = vectors[..., half_width:]
    return jnp.concatenate([first_half * cosine - second_half * sine_part, first_half * sine_part + second_half * cosine], axis=-1)

def memory_pass(queries, key_rows, value_rows, in_gate, log_forget):
    head_count = queries.shape[1]
    head_width = queries.shape[2]
    blocks = queries.shape[0] // ML_BLOCK

    def split_blocks(tensor):
        return tensor.reshape((blocks, ML_BLOCK) + tensor.shape[1:])
    lower_mask = jnp.tril(jnp.ones((ML_BLOCK, ML_BLOCK), dtype=bool))

    def advance(state_carry, block_data):
        memory, normal, stabilizer = state_carry
        query_block, key_block, value_block, gate_block, forget_block = block_data
        query_float = query_block.astype(jnp.float32)
        key_float = key_block.astype(jnp.float32)
        value_float = value_block.astype(jnp.float32)
        cumulated = jnp.cumsum(forget_block, axis=0)
        decays = cumulated[:, None, :] - cumulated[None, :, :] + gate_block[None, :, :]
        decays = jnp.where(lower_mask[:, :, None], decays, -jnp.inf)
        carried_log = cumulated + stabilizer[None, :]
        topmost = jnp.maximum(carried_log, lax.optimization_barrier(jnp.max(decays, axis=1)))
        scores = jnp.einsum('thd,shd->tsh', query_float, key_float)
        weights = scores * jnp.exp(decays - topmost[:, None, :])
        numerator = jnp.einsum('tsh,shd->thd', rounded(weights).astype(jnp.float32), value_float)
        denominator = lax.optimization_barrier(jnp.sum(weights, axis=1))
        carried = jnp.exp(carried_log - topmost)
        numerator = numerator + carried[:, :, None] * jnp.einsum('hvk,thk->thv', memory, query_float, precision=lax.Precision.HIGHEST)
        denominator = denominator + carried * jnp.einsum('hk,thk->th', normal, query_float, precision=lax.Precision.HIGHEST)
        outputs = numerator / jnp.maximum(jnp.abs(denominator), jnp.exp(-topmost))[:, :, None]
        last_total = cumulated[-1]
        growth = last_total[None, :] - cumulated + gate_block
        next_level = jnp.maximum(last_total + stabilizer, lax.optimization_barrier(jnp.max(growth, axis=0)))
        inflow = jnp.exp(growth - next_level[None, :])
        shrink = jnp.exp(last_total + stabilizer - next_level)
        weighted = inflow[:, :, None] * value_float
        memory = shrink[:, None, None] * memory + jnp.einsum('shv,shk->hvk', weighted, key_float, precision=lax.Precision.HIGHEST)
        normal = shrink[:, None] * normal + jnp.einsum('sh,shk->hk', inflow, key_float, precision=lax.Precision.HIGHEST)
        return ((memory, normal, next_level), outputs)
    start_state = (jnp.zeros((head_count, head_width, head_width), jnp.float32), jnp.zeros((head_count, head_width), jnp.float32), jnp.full((head_count,), FLOOR_LOG, jnp.float32))
    block_inputs = (split_blocks(queries), split_blocks(key_rows), split_blocks(value_rows), split_blocks(in_gate), split_blocks(log_forget))
    final_state, outputs = lax.scan(advance, start_state, block_inputs)
    return outputs.reshape(queries.shape[0], head_count, head_width)

def reference(tokens, input_gain, memory_query, memory_key, memory_value, memory_outgate, memory_gates, gate_offset, memory_norm_gain, query_down, query_down_gain, latent_down, latent_gain, rotary_down, query_up, latent_up, query_gain, key_gain, memory_output, attention_output):
    token_count = tokens.shape[0]
    positions = jnp.arange(token_count, dtype=jnp.int32)
    normed = rounded(rms_scale(tokens.astype(jnp.float32), input_gain))

    def project(weight_matrix):
        return jnp.dot(normed, weight_matrix, preferred_element_type=jnp.float32)
    mem_shape = (token_count, MEMORY_HEADS, ML_DH)
    queries_mem = rounded(project(memory_query)).reshape(mem_shape)
    keys_mem = rounded(project(memory_key) * ML_DH ** (-0.5)).reshape(mem_shape)
    values_mem = rounded(project(memory_value)).reshape(mem_shape)
    outgate = rounded(project(memory_outgate)).astype(jnp.float32)
    gate_data = rounded(project(memory_gates.reshape(memory_gates.shape[0], 4 * MEMORY_HEADS)))
    gate_pre = gate_data.astype(jnp.float32).reshape(token_count, 4, MEMORY_HEADS) + jnp.transpose(gate_offset, (1, 0, 2))
    forward_out = memory_pass(queries_mem, keys_mem, values_mem, gate_pre[:, 0], jax.nn.log_sigmoid(gate_pre[:, 1]))
    backward_out = jnp.flip(memory_pass(jnp.flip(queries_mem, 0), jnp.flip(keys_mem, 0), jnp.flip(values_mem, 0), jnp.flip(gate_pre[:, 2], 0), jnp.flip(jax.nn.log_sigmoid(gate_pre[:, 3]), 0)), 0)
    combined = rms_scale(forward_out + backward_out, memory_norm_gain.reshape(MEMORY_HEADS, ML_DH))
    memory_rows = (combined.reshape(token_count, MEMORY_HEADS * ML_DH) * jax.nn.sigmoid(outgate)).astype(jnp.bfloat16)
    query_latent = rounded(rms_scale(project(query_down), query_down_gain))
    query_full = jnp.dot(query_latent, query_up.reshape(query_up.shape[0], -1), preferred_element_type=jnp.float32).reshape(token_count, MLA_HEADS, NOPE + ROPE)
    query_plain = rms_scale(query_full[..., :NOPE], query_gain[:NOPE])
    query_turned = rotate_half(rms_scale(query_full[..., NOPE:], query_gain[NOPE:]), positions)
    queries_att = rounded(jnp.concatenate([query_plain, query_turned], axis=-1) * (NOPE + ROPE) ** (-0.5))
    latent = rounded(rms_scale(project(latent_down), latent_gain))
    rotary = rounded(rotate_half(rms_scale(project(rotary_down), key_gain[NOPE:]), positions))
    expanded = jnp.dot(latent, latent_up.reshape(latent_up.shape[0], -1), preferred_element_type=jnp.float32).reshape(token_count, MLA_HEADS, NOPE + VDIM)
    key_plain = rounded(rms_scale(expanded[..., :NOPE], key_gain[:NOPE]))
    value_att = rounded(expanded[..., NOPE:]).astype(jnp.float32)
    key_full = jnp.concatenate([key_plain.astype(jnp.float32), jnp.broadcast_to(rotary.astype(jnp.float32)[:, None, :], (token_count, MLA_HEADS, ROPE))], axis=-1)

    def attend(query_block):
        scores = jnp.einsum('thd,shd->hts', query_block.astype(jnp.float32), key_full)
        topmost = lax.optimization_barrier(jnp.max(scores, axis=-1, keepdims=True))
        lifted = jnp.exp(scores - topmost)
        totals = lax.optimization_barrier(jnp.sum(lifted, axis=-1))
        probabilities = rounded(lifted).astype(jnp.float32)
        mixture = jnp.einsum('hts,shd->thd', probabilities, value_att) / jnp.transpose(totals)[:, :, None]
        return mixture.astype(jnp.bfloat16)
    block_rows = TOK_DEV
    attended = lax.map(attend, queries_att.reshape(token_count // block_rows, block_rows, MLA_HEADS, NOPE + ROPE))
    attention_rows = attended.reshape(token_count, MLA_HEADS * VDIM)
    mixed = jnp.dot(memory_rows, memory_output, preferred_element_type=jnp.float32) + jnp.dot(attention_rows, attention_output, preferred_element_type=jnp.float32)
    return mixed.astype(jnp.bfloat16)
```

```python
import functools

import jax
import jax.numpy as jnp
from jax import lax
from jax.experimental import pallas as pl
from jax.experimental.pallas import tpu as pltpu
from jax.sharding import Mesh
from jax.sharding import PartitionSpec as P

D = 2048
NOPE = 64
ROPE = 32
ROWS = 64
BLOCK = 256
QR = 384
KVR = 256
SP = ("sp_0", "sp_1", "sp_2")
SP_TP = ("sp_0", "sp_1", "sp_2", "tp")
EPSILON = 1e-06
ROPE_BASE = 10000.0
FLOOR_LOG = -1e30
BF = jnp.bfloat16
F32 = jnp.float32
MESH = pl.DeviceIdType.MESH
HI = lax.Precision.HIGHEST
KCHUNK = 1024


def dot(a, b, precision=None):
    return lax.dot_general(a, b, (((1,), (0,)), ((), ())), precision=precision, preferred_element_type=F32)


def dot_nt(a, b, precision=None):
    return lax.dot_general(a, b, (((1,), (1,)), ((), ())), precision=precision, preferred_element_type=F32)


def lanes(shape):
    return lax.broadcasted_iota(jnp.int32, shape, len(shape) - 1)


def rcopy(src, dst, send_sem, recv_sem, device):
    return pltpu.make_async_remote_copy(
        src_ref=src, dst_ref=dst, send_sem=send_sem, recv_sem=recv_sem, device_id=device, device_id_type=MESH
    )


def rms(v):
    return v * lax.rsqrt(jnp.mean(v * v, axis=-1, keepdims=True) + EPSILON)


def kernel(
    nz, nx, ny,
    tok, gain, hmq, hmk, hmv, hmo, hgt, goff, mng, hqd, qdg, hld, lg, hrt, hqt, hlup,
    cq, sq, cr, sr, kg, hwm, hwa,
    out,
    mq, mk, mv, mo, gt, qd, ld, rt, qt, lup, wm, wa,
    rt4, wqt, normed, ksend, kgot, kvg, psend, qsend, qg, pa, rtot, pb,
    qop, kop, vop, osend, po, fsend, fx, lhs_m, lhs_a,
    w_sem, n_ss, n_rs, g_ss, g_rs, p_ss, p_rs, q_ss, q_rs, a_ss, a_rs, b_ss, b_rs,
    u_ss, u_rs, d_ss, d_rs, o_ss, o_rs, f_ss, f_rs,
):
    z = lax.axis_index("sp_0")
    x = lax.axis_index("sp_1")
    c = lax.axis_index("sp_2")
    y = lax.axis_index("tp")
    nr = nx * 2
    me = x * 2 + c

    def at_y(d):
        return {"tp": lax.rem(y + d, ny)}

    def at_row(d):
        j = lax.rem(me + d, nr)
        return {"sp_1": j // 2, "sp_2": lax.rem(j, 2)}

    def at_z(d):
        return {"sp_0": lax.rem(z + d, nz)}

    pairs = ((hqd, qd), (hld, ld), (hrt, rt), (hqt, qt), (hlup, lup), (hmq, mq), (hmk, mk), (hmv, mv),
             (hmo, mo), (hgt, gt), (hwm, wm), (hwa, wa))
    loads = [pltpu.make_async_copy(a, b, w_sem.at[i]) for i, (a, b) in enumerate(pairs)]
    for load in loads:
        load.start()

    barrier = pltpu.get_barrier_semaphore()
    peers = [at_y(d) for d in range(1, ny)] + [at_row(d) for d in range(1, nr)] + [at_z(d) for d in range(1, nz)]
    for peer in peers:
        pl.semaphore_signal(barrier, inc=1, device_id=peer, device_id_type=MESH)

    xt = tok[...].astype(F32)
    normed_local = (rms(xt) * gain[...]).astype(BF)
    normed[pl.ds(y, 1)] = normed_local[None]
    pl.semaphore_wait(barrier, len(peers))
    n_copies = [rcopy(normed.at[y], normed.at[y], n_ss.at[d], n_rs.at[d], at_y(d)) for d in range(1, ny)]
    for copy in n_copies:
        copy.start()

    loads[0].wait()
    loads[1].wait()
    ql = (rms(dot(normed_local, qd[...])) * qdg[...]).astype(BF)
    la = (rms(dot(normed_local, ld[...])) * lg[...]).astype(BF)
    loads[2].wait()
    for i in range(4):
        rt4[pl.ds(32 * i, 32), :] = rt[...]
        rt4[pl.ds(128 + 32 * i, 16), :] = rt[pl.ds(16, 16), :]
        rt4[pl.ds(128 + 32 * i + 16, 16), :] = rt[pl.ds(0, 16), :]
    ro = dot_nt(normed_local, rt4[...])
    ra, rb = ro[:, :128], ro[:, 128:]
    rscale = lax.rsqrt(jnp.mean(ra * ra, axis=-1, keepdims=True) + EPSILON)
    lane = lanes((ROWS, 128))
    rot = (ra * rscale) * cr[...] + (rb * rscale) * sr[...]
    rot = jnp.where(lane // ROPE == y, rot, 0.0).astype(BF)
    loads[3].wait()
    for h in range(8):
        wqt[pl.ds(128 * h, 96), :] = qt[pl.ds(96 * h, 96), :]
        wqt[pl.ds(128 * h + 96, 16), :] = qt[pl.ds(96 * h + 80, 16), :]
        wqt[pl.ds(128 * h + 112, 16), :] = qt[pl.ds(96 * h + 64, 16), :]
    loads[4].wait()
    qall = dot_nt(ql, wqt[...])
    kvall = dot(la, lup[...])
    for h in range(8):
        q = qall[:, 128 * h : 128 * h + 128]
        q2 = q * q
        mp = jnp.sum(jnp.where(lane < NOPE, q2, 0.0), axis=-1, keepdims=True) * (1.0 / NOPE)
        mr = jnp.sum(jnp.where(lane >= 96, q2, 0.0), axis=-1, keepdims=True) * (1.0 / ROPE)
        qn = q * jnp.where(lane < NOPE, lax.rsqrt(mp + EPSILON), lax.rsqrt(mr + EPSILON))
        qv = (qn * cq[...] + pltpu.roll(qn, 96, 1) * sq[...]).astype(BF)
        kv = kvall[:, 128 * h : 128 * h + 128]
        mp = jnp.sum(jnp.where(lane < NOPE, kv * kv, 0.0), axis=-1, keepdims=True) * (1.0 / NOPE)
        kvv = (kv * jnp.where(lane < NOPE, lax.rsqrt(mp + EPSILON) * kg[...], 1.0)).astype(BF)
        j = h // 2
        o = (h % 2) * 128
        ksend[j, :, o : o + 128] = kvv
        ksend[j, :, 256 + o : 384 + o] = qv
    for j in range(ny):
        ksend[j, :, 512:640] = rot
    k_copies = [rcopy(ksend.at[lax.rem(y + d, ny)], kgot.at[y], g_ss.at[d], g_rs.at[d], at_y(d)) for d in range(1, ny)]
    for copy in k_copies:
        copy.start()
    kgot[pl.ds(y, 1)] = ksend[pl.ds(y, 1)]

    for copy in n_copies:
        copy.wait_recv()
    for i in range(5, 10):
        loads[i].wait()
    rows = normed[...].reshape(BLOCK, D)
    mem_q = dot(rows, mq[...]).astype(BF)
    mem_k = (dot(rows, mk[...]) * 0.125).astype(BF)
    mem_v = dot(rows, mv[...]).astype(BF)
    gate_t = dot_nt(gt[...], rows).astype(BF)

    for copy in k_copies:
        copy.wait_recv()
    got = kgot[...].reshape(BLOCK, 640)
    first = c == 0
    rsum = (
        (kgot[0, :, 512:640].astype(F32) + kgot[1, :, 512:640].astype(F32))
        + (kgot[2, :, 512:640].astype(F32) + kgot[3, :, 512:640].astype(F32))
    ).astype(BF)
    h0, h1 = got[:, 0:128], got[:, 128:256]
    psend[pl.ds(0, BLOCK), :] = jnp.where(first, h1, h0)
    psend[pl.ds(BLOCK, ROWS), :] = rsum
    p_copy = rcopy(psend, kvg.at[z, c], p_ss, p_rs, {"sp_2": 1 - c})
    p_copy.start()
    qsend[0] = got[:, 256:384]
    qsend[1] = got[:, 384:512]
    q_copies = []
    for d in range(1, nr):
        j = lax.rem(me + d, nr)
        copy = rcopy(qsend.at[lax.rem(j, 2)], qg.at[me], q_ss.at[d], q_rs.at[d], at_row(d))
        copy.start()
        q_copies.append(copy)
    kvg[pl.ds(z, 1), pl.ds(c, 1), pl.ds(0, BLOCK), :] = jnp.where(first, h0, h1)[None, None]
    kvg[pl.ds(z, 1), pl.ds(c, 1), pl.ds(BLOCK, ROWS), :] = rsum[None, None]
    qg[pl.ds(me, 1)] = qsend[pl.ds(c, 1)]

    up, down = {}, {}

    def ring_step(s):
        for half in range(2):
            if s <= nz // 2 - 1 or half == 0:
                chunk = lax.rem(z - (s - 1) + nz, nz)
                copy = rcopy(kvg.at[chunk, half], kvg.at[chunk, half], u_ss.at[s, half], u_rs.at[s, half], at_z(1))
                copy.start()
                up[s, half] = copy
            if s <= nz // 2 - 1 or half == 1:
                chunk = lax.rem(z + (s - 1), nz)
                copy = rcopy(kvg.at[chunk, half], kvg.at[chunk, half], d_ss.at[s, half], d_rs.at[s, half], at_z(nz - 1))
                copy.start()
                down[s, half] = copy

    def ring_wait(s):
        for half in range(2):
            if (s, half) in up:
                up[s, half].wait_recv()
            if (s, half) in down:
                down[s, half].wait_recv()

    lane2 = lanes((BLOCK, 128))
    low = lane2 < 64
    row8 = lax.broadcasted_iota(jnp.int32, (8, 32), 0)
    col8 = lax.broadcasted_iota(jnp.int32, (8, 32), 1)
    pick = (col8 == (row8 // 2) * 8 + y * 2 + lax.rem(row8, 2)).astype(BF)
    pre = dot(pick, gate_t) + goff[...]
    low_t = lax.broadcasted_iota(jnp.int32, (128, BLOCK), 0) < 64

    def spread(r0, r1):
        wide = jnp.where(low_t, jnp.broadcast_to(r0, (128, BLOCK)), jnp.broadcast_to(r1, (128, BLOCK)))
        return jnp.transpose(wide)

    log_f = jnp.minimum(pre, 0.0) - jnp.log1p(jnp.exp(-jnp.abs(pre)))
    ti = lax.broadcasted_iota(jnp.int32, (BLOCK, BLOCK), 0)
    si = lax.broadcasted_iota(jnp.int32, (BLOCK, BLOCK), 1)
    masks = (si <= ti, si >= ti)
    zero = jnp.zeros_like(mem_q)
    s_heads = (dot_nt(jnp.where(low, mem_q, zero), mem_k), dot_nt(jnp.where(low, zero, mem_q), mem_k))
    v_f = mem_v.astype(F32)
    k_f = mem_k.astype(F32)
    q_f = mem_q.astype(F32)
    parts = []
    for way in range(2):
        i_wide = spread(pre[4 * way : 4 * way + 1], pre[4 * way + 1 : 4 * way + 2])
        f_wide = spread(log_f[4 * way + 2 : 4 * way + 3], log_f[4 * way + 3 : 4 * way + 4])
        cum = dot(masks[way].astype(F32), f_wide, HI)
        g = i_wide - cum
        g_t = jnp.transpose(g)
        nums, dens, tops = [], [], []
        for h in range(2):
            decay = cum[:, 64 * h : 64 * h + 1] + g_t[64 * h : 64 * h + 1, :]
            decay = jnp.where(masks[way], decay, -jnp.inf)
            top = jnp.max(decay, axis=-1, keepdims=True)
            w = s_heads[h] * jnp.exp(decay - top)
            dens.append(jnp.sum(w, axis=-1, keepdims=True))
            nums.append(dot(w.astype(BF), mem_v))
            tops.append(top)
        num = jnp.where(low, nums[0], nums[1])
        den = jnp.where(low, dens[0], dens[1])
        top = jnp.where(low, tops[0], tops[1])
        total = jnp.sum(f_wide, axis=0, keepdims=True)
        growth = total + g
        level = jnp.max(growth, axis=0, keepdims=True)
        inflow = jnp.exp(growth - level)
        mat = lax.dot_general(
            inflow * v_f, k_f, (((0,), (0,)), ((), ())), precision=HI, preferred_element_type=F32
        )
        fold = jnp.where(lanes((64, 128)) < 64, mat[:64], mat[64:])
        normal = jnp.sum(inflow * k_f, axis=0, keepdims=True)
        pa[pl.ds(me, 1), way, pl.ds(0, 64), :] = fold[None]
        pa[pl.ds(me, 1), way, pl.ds(64, 8), :] = jnp.concatenate(
            [normal, level, total, jnp.zeros((5, 128), F32)], axis=0
        )[None]
        parts.append((num, den, top, cum))
    a_copies = [rcopy(pa.at[me], pa.at[me], a_ss.at[d], a_rs.at[d], at_row(d)) for d in range(1, nr)]
    for copy in a_copies:
        copy.start()
    p_copy.wait_recv()
    ring_step(1)
    out_gate = jax.nn.sigmoid(dot(rows, mo[...]).astype(BF).astype(F32))

    for copy in a_copies:
        copy.wait_recv()

    def gather_levels(get, count, order, valid, running):
        found = []
        for j in order:
            vec = get(j)
            ok = valid(j)
            found.append((j, ok, jnp.where(ok, vec[1:2] + running, FLOOR_LOG)))
            running = running + jnp.where(ok, vec[2:3], 0.0)
        return found, running

    def merge(entries):
        joined = entries[0][2]
        for _, _, level in entries[1:]:
            joined = jnp.maximum(joined, level)
        mat = jnp.zeros((72, 128), F32)
        for fetch, ok, level in entries:
            scale = jnp.where(ok, jnp.exp(level - joined), 0.0)
            mat = mat + jnp.where(ok, fetch(), 0.0) * scale
        return mat, joined

    def row_vec(way):
        return lambda j: pa[j, way, pl.ds(64, 8), :]

    def row_mat(way, j):
        return lambda: pa[j, way]

    orders = (list(reversed(range(nr))), list(range(nr)))
    z_orders = (list(reversed(range(nz))), list(range(nz)))
    for way in range(2):
        found, total = gather_levels(row_vec(way), nr, orders[way], lambda j: j >= 0, jnp.zeros((1, 128), F32))
        mat, joined = merge([(row_mat(way, j), ok, level) for j, ok, level in found])
        rtot[way, pl.ds(0, 64), :] = mat[:64]
        rtot[way, pl.ds(64, 8), :] = jnp.concatenate(
            [mat[64:65], joined, total, jnp.zeros((5, 128), F32)], axis=0
        )
    b_copies = []
    for d in range(1, nz):
        wrapped = (z + d) // nz
        copy = rcopy(rtot.at[wrapped], pb.at[z], b_ss.at[d], b_rs.at[d], at_z(d))
        copy.start()
        b_copies.append(copy)
    pb[pl.ds(z, 1)] = jnp.zeros((1, 72, 128), F32)
    ring_wait(1)
    ring_step(2)
    for copy in b_copies:
        copy.wait_recv()

    hsum = jnp.zeros((BLOCK, 128), F32)
    bi = lax.broadcasted_iota(jnp.int32, (128, 128), 0) // 64
    bj = lax.broadcasted_iota(jnp.int32, (128, 128), 1) // 64
    ones_block = (bi == bj).astype(F32)
    for way in range(2):
        if way == 0:
            ok_row, ok_z = (lambda j: j < me), (lambda j: j < z)
        else:
            ok_row, ok_z = (lambda j: j > me), (lambda j: j > z)
        found, running = gather_levels(row_vec(way), nr, orders[way], ok_row, jnp.zeros((1, 128), F32))
        entries = [(row_mat(way, j), ok, level) for j, ok, level in found]
        found, _ = gather_levels(lambda j: pb[j, pl.ds(64, 8), :], nz, z_orders[way], ok_z, running)
        entries += [((lambda j: (lambda: pb[j]))(j), ok, level) for j, ok, level in found]
        mat, level = merge(entries)
        fold, normal = mat[:64], mat[64:65]
        low64 = lanes((64, 128)) < 64
        full = jnp.concatenate([jnp.where(low64, fold, 0.0), jnp.where(low64, 0.0, fold)], axis=0)
        num, den, top, cum = parts[way]
        carried_log = cum + level
        joined = jnp.maximum(top, carried_log)
        own = jnp.exp(top - joined)
        carried = jnp.exp(carried_log - joined)
        num = num * own + carried * dot_nt(q_f, full, HI)
        den = den * own + carried * dot(q_f * normal, ones_block, HI)
        hsum = hsum + num / jnp.maximum(jnp.abs(den), jnp.exp(-joined))
    mean = dot(hsum * hsum, ones_block, HI) * (1.0 / 64)
    combined = hsum * lax.rsqrt(mean + EPSILON) * mng[pl.ds(y, 1), :]
    mem_rows = (combined * out_gate).astype(BF)
    for j in range(ny):
        fsend[j, :, 0:128] = mem_rows[64 * j : 64 * j + 64]

    for copy in q_copies:
        copy.wait_recv()
    ring_wait(2)
    ring_step(3)
    tile_r = lax.broadcasted_iota(jnp.int32, (128, 128), 0)
    tile_c = lax.broadcasted_iota(jnp.int32, (128, 128), 1)
    tile_m = (tile_r == 64 + lax.rem(tile_c, 32)).astype(BF)

    for j in range(nr):
        slab = qg[j]
        qop[j, :, 0:128] = jnp.where(low, slab, jnp.zeros_like(slab))
        qop[j, :, 128:256] = dot(slab, tile_m).astype(BF)
    ring_wait(3)
    ring_step(nz // 2)
    ring_wait(nz // 2)

    def fill(i, carry):
        for half in range(2):
            base = pl.multiple_of(i * 512 + half * 256, 256)
            kvs = kvg[i, half, pl.ds(0, BLOCK), :]
            kop[pl.ds(base, BLOCK), 0:128] = kvs
            vop[pl.ds(base, BLOCK), :] = jnp.where(low, jnp.ones_like(kvs), kvs)
            r = kvg[i, half, pl.ds(BLOCK, ROWS), :]
            for j in range(4):
                kop[pl.ds(base + 64 * j, ROWS), 128:256] = jnp.where(lane // ROPE == j, r, jnp.zeros_like(r))
        return carry

    lax.fori_loop(0, nz, fill, 0)
    n_chunks = nz * 512 // KCHUNK

    def block(i, carry):
        d = lax.rem(i + 1, nr)
        j = lax.rem(me + d, nr)
        qv = qop[j]
        top = jnp.full((BLOCK, 1), FLOOR_LOG, F32)
        acc = jnp.zeros((BLOCK, 128), F32)
        for k in range(n_chunks):
            s = dot_nt(qv, kop[pl.ds(k * KCHUNK, KCHUNK), :])
            new = jnp.maximum(top, jnp.max(s, axis=-1, keepdims=True))
            p = jnp.exp(s - new).astype(BF)
            acc = acc * jnp.exp(top - new) + dot(p, vop[pl.ds(k * KCHUNK, KCHUNK), :])
            top = new
        den = acc[:, 0:1]
        lse = top + jnp.log(den)
        hi = lse.astype(BF).astype(F32)
        mid = (lse - hi).astype(BF).astype(F32)
        lo = (lse - hi) - mid
        msg = jnp.where(lane2 == 0, hi, jnp.where(lane2 == 1, mid, jnp.where(lane2 == 2, lo, acc / den)))
        osend[pl.ds(d, 1)] = msg.astype(BF)[None]

        @pl.when(i < nr - 1)
        def _():
            rcopy(osend.at[d], po.at[me], o_ss.at[d], o_rs.at[d], at_row(d)).start()

        return carry

    lax.fori_loop(0, nr, block, 0)
    po[pl.ds(me, 1)] = osend[pl.ds(0, 1)]
    o_copies = [rcopy(osend.at[d], po.at[me], o_ss.at[d], o_rs.at[d], at_row(d)) for d in range(1, nr)]
    for copy in o_copies:
        copy.wait_recv()
    heads = []
    for h in range(2):
        msgs = [po[2 * j + h].astype(F32) for j in range(nx)]
        lses = [(m[:, 0:1] + m[:, 1:2]) + m[:, 2:3] for m in msgs]
        joined = functools.reduce(jnp.maximum, lses)
        ws = [jnp.exp(v - joined) for v in lses]
        heads.append(sum(w * m for w, m in zip(ws, msgs)) / sum(ws))
    att = jnp.where(low, pltpu.roll(heads[0], 64, 1), heads[1]).astype(BF)
    for j in range(ny):
        fsend[j, :, 128:256] = att[64 * j : 64 * j + 64]

    f_copies = [rcopy(fsend.at[lax.rem(y + d, ny)], fx.at[y], f_ss.at[d], f_rs.at[d], at_y(d)) for d in range(1, ny)]
    for copy in f_copies:
        copy.start()
    fx[pl.ds(y, 1)] = fsend[pl.ds(y, 1)]
    loads[10].wait()
    loads[11].wait()
    for copy in f_copies:
        copy.wait_recv()
    for j in range(ny):
        lhs_m[:, 128 * j : 128 * j + 128] = fx[j, :, 0:128]
        lhs_a[:, 128 * j : 128 * j + 128] = fx[j, :, 128:256]
    out[...] = (dot(lhs_m[...], wm[...]) + dot(lhs_a[...], wa[...])).astype(BF)

    for copies in (n_copies, k_copies, [p_copy], q_copies, a_copies, b_copies, o_copies, f_copies):
        for copy in copies:
            copy.wait_send()
    for copy in list(up.values()) + list(down.values()):
        copy.wait_send()


def tables(segment, member, query_gain, key_gain):
    lane = jnp.arange(128, dtype=jnp.int32)
    positions = segment * BLOCK + member * ROWS + jnp.arange(ROWS, dtype=jnp.int32)
    frequency = ROPE_BASE ** (-(lane % 16).astype(F32) / 16)
    angles = positions.astype(F32)[:, None] * frequency[None, :]
    cosine, sine = jnp.cos(angles), jnp.sin(angles)
    sign = jnp.where(lane % 32 < 16, -1.0, 1.0)
    own = key_gain[NOPE + lane % 32]
    swapped = key_gain[NOPE + (lane + 16) % 32]
    cr = cosine * own
    sr = sine * sign * swapped
    scale = (NOPE + ROPE) ** (-0.5)
    in_rope = (lane >= 64) & (lane < 96)
    q_own = jnp.where(lane < 96, query_gain[jnp.minimum(lane, 95)], 0.0) * scale
    q_swap = query_gain[NOPE + (lane + 16) % 32] * scale
    cq = jnp.where(lane < 64, 1.0, jnp.where(in_rope, cosine, 0.0)) * q_own
    sq = jnp.where(in_rope, sine * sign * q_swap, 0.0)
    kg = key_gain[jnp.minimum(lane, 63)]
    return cq, sq, cr, sr, kg[None, :]


def body(nz, nx, ny, tokens, input_gain, memory_query, memory_key, memory_value, memory_outgate, memory_gates,
         gate_offset, memory_norm_gain, query_down, query_down_gain, latent_down, latent_gain, rotary_down,
         query_up, latent_up, query_gain, key_gain, memory_output, attention_output):
    segment = lax.axis_index(SP)
    member = lax.axis_index("tp")
    cq, sq, cr, sr, kg = tables(segment, member, query_gain, key_gain)
    args = (
        tokens, input_gain.reshape(1, D), memory_query, memory_key, memory_value, memory_outgate,
        jnp.transpose(memory_gates, (1, 2, 0)).reshape(32, D),
        jnp.transpose(gate_offset, (0, 2, 1)).reshape(8, BLOCK),
        memory_norm_gain.reshape(4, 128), query_down, query_down_gain.reshape(1, QR), latent_down,
        latent_gain.reshape(1, KVR), rotary_down.T,
        jnp.transpose(query_up, (1, 2, 0)).reshape(8 * (NOPE + ROPE), QR),
        latent_up.reshape(KVR, 1024), cq, sq, cr, sr, kg, memory_output, attention_output,
    )
    nr = nx * 2
    in_hbm = {2, 3, 4, 5, 6, 9, 11, 13, 14, 15, 21, 22}
    vmem = pl.BlockSpec(memory_space=pltpu.VMEM)
    hbm = pl.BlockSpec(memory_space=pl.ANY)
    dma = pltpu.SemaphoreType.DMA
    keys = nz * 512
    scratch = [
        pltpu.VMEM((D, 128), BF), pltpu.VMEM((D, 128), BF), pltpu.VMEM((D, 128), BF), pltpu.VMEM((D, 128), BF),
        pltpu.VMEM((32, D), BF), pltpu.VMEM((D, QR), BF), pltpu.VMEM((D, KVR), BF), pltpu.VMEM((32, D), BF),
        pltpu.VMEM((768, QR), BF), pltpu.VMEM((KVR, 1024), BF), pltpu.VMEM((512, D), BF), pltpu.VMEM((512, D), BF),
        pltpu.VMEM((256, D), BF), pltpu.VMEM((1024, QR), BF), pltpu.VMEM((ny, ROWS, D), BF),
        pltpu.VMEM((ny, ROWS, 640), BF), pltpu.VMEM((ny, ROWS, 640), BF),
        pltpu.VMEM((nz, 2, BLOCK + ROWS, 128), BF), pltpu.VMEM((BLOCK + ROWS, 128), BF),
        pltpu.VMEM((2, BLOCK, 128), BF), pltpu.VMEM((nr, BLOCK, 128), BF),
        pltpu.VMEM((nr, 2, 72, 128), F32), pltpu.VMEM((2, 72, 128), F32), pltpu.VMEM((nz, 72, 128), F32),
        pltpu.VMEM((nr, BLOCK, 256), BF), pltpu.VMEM((keys, 256), BF), pltpu.VMEM((keys, 128), BF),
        pltpu.VMEM((nr, BLOCK, 128), BF), pltpu.VMEM((nr, BLOCK, 128), BF),
        pltpu.VMEM((ny, ROWS, 256), BF), pltpu.VMEM((ny, ROWS, 256), BF),
        pltpu.VMEM((ROWS, 512), BF), pltpu.VMEM((ROWS, 512), BF),
        dma((12,)), dma((ny,)), dma((ny,)), dma((ny,)), dma((ny,)), dma, dma,
        dma((nr,)), dma((nr,)), dma((nr,)), dma((nr,)), dma((nz,)), dma((nz,)),
        dma((nz // 2 + 1, 2)), dma((nz // 2 + 1, 2)), dma((nz // 2 + 1, 2)), dma((nz // 2 + 1, 2)),
        dma((nr,)), dma((nr,)), dma((ny,)), dma((ny,)),
    ]
    return pl.pallas_call(
        functools.partial(kernel, nz, nx, ny),
        out_shape=jax.ShapeDtypeStruct((ROWS, D), BF),
        in_specs=[hbm if i in in_hbm else vmem for i in range(len(args))],
        out_specs=vmem,
        scratch_shapes=scratch,
        compiler_params=pltpu.CompilerParams(
            collective_id=0, has_side_effects=True, vmem_limit_bytes=60 * 1024 * 1024
        ),
        name="mixer",
    )(*args)


def solution(mesh):
    ny = mesh.shape["tp"]
    nz, nx = 8, 4
    split = Mesh(mesh.devices.reshape(nz, nx, 2, ny), ("sp_0", "sp_1", "sp_2", "tp"))
    rep = P()
    head = P(None, "tp")
    in_specs = (
        P(SP_TP, None), rep, head, head, head, head, rep, P(None, SP, "tp"),
        rep, rep, rep, rep, rep, rep, rep, rep, rep, rep, rep, rep,
    )
    return jax.shard_map(
        functools.partial(body, nz, nx, ny), mesh=split, in_specs=in_specs, out_specs=P(SP_TP, None), check_vma=False
    )
```

```python
import functools

import jax
import jax.numpy as jnp
from jax import lax
from jax.experimental import pallas as pl
from jax.experimental.pallas import tpu as pltpu
from jax.sharding import Mesh
from jax.sharding import PartitionSpec as P

D = 2048
NOPE = 64
ROPE = 32
ROWS = 64
BLOCK = 256
QR = 384
KVR = 256
SP = ("sp_0", "sp_1", "sp_2")
SP_TP = ("sp_0", "sp_1", "sp_2", "tp")
EPSILON = 1e-06
ROPE_BASE = 10000.0
FLOOR_LOG = -1e30
BF = jnp.bfloat16
F32 = jnp.float32
MESH = pl.DeviceIdType.MESH
HI = lax.Precision.HIGHEST
FREQUENCIES = [float(ROPE_BASE ** (-j / 16)) for j in range(16)]


def dot(a, b, precision=None):
    return lax.dot_general(a, b, (((1,), (0,)), ((), ())), precision=precision, preferred_element_type=F32)


def dot_nt(a, b, precision=None):
    return lax.dot_general(a, b, (((1,), (1,)), ((), ())), precision=precision, preferred_element_type=F32)


def lanes(shape):
    return lax.broadcasted_iota(jnp.int32, shape, len(shape) - 1)


def rcopy(src, dst, send_sem, recv_sem, device):
    return pltpu.make_async_remote_copy(
        src_ref=src, dst_ref=dst, send_sem=send_sem, recv_sem=recv_sem, device_id=device, device_id_type=MESH
    )


def rms(v):
    return v * lax.rsqrt(jnp.mean(v * v, axis=-1, keepdims=True) + EPSILON)


def kernel(
    nz, nx, ny,
    tok, gain, hmq, hmk, hmv, hmo, hgt, goff, mng, hqd, qdg, hld, lg, hrt, hqt, hlup,
    qgain, kgain, hwm, hwa,
    out,
    mq, mk, mv, mo, gt, qd, ld, rt, qt, lup, wm, wa,
    rt4, wqt, lupf, trig, normed, ebuf, kvg, psend, qsend, qg, asend, agot, rtot, pb, csend, cgot,
    qop, kop, vt, acc_s, top_s, osend, po, fsend, fx, lhs_m, lhs_a,
    w_sem, n_ss, n_rs, e_ss, e_rs, p_ss, p_rs, q_ss, q_rs, a_ss, a_rs, b_ss, b_rs, c_ss, c_rs,
    u_ss, u_rs, d_ss, d_rs, o_ss, o_rs, f_ss, f_rs,
):
    z = lax.axis_index("sp_0")
    x = lax.axis_index("sp_1")
    c = lax.axis_index("sp_2")
    y = lax.axis_index("tp")
    nr = nx * 2
    me = x * 2 + c

    def at_y(d):
        return {"tp": lax.rem(y + d, ny)}

    def at_row(d):
        j = lax.rem(me + d, nr)
        return {"sp_1": j // 2, "sp_2": lax.rem(j, 2)}

    def at_z(d):
        return {"sp_0": lax.rem(z + d, nz)}

    pairs = ((hqd, qd), (hld, ld), (hrt, rt), (hlup, lup), (hqt, qt), (hmq, mq), (hmk, mk), (hmv, mv),
             (hgt, gt), (hmo, mo), (hwm, wm), (hwa, wa))
    loads = [pltpu.make_async_copy(a, b, w_sem.at[i]) for i, (a, b) in enumerate(pairs)]
    for load in loads:
        load.start()
    barrier = pltpu.get_barrier_semaphore()
    peers = [at_y(d) for d in range(1, ny)] + [at_row(d) for d in range(1, nr)] + [at_z(d) for d in range(1, nz)]
    for peer in peers:
        pl.semaphore_signal(barrier, inc=1, device_id=peer, device_id_type=MESH)

    xt = tok[...].astype(F32)
    normed_local = (rms(xt) * gain[...]).astype(BF)
    normed[pl.ds(y, 1)] = normed_local[None]

    segment = (z * nx + x) * 2 + c
    places = (segment * BLOCK + lax.broadcasted_iota(jnp.int32, (16, BLOCK), 1)).astype(F32)
    line = lax.broadcasted_iota(jnp.int32, (16, BLOCK), 0)
    frequency = jnp.zeros((16, BLOCK), F32)
    for j in range(16):
        frequency = jnp.where(line == j, FREQUENCIES[j], frequency)
    angles = places * frequency
    trig[0] = jnp.transpose(jnp.concatenate([jnp.cos(angles)] * 8, axis=0))
    trig[1] = jnp.transpose(jnp.concatenate([jnp.sin(angles)] * 8, axis=0))

    src = lax.broadcasted_iota(jnp.int32, (96, 128), 0)
    dst = lax.broadcasted_iota(jnp.int32, (96, 128), 1)
    rope_own, rope_swap = 64 + lax.rem(dst, 32), 64 + lax.rem(dst + 16, 32)
    q8 = jnp.broadcast_to(qgain[...], (8, 96))
    k8 = jnp.broadcast_to(kgain[...], (8, 96))
    scale = (NOPE + ROPE) ** (-0.5)
    q_own = dot(q8, (src == dst).astype(F32), HI)[0:1] * scale
    q_swap = dot(q8, (src == rope_swap).astype(F32), HI)[0:1] * scale
    k_own = dot(k8, (src == rope_own).astype(F32), HI)[0:1]
    k_swap = dot(k8, (src == rope_swap).astype(F32), HI)[0:1]
    k_plain = dot(k8, (src == dst).astype(F32), HI)[0:1]
    lane1 = lanes((1, 128))
    sign = jnp.where(lax.rem(lane1, 32) < 16, -1.0, 1.0)
    in_rope = jnp.logical_and(lane1 >= 64, lane1 < 96)

    loads[0].wait()
    loads[1].wait()
    qdg_row = jnp.concatenate([qdg[i : i + 1, :] for i in range(3)], axis=1)
    ql = (rms(dot(normed_local, qd[...])) * qdg_row).astype(BF)
    la = (rms(dot(normed_local, ld[...])) * lg[...]).astype(BF)
    loads[2].wait()
    for i in range(4):
        rt4[pl.ds(32 * i, 32), :] = rt[...]
        rt4[pl.ds(128 + 32 * i, 16), :] = rt[pl.ds(16, 16), :]
        rt4[pl.ds(128 + 32 * i + 16, 16), :] = rt[pl.ds(0, 16), :]
    ro = dot_nt(normed_local, rt4[...])
    ra, rb = ro[:, :128], ro[:, 128:]
    rscale = lax.rsqrt(jnp.mean(ra * ra, axis=-1, keepdims=True) + EPSILON)
    lane = lanes((ROWS, 128))
    own_rows = pl.ds(pl.multiple_of(y * ROWS, ROWS), ROWS)
    rot = (ra * rscale) * (trig[0, own_rows, :] * k_own) + (rb * rscale) * (trig[1, own_rows, :] * (k_swap * sign))
    rot = jnp.where(lane // ROPE == y, rot, 0.0).astype(BF)
    ebuf[pl.ds(y, 1), :, 0:256] = la[None]
    ebuf[pl.ds(y, 1), :, 256:384] = rot[None]
    ebuf[pl.ds(y, 1), :, 384:768] = ql[None]

    pl.semaphore_wait(barrier, len(peers))

    def spread_y(buf, ss, rs):
        lo, hi = pl.ds(0, ROWS // 2), pl.ds(ROWS // 2, ROWS // 2)
        below, above = lax.rem(y + ny - 1, ny), lax.rem(y + 1, ny)

        def one(i, slot, part, d):
            return rcopy(buf.at[slot, part], buf.at[slot, part], ss.at[i], rs.at[i], at_y(d))

        direct = [one(0, y, lo, 1), one(3, y, hi, ny - 1), one(1, y, hi, 1), one(4, y, lo, ny - 1)]
        onward = [one(2, below, lo, 1), one(5, above, hi, ny - 1)]
        return direct, onward

    e_direct, e_onward = spread_y(ebuf, e_ss, e_rs)
    n_direct, n_onward = spread_y(normed, n_ss, n_rs)
    for copy in e_direct:
        copy.start()
    loads[3].wait()
    lupf[...] = lup[...].astype(F32)
    loads[4].wait()
    for h in range(2):
        base = 96 * (2 * y + h)
        wqt[h, pl.ds(0, 96), :] = qt[pl.ds(pl.multiple_of(base, 32), 96), :]
        wqt[h, pl.ds(96, 16), :] = qt[pl.ds(pl.multiple_of(base + 80, 16), 16), :]
        wqt[h, pl.ds(112, 16), :] = qt[pl.ds(pl.multiple_of(base + 64, 16), 16), :]
    for i in range(2):
        e_direct[i].wait_recv()
        e_onward[i].start()
    for copy in n_direct:
        copy.start()
    e_direct[2].wait_recv()
    e_direct[3].wait_recv()
    for copy in e_onward:
        copy.wait_recv()

    lane2 = lanes((BLOCK, 128))
    low = lane2 < 64
    la_all = ebuf[:, :, 0:256].reshape(BLOCK, KVR)
    kv = []
    for h in range(2):
        w = lupf[pl.ds(2 * y + h, KVR, stride=8), :].astype(BF)
        t = dot(la_all, w)
        mp = jnp.sum(jnp.where(low, t * t, 0.0), axis=-1, keepdims=True) * (1.0 / NOPE)
        kv.append((t * jnp.where(low, lax.rsqrt(mp + EPSILON) * k_plain, 1.0)).astype(BF))
    rsum = (
        (ebuf[0, :, 256:384].astype(F32) + ebuf[1, :, 256:384].astype(F32))
        + (ebuf[2, :, 256:384].astype(F32) + ebuf[3, :, 256:384].astype(F32))
    ).astype(BF)
    first = c == 0
    kvg[pl.ds(z, 1), 0, pl.ds(0, BLOCK), :] = jnp.where(first, kv[0], kv[1])[None]
    kvg[pl.ds(z, 1), 0, pl.ds(BLOCK, ROWS), :] = rsum[None]
    psend[pl.ds(0, BLOCK), :] = jnp.where(first, kv[1], kv[0])
    psend[pl.ds(BLOCK, ROWS), :] = rsum
    p_copy = rcopy(psend, kvg.at[z, 1], p_ss, p_rs, {"sp_2": 1 - c})
    p_copy.start()

    up, down = {}, {}
    far = nz // 2

    def ring_send(s, r):
        if s < far or r == 0:
            k = lax.rem(z - (s - 1) + nz, nz)
            up[s, r] = rcopy(kvg.at[k, r], kvg.at[k, r], u_ss.at[s, r], u_rs.at[s, r], at_z(1))
            up[s, r].start()
        if s < far or r == 1:
            k = lax.rem(z + (s - 1), nz)
            down[s, r] = rcopy(kvg.at[k, r], kvg.at[k, r], d_ss.at[s, r], d_rs.at[s, r], at_z(nz - 1))
            down[s, r].start()

    def ring_recv(s, r):
        for way in (up, down):
            if (s, r) in way:
                way[s, r].wait_recv()
        if s < far:
            ring_send(s + 1, r)

    ring_send(1, 0)
    ql_all = ebuf[:, :, 384:768].reshape(BLOCK, QR)
    cos_q = trig[0] * jnp.where(in_rope, q_own, 0.0) + jnp.where(lane1 < 64, q_own, 0.0)
    sin_q = trig[1] * jnp.where(in_rope, q_swap * sign, 0.0)
    for h in range(2):
        q = dot_nt(ql_all, wqt[h])
        q2 = q * q
        mp = jnp.sum(jnp.where(low, q2, 0.0), axis=-1, keepdims=True) * (1.0 / NOPE)
        mr = jnp.sum(jnp.where(lane2 >= 96, q2, 0.0), axis=-1, keepdims=True) * (1.0 / ROPE)
        qn = q * jnp.where(low, lax.rsqrt(mp + EPSILON), lax.rsqrt(mr + EPSILON))
        qsend[h] = (qn * cos_q + pltpu.roll(qn, 96, 1) * sin_q).astype(BF)
    q_copies = []
    for d in range(1, nr):
        j = lax.rem(me + d, nr)
        copy = rcopy(qsend.at[lax.rem(j, 2)], qg.at[me], q_ss.at[d], q_rs.at[d], at_row(d))
        copy.start()
        q_copies.append(copy)
    qg[pl.ds(me, 1)] = qsend[pl.ds(c, 1)]
    for i in range(2):
        n_direct[i].wait_recv()
        n_onward[i].start()
    p_copy.wait_recv()
    ring_send(1, 1)

    def fill(slot, d):
        k = lax.rem(z + d + nz, nz)
        for r in range(2):
            base = slot * 512 + r * 256
            kvs = kvg[k, r, pl.ds(0, BLOCK), :]
            kop[pl.ds(base, BLOCK), 0:128] = kvs
            vt[:, base : base + BLOCK] = jnp.transpose(jnp.where(low, jnp.ones_like(kvs), kvs))
            rr = kvg[k, r, pl.ds(BLOCK, ROWS), :]
            for j in range(4):
                kop[pl.ds(base + 64 * j, ROWS), 128:256] = jnp.where(lane // ROPE == j, rr, jnp.zeros_like(rr))

    fill(0, 0)
    n_direct[2].wait_recv()
    n_direct[3].wait_recv()
    for copy in n_onward:
        copy.wait_recv()
    for i in range(5, 9):
        loads[i].wait()
    rows = normed[...].reshape(BLOCK, D)
    mem_q = dot(rows, mq[...]).astype(BF)
    mem_k = (dot(rows, mk[...]) * 0.125).astype(BF)
    mem_v = dot(rows, mv[...]).astype(BF)
    gate_t = dot_nt(gt[...], rows).astype(BF)
    ring_recv(1, 0)

    row8 = lax.broadcasted_iota(jnp.int32, (8, 32), 0)
    col8 = lax.broadcasted_iota(jnp.int32, (8, 32), 1)
    pick = (col8 == (row8 // 2) * 8 + y * 2 + lax.rem(row8, 2)).astype(BF)
    pre = dot(pick, gate_t) + jnp.concatenate([goff[i] for i in range(4)], axis=0)
    low_t = lax.broadcasted_iota(jnp.int32, (128, BLOCK), 0) < 64

    def spread(r0, r1):
        wide = jnp.where(low_t, jnp.broadcast_to(r0, (128, BLOCK)), jnp.broadcast_to(r1, (128, BLOCK)))
        return jnp.transpose(wide)

    log_f = jnp.minimum(pre, 0.0) - jnp.log1p(jnp.exp(-jnp.abs(pre)))
    ti = lax.broadcasted_iota(jnp.int32, (BLOCK, BLOCK), 0)
    si = lax.broadcasted_iota(jnp.int32, (BLOCK, BLOCK), 1)
    masks = (si <= ti, si >= ti)
    zero = jnp.zeros_like(mem_q)
    s_heads = (dot_nt(jnp.where(low, mem_q, zero), mem_k), dot_nt(jnp.where(low, zero, mem_q), mem_k))
    v_f = mem_v.astype(F32)
    k_f = mem_k.astype(F32)
    q_f = mem_q.astype(F32)
    parts = []
    for way in range(2):
        i_wide = spread(pre[4 * way : 4 * way + 1], pre[4 * way + 1 : 4 * way + 2])
        f_wide = spread(log_f[4 * way + 2 : 4 * way + 3], log_f[4 * way + 3 : 4 * way + 4])
        cum = dot(masks[way].astype(F32), f_wide, HI)
        g = i_wide - cum
        g_t = jnp.transpose(g)
        total = jnp.sum(f_wide, axis=0, keepdims=True)
        growth = total + g
        level = jnp.max(growth, axis=0, keepdims=True)
        inflow = jnp.exp(growth - level)
        mat = lax.dot_general(
            inflow * v_f, k_f, (((0,), (0,)), ((), ())), precision=HI, preferred_element_type=F32
        )
        fold = jnp.where(lanes((64, 128)) < 64, mat[:64], mat[64:])
        normal = jnp.sum(inflow * k_f, axis=0, keepdims=True)
        vecs = jnp.concatenate([normal, level, total, jnp.zeros((5, 128), F32)], axis=0)
        for j in range(nr):
            asend[j, way, pl.ds(0, 8), :] = fold[8 * j : 8 * j + 8]
            asend[j, way, pl.ds(8, 8), :] = vecs
        parts.append((cum, g_t))
    a_copies = [
        rcopy(asend.at[lax.rem(me + d, nr)], agot.at[me], a_ss.at[d], a_rs.at[d], at_row(d)) for d in range(1, nr)
    ]
    for copy in a_copies:
        copy.start()
    agot[pl.ds(me, 1)] = asend[pl.ds(me, 1)]
    ring_recv(1, 1)
    own_parts = []
    for way in range(2):
        cum, g_t = parts[way]
        nums, dens, tops = [], [], []
        for h in range(2):
            decay = cum[:, 64 * h : 64 * h + 1] + g_t[64 * h : 64 * h + 1, :]
            decay = jnp.where(masks[way], decay, -jnp.inf)
            top = jnp.max(decay, axis=-1, keepdims=True)
            w = s_heads[h] * jnp.exp(decay - top)
            dens.append(jnp.sum(w, axis=-1, keepdims=True))
            nums.append(dot(w.astype(BF), mem_v))
            tops.append(top)
        own_parts.append((
            jnp.where(low, nums[0], nums[1]), jnp.where(low, dens[0], dens[1]), jnp.where(low, tops[0], tops[1]), cum
        ))
    loads[9].wait()
    out_gate = jax.nn.sigmoid(dot(rows, mo[...]).astype(BF).astype(F32))
    fill(1, -1)
    fill(2, 1)

    def chain(early, late):
        joined = jnp.maximum(late[10:11] + early[1], late[9:10])
        scale_e = jnp.exp(late[10:11] + early[1] - joined)
        scale_l = jnp.exp(late[9:10] - joined)
        return (scale_e * early[0] + scale_l * late, joined, early[2] + late[10:11])

    blank = (jnp.zeros((16, 128), F32), jnp.full((1, 128), FLOOR_LOG, F32), jnp.zeros((1, 128), F32))

    def packed(state):
        mat, level, total = state
        line = lax.broadcasted_iota(jnp.int32, (16, 128), 0)
        return jnp.where(line == 9, level, jnp.where(line == 10, total, mat))

    row_orders = (list(range(nr)), list(reversed(range(nr))))
    z_orders = (list(range(nz)), list(reversed(range(nz))))

    for copy in a_copies:
        copy.wait_recv()
    for way in range(2):
        state = blank
        for j in row_orders[way]:
            state = chain(state, agot[j, way])
        rtot[way] = packed(state)
    b_copies = []
    for d in range(1, nz):
        copy = rcopy(rtot.at[(z + d) // nz], pb.at[z], b_ss.at[d], b_rs.at[d], at_z(d))
        copy.start()
        b_copies.append(copy)
    pb[pl.ds(z, 1)] = jnp.zeros((1, 16, 128), F32)

    for copy in q_copies:
        copy.wait_recv()
    tile_r = lax.broadcasted_iota(jnp.int32, (128, 128), 0)
    tile_c = lax.broadcasted_iota(jnp.int32, (128, 128), 1)
    tile_m = (tile_r == 64 + lax.rem(tile_c, 32)).astype(BF)
    for j in range(nr):
        slab = qg[j]
        qop[j, :, 0:128] = jnp.where(low, slab, jnp.zeros_like(slab))
        qop[j, :, 128:256] = dot(slab, tile_m).astype(BF)

    def attend(begin, end, slots, start):
        def block(i, carry):
            j = lax.rem(me + i + 1, nr)
            qv = qop[j]
            if start:
                top = jnp.full((1, BLOCK), FLOOR_LOG, F32)
                acc = jnp.zeros((128, BLOCK), F32)
            else:
                top = top_s[j, 0:1, :]
                acc = acc_s[j]
            for k in slots:
                s = dot_nt(kop[pl.ds(k * 512, 512), :], qv)
                new = jnp.maximum(top, jnp.max(s, axis=0, keepdims=True))
                p = jnp.exp(s - new).astype(BF)
                acc = acc * jnp.exp(top - new) + dot(vt[:, k * 512 : k * 512 + 512], p)
                top = new
            return finish(i, j, top, acc)

        def keep(i, j, top, acc):
            top_s[j] = jnp.broadcast_to(top, (8, BLOCK))
            acc_s[j] = acc
            return 0

        def send(i, j, top, acc):
            d = lax.rem(i + 1, nr)
            den = acc[0:1, :]
            lse = top + jnp.log(den)
            hi = lse.astype(BF).astype(F32)
            mid = (lse - hi).astype(BF).astype(F32)
            lo = (lse - hi) - mid
            at = lax.broadcasted_iota(jnp.int32, (128, BLOCK), 0)
            msg = jnp.where(at == 0, hi, jnp.where(at == 1, mid, jnp.where(at == 2, lo, acc / den)))
            osend[pl.ds(d, 1)] = jnp.transpose(msg).astype(BF)[None]

            @pl.when(i < nr - 1)
            def _():
                rcopy(osend.at[d], po.at[me], o_ss.at[d], o_rs.at[d], at_row(d)).start()

            return 0

        finish = send if end is None else keep
        stop = nr if end is None else end
        lax.fori_loop(begin, stop, block, 0)

    attend(0, nr // 2, (0, 1, 2), True)
    ring_recv(2, 0)
    attend(nr // 2, nr, (0, 1, 2), True)
    ring_recv(2, 1)
    for copy in b_copies:
        copy.wait_recv()
    for way in range(2):
        state = blank
        for j in z_orders[way]:
            ok = (j < z) if way == 0 else (j > z)
            new = chain(state, pb[j])
            state = tuple(jnp.where(ok, a, b) for a, b in zip(new, state))
        for j in row_orders[way]:
            csend[j, way] = packed(state)
            state = chain(state, agot[j, way])
    c_copies = [
        rcopy(csend.at[lax.rem(me + d, nr)], cgot.at[me], c_ss.at[d], c_rs.at[d], at_row(d)) for d in range(1, nr)
    ]
    for copy in c_copies:
        copy.start()
    cgot[pl.ds(me, 1)] = csend[pl.ds(me, 1)]
    fill(3, -2)
    fill(4, 2)
    attend(0, nr // 2, (3, 4), False)
    ring_recv(3, 0)
    attend(nr // 2, nr, (3, 4), False)
    ring_recv(3, 1)
    for copy in c_copies:
        copy.wait_recv()

    hsum = jnp.zeros((BLOCK, 128), F32)
    bi = lax.broadcasted_iota(jnp.int32, (128, 128), 0) // 64
    bj = lax.broadcasted_iota(jnp.int32, (128, 128), 1) // 64
    ones_block = (bi == bj).astype(F32)
    low64 = lanes((64, 128)) < 64
    for way in range(2):
        fold = jnp.concatenate([cgot[j, way, pl.ds(0, 8), :] for j in range(nr)], axis=0)
        normal = cgot[0, way, pl.ds(8, 1), :]
        level = cgot[0, way, pl.ds(9, 1), :]
        full = jnp.concatenate([jnp.where(low64, fold, 0.0), jnp.where(low64, 0.0, fold)], axis=0)
        num, den, top, cum = own_parts[way]
        carried_log = cum + level
        joined = jnp.maximum(top, carried_log)
        own = jnp.exp(top - joined)
        carried = jnp.exp(carried_log - joined)
        num = num * own + carried * dot_nt(q_f, full, HI)
        den = den * own + carried * dot(q_f * normal, ones_block, HI)
        hsum = hsum + num / jnp.maximum(jnp.abs(den), jnp.exp(-joined))
    mean = dot(hsum * hsum, ones_block, HI) * (1.0 / 64)
    combined = hsum * lax.rsqrt(mean + EPSILON) * mng[pl.ds(y, 1), :]
    mem_rows = (combined * out_gate).astype(BF)
    for j in range(ny):
        fsend[0, j] = mem_rows[64 * j : 64 * j + 64]

    def to_owner(i):
        copies = [
            rcopy(fsend.at[i, lax.rem(y + d, ny)], fx.at[i, y], f_ss.at[i, d], f_rs.at[i, d], at_y(d))
            for d in range(1, ny)
        ]
        for copy in copies:
            copy.start()
        fx[i, pl.ds(y, 1)] = fsend[i, pl.ds(y, 1)]
        return copies

    fm_copies = to_owner(0)
    ring_recv(far, 0)
    ring_recv(far, 1)
    fill(5, -3)
    fill(6, 3)
    fill(7, far)
    attend(0, None, (5, 6, 7), False)
    po[pl.ds(me, 1)] = osend[pl.ds(0, 1)]
    loads[10].wait()
    for copy in fm_copies:
        copy.wait_recv()
    for j in range(ny):
        lhs_m[:, 128 * j : 128 * j + 128] = fx[0, j]
    mixed = dot(lhs_m[...], wm[...])
    o_copies = [rcopy(osend.at[d], po.at[me], o_ss.at[d], o_rs.at[d], at_row(d)) for d in range(1, nr)]
    for copy in o_copies:
        copy.wait_recv()
    heads = []
    for h in range(2):
        msgs = [po[2 * j + h].astype(F32) for j in range(nx)]
        lses = [(m[:, 0:1] + m[:, 1:2]) + m[:, 2:3] for m in msgs]
        joined = functools.reduce(jnp.maximum, lses)
        ws = [jnp.exp(v - joined) for v in lses]
        heads.append(sum(w * m for w, m in zip(ws, msgs)) / sum(ws))
    att = jnp.where(low, pltpu.roll(heads[0], 64, 1), heads[1]).astype(BF)
    for j in range(ny):
        fsend[1, j] = att[64 * j : 64 * j + 64]
    fa_copies = to_owner(1)
    loads[11].wait()
    for copy in fa_copies:
        copy.wait_recv()
    for j in range(ny):
        lhs_a[:, 128 * j : 128 * j + 128] = fx[1, j]
    out[...] = (mixed + dot(lhs_a[...], wa[...])).astype(BF)

    for copies in (e_direct, e_onward, n_direct, n_onward, [p_copy], q_copies, a_copies, b_copies, c_copies,
                   o_copies, fm_copies, fa_copies):
        for copy in copies:
            copy.wait_send()
    for copy in list(up.values()) + list(down.values()):
        copy.wait_send()


def body(nz, nx, ny, tokens, input_gain, memory_query, memory_key, memory_value, memory_outgate, memory_gates,
         gate_offset, memory_norm_gain, query_down, query_down_gain, latent_down, latent_gain, rotary_down,
         query_up, latent_up, query_gain, key_gain, memory_output, attention_output):
    args = (
        tokens, input_gain.reshape(1, D), memory_query, memory_key, memory_value, memory_outgate,
        jnp.transpose(memory_gates, (1, 2, 0)).reshape(32, D),
        jnp.transpose(gate_offset, (0, 2, 1)),
        memory_norm_gain.reshape(4, 128), query_down, query_down_gain.reshape(3, 128), latent_down,
        latent_gain.reshape(1, KVR), rotary_down.T,
        jnp.transpose(query_up, (1, 2, 0)).reshape(8 * (NOPE + ROPE), QR),
        latent_up.reshape(KVR * 8, 128), query_gain.reshape(1, 96), key_gain.reshape(1, 96),
        memory_output, attention_output,
    )
    nr = nx * 2
    in_hbm = {2, 3, 4, 5, 6, 9, 11, 13, 14, 15, 18, 19}
    vmem = pl.BlockSpec(memory_space=pltpu.VMEM)
    hbm = pl.BlockSpec(memory_space=pl.ANY)
    dma = pltpu.SemaphoreType.DMA
    keys = nz * 512
    far = nz // 2 + 1
    scratch = [
        pltpu.VMEM((D, 128), BF), pltpu.VMEM((D, 128), BF), pltpu.VMEM((D, 128), BF), pltpu.VMEM((D, 128), BF),
        pltpu.VMEM((32, D), BF), pltpu.VMEM((D, QR), BF), pltpu.VMEM((D, KVR), BF), pltpu.VMEM((32, D), BF),
        pltpu.VMEM((768, QR), BF), pltpu.VMEM((KVR * 8, 128), BF), pltpu.VMEM((512, D), BF), pltpu.VMEM((512, D), BF),
        pltpu.VMEM((256, D), BF), pltpu.VMEM((2, 128, QR), BF), pltpu.VMEM((KVR * 8, 128), F32),
        pltpu.VMEM((2, BLOCK, 128), F32),
        pltpu.VMEM((ny, ROWS, D), BF), pltpu.VMEM((ny, ROWS, 768), BF),
        pltpu.VMEM((nz, 2, BLOCK + ROWS, 128), BF), pltpu.VMEM((BLOCK + ROWS, 128), BF),
        pltpu.VMEM((2, BLOCK, 128), BF), pltpu.VMEM((nr, BLOCK, 128), BF),
        pltpu.VMEM((nr, 2, 16, 128), F32), pltpu.VMEM((nr, 2, 16, 128), F32), pltpu.VMEM((2, 16, 128), F32),
        pltpu.VMEM((nz, 16, 128), F32), pltpu.VMEM((nr, 2, 16, 128), F32), pltpu.VMEM((nr, 2, 16, 128), F32),
        pltpu.VMEM((nr, BLOCK, 256), BF), pltpu.VMEM((keys, 256), BF), pltpu.VMEM((128, keys), BF),
        pltpu.VMEM((nr, 128, BLOCK), F32), pltpu.VMEM((nr, 8, BLOCK), F32),
        pltpu.VMEM((nr, BLOCK, 128), BF), pltpu.VMEM((nr, BLOCK, 128), BF),
        pltpu.VMEM((2, ny, ROWS, 128), BF), pltpu.VMEM((2, ny, ROWS, 128), BF),
        pltpu.VMEM((ROWS, 512), BF), pltpu.VMEM((ROWS, 512), BF),
        dma((12,)), dma((6,)), dma((6,)), dma((6,)), dma((6,)), dma, dma,
        dma((nr,)), dma((nr,)), dma((nr,)), dma((nr,)), dma((nz,)), dma((nz,)), dma((nr,)), dma((nr,)),
        dma((far, 2)), dma((far, 2)), dma((far, 2)), dma((far, 2)),
        dma((nr,)), dma((nr,)), dma((2, ny)), dma((2, ny)),
    ]
    return pl.pallas_call(
        functools.partial(kernel, nz, nx, ny),
        out_shape=jax.ShapeDtypeStruct((ROWS, D), BF),
        in_specs=[hbm if i in in_hbm else vmem for i in range(len(args))],
        out_specs=vmem,
        scratch_shapes=scratch,
        compiler_params=pltpu.CompilerParams(
            collective_id=0, has_side_effects=True, vmem_limit_bytes=60 * 1024 * 1024
        ),
        name="mixer",
    )(*args)


def solution(mesh):
    ny = mesh.shape["tp"]
    nz, nx = 8, 4
    split = Mesh(mesh.devices.reshape(nz, nx, 2, ny), ("sp_0", "sp_1", "sp_2", "tp"))
    rep = P()
    head = P(None, "tp")
    in_specs = (
        P(SP_TP, None), rep, head, head, head, head, rep, P(None, SP, "tp"),
        rep, rep, rep, rep, rep, rep, rep, rep, rep, rep, rep, rep,
    )
    return jax.shard_map(
        functools.partial(body, nz, nx, ny), mesh=split, in_specs=in_specs, out_specs=P(SP_TP, None), check_vma=False
    )
```

```python
import functools

import jax
import jax.numpy as jnp
from jax import lax
from jax.experimental import pallas as pl
from jax.experimental.pallas import tpu as pltpu
from jax.sharding import Mesh
from jax.sharding import PartitionSpec as P

D = 2048
NOPE = 64
ROPE = 32
ROWS = 64
BLOCK = 256
QR = 384
KVR = 256
SP = ("sp_0", "sp_1", "sp_2")
SP_TP = ("sp_0", "sp_1", "sp_2", "tp")
EPSILON = 1e-06
ROPE_BASE = 10000.0
FLOOR_LOG = -1e30
BF = jnp.bfloat16
F32 = jnp.float32
MESH = pl.DeviceIdType.MESH
HI = lax.Precision.HIGHEST
FREQUENCIES = [float(ROPE_BASE ** (-j / 16)) for j in range(16)]


def dot(a, b, precision=None):
    return lax.dot_general(a, b, (((1,), (0,)), ((), ())), precision=precision, preferred_element_type=F32)


def dot_nt(a, b, precision=None):
    return lax.dot_general(a, b, (((1,), (1,)), ((), ())), precision=precision, preferred_element_type=F32)


def lanes(shape):
    return lax.broadcasted_iota(jnp.int32, shape, len(shape) - 1)


def rcopy(src, dst, send_sem, recv_sem, device):
    return pltpu.make_async_remote_copy(
        src_ref=src, dst_ref=dst, send_sem=send_sem, recv_sem=recv_sem, device_id=device, device_id_type=MESH
    )


def rms(v):
    return v * lax.rsqrt(jnp.mean(v * v, axis=-1, keepdims=True) + EPSILON)


def kernel(
    nz, nx, ny,
    tok, gain, hmq, hmk, hmv, hmo, hgt, goff, mng, hqd, qdg, hld, lg, hrt, hqt, hlup,
    qgain, kgain, hwm, hwa,
    out,
    mq, mk, mv, mo, gt, qd, ld, rt, qt, lup, wm, wa,
    rt4, wqt, lupf, trig, normed, ebuf, kvg, psend, qsend, qg, asend, agot, rtot, pb, csend, cgot,
    memp, memg, qop, kop, vt, acc_s, top_s, osend, po, fsend, fx, lhs_m, lhs_a,
    w_sem, n_ss, n_rs, e_ss, e_rs, p_ss, p_rs, q_ss, q_rs, a_ss, a_rs, b_ss, b_rs, c_ss, c_rs,
    u_ss, u_rs, d_ss, d_rs, o_ss, o_rs, f_ss, f_rs,
):
    z = lax.axis_index("sp_0")
    x = lax.axis_index("sp_1")
    c = lax.axis_index("sp_2")
    y = lax.axis_index("tp")
    nr = nx * 2
    me = x * 2 + c

    def at_y(d):
        return {"tp": lax.rem(y + d, ny)}

    def at_row(d):
        j = lax.rem(me + d, nr)
        return {"sp_1": j // 2, "sp_2": lax.rem(j, 2)}

    def at_z(d):
        return {"sp_0": lax.rem(z + d, nz)}

    pairs = ((hqd, qd), (hld, ld), (hrt, rt), (hlup, lup), (hqt, qt), (hmq, mq), (hmk, mk), (hmv, mv),
             (hgt, gt), (hmo, mo), (hwm, wm), (hwa, wa))
    loads = [pltpu.make_async_copy(a, b, w_sem.at[i]) for i, (a, b) in enumerate(pairs)]
    for load in loads:
        load.start()
    barrier = pltpu.get_barrier_semaphore()
    peers = [at_y(d) for d in range(1, ny)] + [at_row(d) for d in range(1, nr)] + [at_z(d) for d in range(1, nz)]
    for peer in peers:
        pl.semaphore_signal(barrier, inc=1, device_id=peer, device_id_type=MESH)

    xt = tok[...].astype(F32)
    normed_local = (rms(xt) * gain[...]).astype(BF)
    normed[pl.ds(y, 1)] = normed_local[None]

    segment = (z * nx + x) * 2 + c
    places = (segment * BLOCK + lax.broadcasted_iota(jnp.int32, (16, BLOCK), 1)).astype(F32)
    line = lax.broadcasted_iota(jnp.int32, (16, BLOCK), 0)
    frequency = jnp.zeros((16, BLOCK), F32)
    for j in range(16):
        frequency = jnp.where(line == j, FREQUENCIES[j], frequency)
    angles = places * frequency
    trig[0] = jnp.transpose(jnp.concatenate([jnp.cos(angles)] * 8, axis=0))
    trig[1] = jnp.transpose(jnp.concatenate([jnp.sin(angles)] * 8, axis=0))

    src = lax.broadcasted_iota(jnp.int32, (96, 128), 0)
    dst = lax.broadcasted_iota(jnp.int32, (96, 128), 1)
    rope_own, rope_swap = 64 + lax.rem(dst, 32), 64 + lax.rem(dst + 16, 32)
    q8 = jnp.broadcast_to(qgain[...], (8, 96))
    k8 = jnp.broadcast_to(kgain[...], (8, 96))
    scale = (NOPE + ROPE) ** (-0.5)
    q_own = dot(q8, (src == dst).astype(F32), HI)[0:1] * scale
    q_swap = dot(q8, (src == rope_swap).astype(F32), HI)[0:1] * scale
    k_own = dot(k8, (src == rope_own).astype(F32), HI)[0:1]
    k_swap = dot(k8, (src == rope_swap).astype(F32), HI)[0:1]
    k_plain = dot(k8, (src == dst).astype(F32), HI)[0:1]
    lane1 = lanes((1, 128))
    sign = jnp.where(lax.rem(lane1, 32) < 16, -1.0, 1.0)
    in_rope = jnp.logical_and(lane1 >= 64, lane1 < 96)

    loads[0].wait()
    loads[1].wait()
    qdg_row = jnp.concatenate([qdg[i : i + 1, :] for i in range(3)], axis=1)
    ql = (rms(dot(normed_local, qd[...])) * qdg_row).astype(BF)
    la = (rms(dot(normed_local, ld[...])) * lg[...]).astype(BF)
    loads[2].wait()
    for i in range(4):
        rt4[pl.ds(32 * i, 32), :] = rt[...]
        rt4[pl.ds(128 + 32 * i, 16), :] = rt[pl.ds(16, 16), :]
        rt4[pl.ds(128 + 32 * i + 16, 16), :] = rt[pl.ds(0, 16), :]
    ro = dot_nt(normed_local, rt4[...])
    ra, rb = ro[:, :128], ro[:, 128:]
    rscale = lax.rsqrt(jnp.mean(ra * ra, axis=-1, keepdims=True) + EPSILON)
    lane = lanes((ROWS, 128))
    own_rows = pl.ds(pl.multiple_of(y * ROWS, ROWS), ROWS)
    rot = (ra * rscale) * (trig[0, own_rows, :] * k_own) + (rb * rscale) * (trig[1, own_rows, :] * (k_swap * sign))
    rot = jnp.where(lane // ROPE == y, rot, 0.0).astype(BF)
    ebuf[pl.ds(y, 1), :, 0:256] = la[None]
    ebuf[pl.ds(y, 1), :, 256:384] = rot[None]
    ebuf[pl.ds(y, 1), :, 384:768] = ql[None]

    pl.semaphore_wait(barrier, len(peers))

    def spread_y(buf, ss, rs):
        lo, hi = pl.ds(0, ROWS // 2), pl.ds(ROWS // 2, ROWS // 2)
        below, above = lax.rem(y + ny - 1, ny), lax.rem(y + 1, ny)

        def one(i, slot, part, d):
            return rcopy(buf.at[slot, part], buf.at[slot, part], ss.at[i], rs.at[i], at_y(d))

        direct = [one(0, y, lo, 1), one(3, y, hi, ny - 1), one(1, y, hi, 1), one(4, y, lo, ny - 1)]
        onward = [one(2, below, lo, 1), one(5, above, hi, ny - 1)]
        return direct, onward

    e_direct, e_onward = spread_y(ebuf, e_ss, e_rs)
    n_direct, n_onward = spread_y(normed, n_ss, n_rs)
    for copy in e_direct:
        copy.start()
    for copy in n_direct[:2]:
        copy.start()
    loads[3].wait()
    lupf[...] = lup[...].astype(F32)
    loads[4].wait()
    for h in range(2):
        base = 96 * (2 * y + h)
        wqt[h, pl.ds(0, 96), :] = qt[pl.ds(pl.multiple_of(base, 32), 96), :]
        wqt[h, pl.ds(96, 16), :] = qt[pl.ds(pl.multiple_of(base + 80, 16), 16), :]
        wqt[h, pl.ds(112, 16), :] = qt[pl.ds(pl.multiple_of(base + 64, 16), 16), :]
    for i in range(2):
        e_direct[i].wait_recv()
        e_onward[i].start()
    for copy in n_direct[2:]:
        copy.start()
    e_direct[2].wait_recv()
    e_direct[3].wait_recv()
    for copy in e_onward:
        copy.wait_recv()

    lane2 = lanes((BLOCK, 128))
    low = lane2 < 64
    la_all = ebuf[:, :, 0:256].reshape(BLOCK, KVR)
    kv = []
    for h in range(2):
        w = lupf[pl.ds(2 * y + h, KVR, stride=8), :].astype(BF)
        t = dot(la_all, w)
        mp = jnp.sum(jnp.where(low, t * t, 0.0), axis=-1, keepdims=True) * (1.0 / NOPE)
        kv.append((t * jnp.where(low, lax.rsqrt(mp + EPSILON) * k_plain, 1.0)).astype(BF))
    rsum = (
        (ebuf[0, :, 256:384].astype(F32) + ebuf[1, :, 256:384].astype(F32))
        + (ebuf[2, :, 256:384].astype(F32) + ebuf[3, :, 256:384].astype(F32))
    ).astype(BF)
    first = c == 0
    kvg[pl.ds(z, 1), 0, pl.ds(0, BLOCK), :] = jnp.where(first, kv[0], kv[1])[None]
    kvg[pl.ds(z, 1), 0, pl.ds(BLOCK, ROWS), :] = rsum[None]
    psend[pl.ds(0, BLOCK), :] = jnp.where(first, kv[1], kv[0])
    psend[pl.ds(BLOCK, ROWS), :] = rsum
    p_copy = rcopy(psend, kvg.at[z, 1], p_ss, p_rs, {"sp_2": 1 - c})
    p_copy.start()

    up, down = {}, {}
    far = nz // 2

    def ring_send(s, r):
        if s < far or r == 0:
            k = lax.rem(z - (s - 1) + nz, nz)
            up[s, r] = rcopy(kvg.at[k, r], kvg.at[k, r], u_ss.at[s, r], u_rs.at[s, r], at_z(1))
            up[s, r].start()
        if s < far or r == 1:
            k = lax.rem(z + (s - 1), nz)
            down[s, r] = rcopy(kvg.at[k, r], kvg.at[k, r], d_ss.at[s, r], d_rs.at[s, r], at_z(nz - 1))
            down[s, r].start()

    def ring_recv(s, r):
        for way in (up, down):
            if (s, r) in way:
                way[s, r].wait_recv()
        if s < far:
            ring_send(s + 1, r)

    ring_send(1, 0)
    ql_all = ebuf[:, :, 384:768].reshape(BLOCK, QR)
    cos_q = trig[0] * jnp.where(in_rope, q_own, 0.0) + jnp.where(lane1 < 64, q_own, 0.0)
    sin_q = trig[1] * jnp.where(in_rope, q_swap * sign, 0.0)
    for h in range(2):
        q = dot_nt(ql_all, wqt[h])
        q2 = q * q
        mp = jnp.sum(jnp.where(low, q2, 0.0), axis=-1, keepdims=True) * (1.0 / NOPE)
        mr = jnp.sum(jnp.where(lane2 >= 96, q2, 0.0), axis=-1, keepdims=True) * (1.0 / ROPE)
        qn = q * jnp.where(low, lax.rsqrt(mp + EPSILON), lax.rsqrt(mr + EPSILON))
        qsend[h] = (qn * cos_q + pltpu.roll(qn, 96, 1) * sin_q).astype(BF)
    def row_copy(src, dst, ss, rs, i, t):
        device = {"sp_1": lax.rem(x + i + 1, nx), "sp_2": lax.rem(c + t, 2)}
        return rcopy(src, dst, ss.at[2 * i + t], rs.at[2 * i + t], device)

    q_copies = {}
    for i in (nx - 1, 0, nx - 2, 1):
        for t in range(2):
            if i < nx - 1 or t == 1:
                q_copies[i, t] = row_copy(qsend.at[lax.rem(c + t, 2)], qg.at[me], q_ss, q_rs, i, t)
                q_copies[i, t].start()
    qg[pl.ds(me, 1)] = qsend[pl.ds(c, 1)]
    p_copy.wait_recv()
    ring_send(1, 1)

    def fill(slot, d):
        k = lax.rem(z + d + nz, nz)
        for r in range(2):
            base = slot * 512 + r * 256
            kvs = kvg[k, r, pl.ds(0, BLOCK), :]
            kop[pl.ds(base, BLOCK), 0:128] = kvs
            vt[pl.ds(base, BLOCK), :] = jnp.where(low, jnp.ones_like(kvs), kvs)
            rr = kvg[k, r, pl.ds(BLOCK, ROWS), :]
            for j in range(4):
                kop[pl.ds(base + 64 * j, ROWS), 128:256] = jnp.where(lane // ROPE == j, rr, jnp.zeros_like(rr))

    fill(0, 0)
    for i in range(5, 9):
        loads[i].wait()
    loads[9].wait()

    def project(slot):
        part = normed[slot]
        at = pl.ds(pl.multiple_of(slot * ROWS, ROWS), ROWS)
        memp[0, at, :] = dot(part, mq[...]).astype(BF)
        memp[1, at, :] = (dot(part, mk[...]) * 0.125).astype(BF)
        memp[2, at, :] = dot(part, mv[...]).astype(BF)
        memp[3, at, :] = dot(part, mo[...]).astype(BF)
        memg[at, :] = dot_nt(part, gt[...]).astype(BF)

    for i in range(2):
        n_direct[i].wait_recv()
        n_onward[i].start()
    project(y)
    n_direct[2].wait_recv()
    n_direct[3].wait_recv()
    project(lax.rem(y + 1, ny))
    project(lax.rem(y + ny - 1, ny))
    ring_recv(1, 0)
    for copy in n_onward:
        copy.wait_recv()
    project(lax.rem(y + 2, ny))
    mem_q, mem_k, mem_v = memp[0], memp[1], memp[2]
    ring_recv(1, 1)
    row8 = lax.broadcasted_iota(jnp.int32, (8, 32), 0)
    col8 = lax.broadcasted_iota(jnp.int32, (8, 32), 1)
    pick = (col8 == (row8 // 2) * 8 + y * 2 + lax.rem(row8, 2)).astype(BF)
    pre = dot_nt(pick, memg[...]) + jnp.concatenate([goff[i] for i in range(4)], axis=0)
    low_t = lax.broadcasted_iota(jnp.int32, (128, BLOCK), 0) < 64

    def spread(r0, r1):
        wide = jnp.where(low_t, jnp.broadcast_to(r0, (128, BLOCK)), jnp.broadcast_to(r1, (128, BLOCK)))
        return jnp.transpose(wide)

    log_f = jnp.minimum(pre, 0.0) - jnp.log1p(jnp.exp(-jnp.abs(pre)))
    ti = lax.broadcasted_iota(jnp.int32, (BLOCK, BLOCK), 0)
    si = lax.broadcasted_iota(jnp.int32, (BLOCK, BLOCK), 1)
    masks = (si <= ti, si >= ti)
    zero = jnp.zeros_like(mem_q)
    s_heads = (dot_nt(jnp.where(low, mem_q, zero), mem_k), dot_nt(jnp.where(low, zero, mem_q), mem_k))
    v_f = mem_v.astype(F32)
    k_f = mem_k.astype(F32)
    q_f = mem_q.astype(F32)
    parts = []
    for way in range(2):
        i_wide = spread(pre[4 * way : 4 * way + 1], pre[4 * way + 1 : 4 * way + 2])
        f_wide = spread(log_f[4 * way + 2 : 4 * way + 3], log_f[4 * way + 3 : 4 * way + 4])
        cum = dot(masks[way].astype(F32), f_wide, HI)
        g = i_wide - cum
        g_t = jnp.transpose(g)
        total = jnp.sum(f_wide, axis=0, keepdims=True)
        growth = total + g
        level = jnp.max(growth, axis=0, keepdims=True)
        inflow = jnp.exp(growth - level)
        mat = lax.dot_general(
            inflow * v_f, k_f, (((0,), (0,)), ((), ())), precision=HI, preferred_element_type=F32
        )
        fold = jnp.where(lanes((64, 128)) < 64, mat[:64], mat[64:])
        normal = jnp.sum(inflow * k_f, axis=0, keepdims=True)
        vecs = jnp.concatenate([normal, level, total, jnp.zeros((5, 128), F32)], axis=0)
        for j in range(nr):
            asend[j, way, pl.ds(0, 8), :] = fold[8 * j : 8 * j + 8]
            asend[j, way, pl.ds(8, 8), :] = vecs
        parts.append((cum, g_t))
    a_copies = [
        rcopy(asend.at[lax.rem(me + d, nr)], agot.at[me], a_ss.at[d], a_rs.at[d], at_row(d)) for d in range(1, nr)
    ]
    for copy in a_copies:
        copy.start()
    agot[pl.ds(me, 1)] = asend[pl.ds(me, 1)]
    ring_recv(2, 0)
    own_parts = []
    for way in range(2):
        cum, g_t = parts[way]
        nums, dens, tops = [], [], []
        for h in range(2):
            decay = cum[:, 64 * h : 64 * h + 1] + g_t[64 * h : 64 * h + 1, :]
            decay = jnp.where(masks[way], decay, -jnp.inf)
            top = jnp.max(decay, axis=-1, keepdims=True)
            w = s_heads[h] * jnp.exp(decay - top)
            dens.append(jnp.sum(w, axis=-1, keepdims=True))
            nums.append(dot(w.astype(BF), mem_v))
            tops.append(top)
        own_parts.append((
            jnp.where(low, nums[0], nums[1]), jnp.where(low, dens[0], dens[1]), jnp.where(low, tops[0], tops[1]), cum
        ))
    ring_recv(2, 1)
    out_gate = jax.nn.sigmoid(memp[3].astype(F32))
    fill(1, -1)
    fill(2, 1)

    def chain(early, late):
        joined = jnp.maximum(late[10:11] + early[1], late[9:10])
        scale_e = jnp.exp(late[10:11] + early[1] - joined)
        scale_l = jnp.exp(late[9:10] - joined)
        return (scale_e * early[0] + scale_l * late, joined, early[2] + late[10:11])

    blank = (jnp.zeros((16, 128), F32), jnp.full((1, 128), FLOOR_LOG, F32), jnp.zeros((1, 128), F32))

    def packed(state):
        mat, level, total = state
        line = lax.broadcasted_iota(jnp.int32, (16, 128), 0)
        return jnp.where(line == 9, level, jnp.where(line == 10, total, mat))

    row_orders = (list(range(nr)), list(reversed(range(nr))))
    z_orders = (list(range(nz)), list(reversed(range(nz))))

    tile_r = lax.broadcasted_iota(jnp.int32, (128, 128), 0)
    tile_c = lax.broadcasted_iota(jnp.int32, (128, 128), 1)
    tile_m = (tile_r == 64 + lax.rem(tile_c, 32)).astype(BF)

    def take_queries(i):
        xx = lax.rem(x + i + 1, nx)
        back = (2 * nx - i - 2) % nx
        for t in range(2):
            if (back, t) in q_copies:
                q_copies[back, t].wait_recv()
        for t in range(2):
            slab = qg[2 * xx + t]
            qop[2 * xx + t, :, 0:128] = jnp.where(low, slab, jnp.zeros_like(slab))
            qop[2 * xx + t, :, 128:256] = dot(slab, tile_m).astype(BF)

    take_queries(nx - 1)
    take_queries(0)

    def o_copy(i, t):
        return row_copy(osend.at[2 * i + t], po.at[me], o_ss, o_rs, i, t)

    def attend(begin, end, slots, start=False, last=False):
        def block(n, carry):
            i = lax.rem(n + nx - 1, nx) if start else n
            xx = lax.rem(x + i + 1, nx)
            cores = [lax.rem(c + t, 2) for t in range(2)]
            qv = jnp.concatenate([qop[2 * xx + cores[t]] for t in range(2)], axis=0)
            if start:
                top = jnp.full((2 * BLOCK, 128), FLOOR_LOG, F32)
                acc = jnp.zeros((2 * BLOCK, 128), F32)
            else:
                top = top_s[i]
                acc = acc_s[i]
            score = dot_nt(qv, kop[pl.ds(slots[0] * 512, 512), :])
            for k in slots:
                after = dot_nt(qv, kop[pl.ds((k + 1) * 512, 512), :]) if k != slots[-1] else None
                new = jnp.maximum(top, jnp.max(score, axis=-1, keepdims=True))
                p = jnp.exp(score - jnp.concatenate([new] * 4, axis=1)).astype(BF)
                acc = acc * jnp.exp(top - new) + dot(p, vt[pl.ds(k * 512, 512), :])
                top = new
                score = after
            if not last:
                top_s[i] = top
                acc_s[i] = acc
                return carry
            at = lanes((2 * BLOCK, 128))
            den = acc[:, 0:1]
            lse = top + jnp.log(den)
            hi = lse.astype(BF).astype(F32)
            mid = (lse - hi).astype(BF).astype(F32)
            lo = (lse - hi) - mid
            msg = jnp.where(at == 0, hi, jnp.where(at == 1, mid, jnp.where(at == 2, lo, acc / den))).astype(BF)
            for t in range(2):
                d = 2 * i + t
                osend[pl.ds(d, 1)] = msg[BLOCK * t : BLOCK * t + BLOCK][None]

                @pl.when(jnp.logical_or(i < nx - 1, t == 1))
                def _():
                    o_copy(i, t).start()

            return carry

        lax.fori_loop(begin, end, block, 0)

    half = nr // 4
    attend(0, half, (0, 1, 2), start=True)
    ring_recv(3, 0)
    for copy in a_copies:
        copy.wait_recv()
    for way in range(2):
        state = blank
        for j in row_orders[way]:
            state = chain(state, agot[j, way])
        rtot[way] = packed(state)
    b_copies = []
    for d in range(1, nz):
        copy = rcopy(rtot.at[(z + d) // nz], pb.at[z], b_ss.at[d], b_rs.at[d], at_z(d))
        copy.start()
        b_copies.append(copy)
    pb[pl.ds(z, 1)] = jnp.zeros((1, 16, 128), F32)
    take_queries(1)
    take_queries(2)
    attend(half, 2 * half, (0, 1, 2), start=True)
    ring_recv(3, 1)
    fill(3, -2)
    fill(4, 2)
    attend(0, half, (3, 4))
    attend(half, 2 * half, (3, 4))
    for copy in b_copies:
        copy.wait_recv()
    for way in range(2):
        state = blank
        for j in z_orders[way]:
            ok = (j < z) if way == 0 else (j > z)
            new = chain(state, pb[j])
            state = tuple(jnp.where(ok, a, b) for a, b in zip(new, state))
        for j in row_orders[way]:
            csend[j, way] = packed(state)
            state = chain(state, agot[j, way])
    c_copies = [
        rcopy(csend.at[lax.rem(me + d, nr)], cgot.at[me], c_ss.at[d], c_rs.at[d], at_row(d)) for d in range(1, nr)
    ]
    for copy in c_copies:
        copy.start()
    cgot[pl.ds(me, 1)] = csend[pl.ds(me, 1)]
    fill(5, -3)
    fill(6, 3)
    ring_recv(far, 0)
    ring_recv(far, 1)
    fill(7, far)
    attend(0, 2 * half, (5, 6, 7), last=True)
    po[pl.ds(me, 1)] = osend[pl.ds(nr - 2, 1)]
    for copy in c_copies:
        copy.wait_recv()
    hsum = jnp.zeros((BLOCK, 128), F32)
    bi = lax.broadcasted_iota(jnp.int32, (128, 128), 0) // 64
    bj = lax.broadcasted_iota(jnp.int32, (128, 128), 1) // 64
    ones_block = (bi == bj).astype(F32)
    low64 = lanes((64, 128)) < 64
    for way in range(2):
        fold = jnp.concatenate([cgot[j, way, pl.ds(0, 8), :] for j in range(nr)], axis=0)
        normal = cgot[0, way, pl.ds(8, 1), :]
        level = cgot[0, way, pl.ds(9, 1), :]
        full = jnp.concatenate([jnp.where(low64, fold, 0.0), jnp.where(low64, 0.0, fold)], axis=0)
        num, den, top, cum = own_parts[way]
        carried_log = cum + level
        joined = jnp.maximum(top, carried_log)
        own = jnp.exp(top - joined)
        carried = jnp.exp(carried_log - joined)
        num = num * own + carried * dot_nt(q_f, full, HI)
        den = den * own + carried * dot(q_f * normal, ones_block, HI)
        hsum = hsum + num / jnp.maximum(jnp.abs(den), jnp.exp(-joined))
    mean = dot(hsum * hsum, ones_block, HI) * (1.0 / 64)
    combined = hsum * lax.rsqrt(mean + EPSILON) * mng[pl.ds(y, 1), :]
    mem_rows = (combined * out_gate).astype(BF)
    for j in range(ny):
        fsend[0, j] = mem_rows[64 * j : 64 * j + 64]

    def to_owner(i):
        copies = [
            rcopy(fsend.at[i, lax.rem(y + d, ny)], fx.at[i, y], f_ss.at[i, d], f_rs.at[i, d], at_y(d))
            for d in range(1, ny)
        ]
        for copy in copies:
            copy.start()
        fx[i, pl.ds(y, 1)] = fsend[i, pl.ds(y, 1)]
        return copies

    fm_copies = to_owner(0)
    o_copies = [o_copy(i, t) for i in range(nx) for t in range(2) if i < nx - 1 or t == 1]
    for copy in o_copies:
        copy.wait_recv()
    heads = []
    for h in range(2):
        msgs = [po[2 * j + h].astype(F32) for j in range(nx)]
        lses = [(m[:, 0:1] + m[:, 1:2]) + m[:, 2:3] for m in msgs]
        joined = functools.reduce(jnp.maximum, lses)
        ws = [jnp.exp(v - joined) for v in lses]
        heads.append(sum(w * m for w, m in zip(ws, msgs)) / sum(ws))
    att = jnp.where(low, pltpu.roll(heads[0], 64, 1), heads[1]).astype(BF)
    for j in range(ny):
        fsend[1, j] = att[64 * j : 64 * j + 64]
    fa_copies = to_owner(1)
    loads[10].wait()
    for copy in fm_copies:
        copy.wait_recv()
    for j in range(ny):
        lhs_m[:, 128 * j : 128 * j + 128] = fx[0, j]
    mixed = dot(lhs_m[...], wm[...])
    loads[11].wait()
    for copy in fa_copies:
        copy.wait_recv()
    for j in range(ny):
        lhs_a[:, 128 * j : 128 * j + 128] = fx[1, j]
    out[...] = (mixed + dot(lhs_a[...], wa[...])).astype(BF)

    for copies in (e_direct, e_onward, n_direct, n_onward, [p_copy], q_copies.values(), a_copies, b_copies, c_copies,
                   o_copies, fm_copies, fa_copies):
        for copy in copies:
            copy.wait_send()
    for copy in list(up.values()) + list(down.values()):
        copy.wait_send()


def body(nz, nx, ny, tokens, input_gain, memory_query, memory_key, memory_value, memory_outgate, memory_gates,
         gate_offset, memory_norm_gain, query_down, query_down_gain, latent_down, latent_gain, rotary_down,
         query_up, latent_up, query_gain, key_gain, memory_output, attention_output):
    args = (
        tokens, input_gain.reshape(1, D), memory_query, memory_key, memory_value, memory_outgate,
        jnp.transpose(memory_gates, (1, 2, 0)).reshape(32, D),
        jnp.transpose(gate_offset, (0, 2, 1)),
        memory_norm_gain.reshape(4, 128), query_down, query_down_gain.reshape(3, 128), latent_down,
        latent_gain.reshape(1, KVR), rotary_down.T,
        jnp.transpose(query_up, (1, 2, 0)).reshape(8 * (NOPE + ROPE), QR),
        latent_up.reshape(KVR * 8, 128), query_gain.reshape(1, 96), key_gain.reshape(1, 96),
        memory_output, attention_output,
    )
    nr = nx * 2
    in_hbm = {2, 3, 4, 5, 6, 9, 11, 13, 14, 15, 18, 19}
    vmem = pl.BlockSpec(memory_space=pltpu.VMEM)
    hbm = pl.BlockSpec(memory_space=pltpu.HBM)
    dma = pltpu.SemaphoreType.DMA
    keys = nz * 512
    far = nz // 2 + 1
    scratch = [
        pltpu.VMEM((D, 128), BF), pltpu.VMEM((D, 128), BF), pltpu.VMEM((D, 128), BF), pltpu.VMEM((D, 128), BF),
        pltpu.VMEM((32, D), BF), pltpu.VMEM((D, QR), BF), pltpu.VMEM((D, KVR), BF), pltpu.VMEM((32, D), BF),
        pltpu.VMEM((768, QR), BF), pltpu.VMEM((KVR * 8, 128), BF), pltpu.VMEM((512, D), BF), pltpu.VMEM((512, D), BF),
        pltpu.VMEM((256, D), BF), pltpu.VMEM((2, 128, QR), BF), pltpu.VMEM((KVR * 8, 128), F32),
        pltpu.VMEM((2, BLOCK, 128), F32),
        pltpu.VMEM((ny, ROWS, D), BF), pltpu.VMEM((ny, ROWS, 768), BF),
        pltpu.VMEM((nz, 2, BLOCK + ROWS, 128), BF), pltpu.VMEM((BLOCK + ROWS, 128), BF),
        pltpu.VMEM((2, BLOCK, 128), BF), pltpu.VMEM((nr, BLOCK, 128), BF),
        pltpu.VMEM((nr, 2, 16, 128), F32), pltpu.VMEM((nr, 2, 16, 128), F32), pltpu.VMEM((2, 16, 128), F32),
        pltpu.VMEM((nz, 16, 128), F32), pltpu.VMEM((nr, 2, 16, 128), F32), pltpu.VMEM((nr, 2, 16, 128), F32),
        pltpu.VMEM((4, BLOCK, 128), BF), pltpu.VMEM((BLOCK, 32), BF),
        pltpu.VMEM((nr, BLOCK, 256), BF), pltpu.VMEM((keys, 256), BF), pltpu.VMEM((keys, 128), BF),
        pltpu.VMEM((nr // 2, 2 * BLOCK, 128), F32), pltpu.VMEM((nr // 2, 2 * BLOCK, 128), F32),
        pltpu.VMEM((nr, BLOCK, 128), BF), pltpu.VMEM((nr, BLOCK, 128), BF),
        pltpu.VMEM((2, ny, ROWS, 128), BF), pltpu.VMEM((2, ny, ROWS, 128), BF),
        pltpu.VMEM((ROWS, 512), BF), pltpu.VMEM((ROWS, 512), BF),
        dma((12,)), dma((6,)), dma((6,)), dma((6,)), dma((6,)), dma, dma,
        dma((nr,)), dma((nr,)), dma((nr,)), dma((nr,)), dma((nz,)), dma((nz,)), dma((nr,)), dma((nr,)),
        dma((far, 2)), dma((far, 2)), dma((far, 2)), dma((far, 2)),
        dma((nr,)), dma((nr,)), dma((2, ny)), dma((2, ny)),
    ]
    return pl.pallas_call(
        functools.partial(kernel, nz, nx, ny),
        out_shape=jax.ShapeDtypeStruct((ROWS, D), BF),
        in_specs=[hbm if i in in_hbm else vmem for i in range(len(args))],
        out_specs=vmem,
        scratch_shapes=scratch,
        compiler_params=pltpu.CompilerParams(
            collective_id=0, has_side_effects=True, vmem_limit_bytes=60 * 1024 * 1024
        ),
        name="mixer",
    )(*args)


def solution(mesh):
    ny = mesh.shape["tp"]
    nz, nx = 8, 4
    split = Mesh(mesh.devices.reshape(nz, nx, 2, ny), ("sp_0", "sp_1", "sp_2", "tp"))
    rep = P()
    head = P(None, "tp")
    in_specs = (
        P(SP_TP, None), rep, head, head, head, head, rep, P(None, SP, "tp"),
        rep, rep, rep, rep, rep, rep, rep, rep, rep, rep, rep, rep,
    )
    return jax.shard_map(
        functools.partial(body, nz, nx, ny), mesh=split, in_specs=in_specs, out_specs=P(SP_TP, None), check_vma=False
    )
```

```python
import functools

import jax
import jax.numpy as jnp
from jax import lax
from jax.experimental import pallas as pl
from jax.experimental.pallas import tpu as pltpu
from jax.sharding import Mesh
from jax.sharding import PartitionSpec as P

D = 2048
NOPE = 64
ROPE = 32
ROWS = 64
BLOCK = 256
QR = 384
KVR = 256
SP = ("sp_0", "sp_1", "sp_2")
SP_TP = ("sp_0", "sp_1", "sp_2", "tp")
EPSILON = 1e-06
ROPE_BASE = 10000.0
FLOOR_LOG = -1e30
BF = jnp.bfloat16
F32 = jnp.float32
MESH = pl.DeviceIdType.MESH
HI = lax.Precision.HIGHEST
FREQUENCIES = [float(ROPE_BASE ** (-j / 16)) for j in range(16)]


def dot(a, b, precision=None):
    return lax.dot_general(a, b, (((1,), (0,)), ((), ())), precision=precision, preferred_element_type=F32)


def dot_nt(a, b, precision=None):
    return lax.dot_general(a, b, (((1,), (1,)), ((), ())), precision=precision, preferred_element_type=F32)


def pieces(v, n):
    found = []
    for _ in range(n):
        found.append(v.astype(BF))
        v = v - found[-1].astype(F32)
    return found


def lanes(shape):
    return lax.broadcasted_iota(jnp.int32, shape, len(shape) - 1)


def rcopy(src, dst, send_sem, recv_sem, device):
    return pltpu.make_async_remote_copy(
        src_ref=src, dst_ref=dst, send_sem=send_sem, recv_sem=recv_sem, device_id=device, device_id_type=MESH
    )


def rms(v):
    return v * lax.rsqrt(jnp.mean(v * v, axis=-1, keepdims=True) + EPSILON)


def kernel(
    nz, nx, ny,
    tok, gain, hmq, hmk, hmv, hmo, hgt, goff, mng, hqd, qdg, hld, lg, hrt, hqt, hlup,
    qgain, kgain, hwm, hwa,
    out,
    mq, mk, mv, mo, gt, qd, ld, rt, qt, lup, wm, wa,
    rt4, wqt, lupf, trig, normed, ebuf, kvg, psend, qsend, qg, asend, agot, rtot, pb, csend, cgot,
    memp, memg, qop, kop, vt, acc_s, top_s, osend, po, fsend, fx, lhs_m, lhs_a,
    w_sem, n_ss, n_rs, e_ss, e_rs, p_ss, p_rs, q_ss, q_rs, a_ss, a_rs, b_ss, b_rs, c_ss, c_rs,
    u_ss, u_rs, d_ss, d_rs, o_ss, o_rs, f_ss, f_rs,
):
    z = lax.axis_index("sp_0")
    x = lax.axis_index("sp_1")
    c = lax.axis_index("sp_2")
    y = lax.axis_index("tp")
    nr = nx * 2
    me = x * 2 + c

    def at_y(d):
        return {"tp": lax.rem(y + d, ny)}

    def at_row(d):
        j = lax.rem(me + d, nr)
        return {"sp_1": j // 2, "sp_2": lax.rem(j, 2)}

    def at_z(d):
        return {"sp_0": lax.rem(z + d, nz)}

    pairs = ((hqd, qd), (hld, ld), (hrt, rt), (hlup, lup), (hqt, qt), (hmq, mq), (hmk, mk), (hmv, mv),
             (hgt, gt), (hmo, mo), (hwm, wm), (hwa, wa))
    loads = [pltpu.make_async_copy(a, b, w_sem.at[i]) for i, (a, b) in enumerate(pairs)]
    for load in loads:
        load.start()
    barrier = pltpu.get_barrier_semaphore()
    peers = [at_y(d) for d in range(1, ny)] + [at_row(d) for d in range(1, nr)] + [at_z(d) for d in range(1, nz)]
    for peer in peers:
        pl.semaphore_signal(barrier, inc=1, device_id=peer, device_id_type=MESH)

    xt = tok[...].astype(F32)
    normed_local = (rms(xt) * gain[...]).astype(BF)
    normed[pl.ds(y, 1)] = normed_local[None]

    segment = (z * nx + x) * 2 + c
    places = (segment * BLOCK + lax.broadcasted_iota(jnp.int32, (16, BLOCK), 1)).astype(F32)
    line = lax.broadcasted_iota(jnp.int32, (16, BLOCK), 0)
    frequency = jnp.zeros((16, BLOCK), F32)
    for j in range(16):
        frequency = jnp.where(line == j, FREQUENCIES[j], frequency)
    angles = places * frequency
    trig[0] = jnp.transpose(jnp.concatenate([jnp.cos(angles)] * 8, axis=0))
    trig[1] = jnp.transpose(jnp.concatenate([jnp.sin(angles)] * 8, axis=0))

    src = lax.broadcasted_iota(jnp.int32, (96, 128), 0)
    dst = lax.broadcasted_iota(jnp.int32, (96, 128), 1)
    rope_own, rope_swap = 64 + lax.rem(dst, 32), 64 + lax.rem(dst + 16, 32)
    q8 = jnp.broadcast_to(qgain[...], (8, 96))
    k8 = jnp.broadcast_to(kgain[...], (8, 96))
    scale = (NOPE + ROPE) ** (-0.5)
    q_own = dot(q8, (src == dst).astype(F32), HI)[0:1] * scale
    q_swap = dot(q8, (src == rope_swap).astype(F32), HI)[0:1] * scale
    k_own = dot(k8, (src == rope_own).astype(F32), HI)[0:1]
    k_swap = dot(k8, (src == rope_swap).astype(F32), HI)[0:1]
    k_plain = dot(k8, (src == dst).astype(F32), HI)[0:1]
    lane1 = lanes((1, 128))
    sign = jnp.where(lax.rem(lane1, 32) < 16, -1.0, 1.0)
    in_rope = jnp.logical_and(lane1 >= 64, lane1 < 96)

    loads[0].wait()
    loads[1].wait()
    qdg_row = jnp.concatenate([qdg[i : i + 1, :] for i in range(3)], axis=1)
    ql = (rms(dot(normed_local, qd[...])) * qdg_row).astype(BF)
    la = (rms(dot(normed_local, ld[...])) * lg[...]).astype(BF)
    loads[2].wait()
    for i in range(4):
        rt4[pl.ds(32 * i, 32), :] = rt[...]
        rt4[pl.ds(128 + 32 * i, 16), :] = rt[pl.ds(16, 16), :]
        rt4[pl.ds(128 + 32 * i + 16, 16), :] = rt[pl.ds(0, 16), :]
    ro = dot_nt(normed_local, rt4[...])
    ra, rb = ro[:, :128], ro[:, 128:]
    rscale = lax.rsqrt(jnp.mean(ra * ra, axis=-1, keepdims=True) + EPSILON)
    lane = lanes((ROWS, 128))
    own_rows = pl.ds(pl.multiple_of(y * ROWS, ROWS), ROWS)
    rot = (ra * rscale) * (trig[0, own_rows, :] * k_own) + (rb * rscale) * (trig[1, own_rows, :] * (k_swap * sign))
    rot = jnp.where(lane // ROPE == y, rot, 0.0).astype(BF)
    ebuf[pl.ds(y, 1), :, 0:256] = la[None]
    ebuf[pl.ds(y, 1), :, 256:384] = rot[None]
    ebuf[pl.ds(y, 1), :, 384:768] = ql[None]

    pl.semaphore_wait(barrier, len(peers))

    def spread_y(buf, ss, rs):
        lo, hi = pl.ds(0, ROWS // 2), pl.ds(ROWS // 2, ROWS // 2)
        below, above = lax.rem(y + ny - 1, ny), lax.rem(y + 1, ny)

        def one(i, slot, part, d):
            return rcopy(buf.at[slot, part], buf.at[slot, part], ss.at[i], rs.at[i], at_y(d))

        direct = [one(0, y, lo, 1), one(3, y, hi, ny - 1), one(1, y, hi, 1), one(4, y, lo, ny - 1)]
        onward = [one(2, below, lo, 1), one(5, above, hi, ny - 1)]
        return direct, onward

    e_direct, e_onward = spread_y(ebuf, e_ss, e_rs)
    n_direct, n_onward = spread_y(normed, n_ss, n_rs)
    for copy in e_direct:
        copy.start()
    loads[3].wait()
    lupf[...] = lup[...].astype(F32)
    loads[4].wait()
    for h in range(2):
        base = 96 * (2 * y + h)
        wqt[h, pl.ds(0, 96), :] = qt[pl.ds(pl.multiple_of(base, 32), 96), :]
        wqt[h, pl.ds(96, 16), :] = qt[pl.ds(pl.multiple_of(base + 80, 16), 16), :]
        wqt[h, pl.ds(112, 16), :] = qt[pl.ds(pl.multiple_of(base + 64, 16), 16), :]
    for i in range(2):
        e_direct[i].wait_recv()
        e_onward[i].start()
    for copy in n_direct:
        copy.start()
    e_direct[2].wait_recv()
    e_direct[3].wait_recv()
    for copy in e_onward:
        copy.wait_recv()

    lane2 = lanes((BLOCK, 128))
    low = lane2 < 64
    la_all = ebuf[:, :, 0:256].reshape(BLOCK, KVR)
    kv = []
    for h in range(2):
        w = lupf[pl.ds(2 * y + h, KVR, stride=8), :].astype(BF)
        t = dot(la_all, w)
        mp = jnp.sum(jnp.where(low, t * t, 0.0), axis=-1, keepdims=True) * (1.0 / NOPE)
        kv.append((t * jnp.where(low, lax.rsqrt(mp + EPSILON) * k_plain, 1.0)).astype(BF))
    rsum = (
        (ebuf[0, :, 256:384].astype(F32) + ebuf[1, :, 256:384].astype(F32))
        + (ebuf[2, :, 256:384].astype(F32) + ebuf[3, :, 256:384].astype(F32))
    ).astype(BF)
    first = c == 0
    kvg[pl.ds(z, 1), 0, pl.ds(0, BLOCK), :] = jnp.where(first, kv[0], kv[1])[None]
    kvg[pl.ds(z, 1), 0, pl.ds(BLOCK, ROWS), :] = rsum[None]
    psend[pl.ds(0, BLOCK), :] = jnp.where(first, kv[1], kv[0])
    psend[pl.ds(BLOCK, ROWS), :] = rsum
    p_copy = rcopy(psend, kvg.at[z, 1], p_ss, p_rs, {"sp_2": 1 - c})
    p_copy.start()

    up, down = {}, {}
    far = nz // 2

    def ring_send(s, r):
        if s < far or r == 0:
            k = lax.rem(z - (s - 1) + nz, nz)
            up[s, r] = rcopy(kvg.at[k, r], kvg.at[k, r], u_ss.at[s, r], u_rs.at[s, r], at_z(1))
            up[s, r].start()
        if s < far or r == 1:
            k = lax.rem(z + (s - 1), nz)
            down[s, r] = rcopy(kvg.at[k, r], kvg.at[k, r], d_ss.at[s, r], d_rs.at[s, r], at_z(nz - 1))
            down[s, r].start()

    def ring_recv(s, r):
        for way in (up, down):
            if (s, r) in way:
                way[s, r].wait_recv()
        if s < far:
            ring_send(s + 1, r)

    ring_send(1, 0)
    ql_all = ebuf[:, :, 384:768].reshape(BLOCK, QR)
    cos_q = trig[0] * jnp.where(in_rope, q_own, 0.0) + jnp.where(lane1 < 64, q_own, 0.0)
    sin_q = trig[1] * jnp.where(in_rope, q_swap * sign, 0.0)
    for h in range(2):
        q = dot_nt(ql_all, wqt[h])
        q2 = q * q
        mp = jnp.sum(jnp.where(low, q2, 0.0), axis=-1, keepdims=True) * (1.0 / NOPE)
        mr = jnp.sum(jnp.where(lane2 >= 96, q2, 0.0), axis=-1, keepdims=True) * (1.0 / ROPE)
        qn = q * jnp.where(low, lax.rsqrt(mp + EPSILON), lax.rsqrt(mr + EPSILON))
        qsend[h] = (qn * cos_q + pltpu.roll(qn, 96, 1) * sin_q).astype(BF)
    def row_copy(src, dst, ss, rs, i, t):
        device = {"sp_1": lax.rem(x + i + 1, nx), "sp_2": lax.rem(c + t, 2)}
        return rcopy(src, dst, ss.at[2 * i + t], rs.at[2 * i + t], device)

    q_copies = {}
    for i in (nx - 1, 0, nx - 2, 1):
        for t in range(2):
            if i < nx - 1 or t == 1:
                q_copies[i, t] = row_copy(qsend.at[lax.rem(c + t, 2)], qg.at[me], q_ss, q_rs, i, t)
                q_copies[i, t].start()
    qg[pl.ds(me, 1)] = qsend[pl.ds(c, 1)]
    p_copy.wait_recv()
    ring_send(1, 1)

    def fill(slot, d):
        k = lax.rem(z + d + nz, nz)
        for r in range(2):
            base = slot * 512 + r * 256
            kvs = kvg[k, r, pl.ds(0, BLOCK), :]
            kop[pl.ds(base, BLOCK), 0:128] = kvs
            vt[pl.ds(base, BLOCK), :] = jnp.where(low, jnp.ones_like(kvs), kvs)
            rr = kvg[k, r, pl.ds(BLOCK, ROWS), :]
            for j in range(4):
                kop[pl.ds(base + 64 * j, ROWS), 128:256] = jnp.where(lane // ROPE == j, rr, jnp.zeros_like(rr))

    fill(0, 0)
    tile_r = lax.broadcasted_iota(jnp.int32, (128, 128), 0)
    tile_c = lax.broadcasted_iota(jnp.int32, (128, 128), 1)
    tile_m = (tile_r == 64 + lax.rem(tile_c, 32)).astype(BF)

    def take_queries(i):
        xx = lax.rem(x + i + 1, nx)
        back = (2 * nx - i - 2) % nx
        for t in range(2):
            if (back, t) in q_copies:
                q_copies[back, t].wait_recv()
        for t in range(2):
            slab = qg[2 * xx + t]
            qop[2 * xx + t, :, 0:128] = jnp.where(low, slab, jnp.zeros_like(slab))
            qop[2 * xx + t, :, 128:256] = dot(slab, tile_m).astype(BF)

    def o_copy(i, t):
        return row_copy(osend.at[2 * i + t], po.at[me], o_ss, o_rs, i, t)

    def attend(begin, end, slots, start=False, last=False):
        def block(n, carry):
            i = lax.rem(n + nx - 1, nx) if start else n
            xx = lax.rem(x + i + 1, nx)
            cores = [lax.rem(c + t, 2) for t in range(2)]
            qv = jnp.concatenate([qop[2 * xx + cores[t]] for t in range(2)], axis=0)
            if start:
                top = jnp.full((2 * BLOCK, 128), FLOOR_LOG, F32)
                acc = jnp.zeros((2 * BLOCK, 128), F32)
            else:
                top = top_s[i]
                acc = acc_s[i]
            score = dot_nt(qv, kop[pl.ds(slots[0] * 512, 512), :])
            for k in slots:
                after = dot_nt(qv, kop[pl.ds((k + 1) * 512, 512), :]) if k != slots[-1] else None
                new = jnp.maximum(top, jnp.max(score, axis=-1, keepdims=True))
                p = jnp.exp(score - jnp.concatenate([new] * 4, axis=1)).astype(BF)
                acc = acc * jnp.exp(top - new) + dot(p, vt[pl.ds(k * 512, 512), :])
                top = new
                score = after
            if not last:
                top_s[i] = top
                acc_s[i] = acc
                return carry
            den = acc[:, 0:1]
            lse = top + jnp.log(acc)
            share = acc / den
            low1 = lane2[:128] < 64
            for t in range(2):
                d = 2 * i + t
                a0, a1 = share[256 * t : 256 * t + 128], share[256 * t + 128 : 256 * t + 256]
                l0, l1 = lse[256 * t : 256 * t + 128], lse[256 * t + 128 : 256 * t + 256]
                osend[d, pl.ds(0, 128), :] = jnp.where(low1, pltpu.roll(a0, 64, 1), a1).astype(BF)
                rows_l = jnp.transpose(jnp.where(low1, l0, pltpu.roll(l1, 64, 1)))
                three = pieces(jnp.concatenate([rows_l[0:1], rows_l[64:65]], axis=0), 3)
                osend[d, pl.ds(128, 16), :] = jnp.concatenate(three + [jnp.zeros((10, 128), BF)], axis=0)

                @pl.when(jnp.logical_or(i < nx - 1, t == 1))
                def _():
                    o_copy(i, t).start()

            return carry

        lax.fori_loop(begin, end, block, 0)

    half = nr // 4
    for i in range(5, 9):
        loads[i].wait()
    loads[9].wait()

    def project(slot):
        part = normed[slot]
        at = pl.ds(pl.multiple_of(slot * ROWS, ROWS), ROWS)
        memp[0, at, :] = dot(part, mq[...]).astype(BF)
        memp[1, at, :] = (dot(part, mk[...]) * 0.125).astype(BF)
        memp[2, at, :] = dot(part, mv[...]).astype(BF)
        memp[3, at, :] = dot(part, mo[...]).astype(BF)
        memg[at, :] = dot_nt(part, gt[...]).astype(BF)

    for i in range(2):
        n_direct[i].wait_recv()
        n_onward[i].start()
    project(y)
    n_direct[2].wait_recv()
    n_direct[3].wait_recv()
    project(lax.rem(y + 1, ny))
    project(lax.rem(y + ny - 1, ny))
    ring_recv(1, 0)
    take_queries(nx - 1)
    ring_recv(1, 1)
    fill(1, -1)
    fill(2, 1)
    attend(0, 1, (0, 1, 2), start=True)
    for copy in n_onward:
        copy.wait_recv()
    project(lax.rem(y + 2, ny))
    mem_q, mem_k, mem_v = memp[0], memp[1], memp[2]
    row8 = lax.broadcasted_iota(jnp.int32, (8, 32), 0)
    col8 = lax.broadcasted_iota(jnp.int32, (8, 32), 1)
    pick = (col8 == (row8 // 2) * 8 + y * 2 + lax.rem(row8, 2)).astype(BF)
    pre = dot_nt(pick, memg[...]) + jnp.concatenate([goff[i] for i in range(4)], axis=0)
    low_t = lax.broadcasted_iota(jnp.int32, (128, BLOCK), 0) < 64

    def spread(r0, r1):
        wide = jnp.where(low_t, jnp.broadcast_to(r0, (128, BLOCK)), jnp.broadcast_to(r1, (128, BLOCK)))
        return jnp.transpose(wide)

    log_f = jnp.minimum(pre, 0.0) - jnp.log1p(jnp.exp(-jnp.abs(pre)))
    ti = lax.broadcasted_iota(jnp.int32, (BLOCK, BLOCK), 0)
    si = lax.broadcasted_iota(jnp.int32, (BLOCK, BLOCK), 1)
    masks = (si <= ti, si >= ti)
    log_3 = pieces(log_f, 3)
    zero = jnp.zeros_like(mem_q)
    v_f = mem_v.astype(F32)
    parts = []
    line16 = lax.broadcasted_iota(jnp.int32, (8, 128), 0)
    lane8 = lanes((8, 128))
    for way in range(2):
        ones = masks[1 - way].astype(BF)
        cums = (dot(log_3[0], ones) + dot(log_3[1], ones)) + dot(log_3[2], ones)
        cum = cums[4 * way + 2 : 4 * way + 4]
        g = pre[4 * way : 4 * way + 2] - cum
        last = BLOCK - 1 if way == 0 else 0
        total = cum[:, last : last + 1]
        growth = total + g
        level = jnp.max(growth, axis=-1, keepdims=True)
        inflow = jnp.exp(growth - level)
        wide = spread(inflow[0:1], inflow[1:2])
        vw = pieces(wide * v_f, 2)
        mat = sum(
            lax.dot_general(a, mem_k, (((0,), (0,)), ((), ())), preferred_element_type=F32) for a in vw
        )
        fold = jnp.where(lanes((64, 128)) < 64, mat[:64], mat[64:])
        inflow8 = jnp.concatenate([inflow, jnp.zeros((6, BLOCK), F32)], axis=0)
        sums = sum(dot(a, mem_k) for a in pieces(inflow8, 2))
        normal = jnp.where(lane1 < 64, sums[0:1], sums[1:2])

        def by_lane(v):
            return jnp.where(lane8 < 64, jnp.broadcast_to(v[0:1], (8, 128)), jnp.broadcast_to(v[1:2], (8, 128)))

        vecs = jnp.where(line16 == 0, normal, jnp.where(line16 == 1, by_lane(level), by_lane(total)))
        for j in range(nr):
            asend[j, way, pl.ds(0, 8), :] = fold[8 * j : 8 * j + 8]
            asend[j, way, pl.ds(8, 8), :] = vecs
        parts.append((cum, g))
    a_copies = [
        rcopy(asend.at[lax.rem(me + d, nr)], agot.at[me], a_ss.at[d], a_rs.at[d], at_row(d)) for d in range(1, nr)
    ]
    for copy in a_copies:
        copy.start()
    agot[pl.ds(me, 1)] = asend[pl.ds(me, 1)]
    ring_recv(2, 0)
    own_parts = []
    s_heads = (dot_nt(jnp.where(low, mem_q, zero), mem_k), dot_nt(jnp.where(low, zero, mem_q), mem_k))
    for way in range(2):
        cum, g_t = parts[way]
        cum = spread(cum[0:1], cum[1:2])
        nums, dens, tops = [], [], []
        for h in range(2):
            decay = cum[:, 64 * h : 64 * h + 1] + g_t[h : h + 1, :]
            decay = jnp.where(masks[way], decay, -jnp.inf)
            top = jnp.max(decay, axis=-1, keepdims=True)
            w = s_heads[h] * jnp.exp(decay - top)
            dens.append(jnp.sum(w, axis=-1, keepdims=True))
            nums.append(dot(w.astype(BF), mem_v))
            tops.append(top)
        own_parts.append((
            jnp.where(low, nums[0], nums[1]), jnp.where(low, dens[0], dens[1]), jnp.where(low, tops[0], tops[1]), cum
        ))
    ring_recv(2, 1)
    out_gate = jax.nn.sigmoid(memp[3].astype(F32))

    def chain(early, late):
        joined = jnp.maximum(late[10:11] + early[1], late[9:10])
        scale_e = jnp.exp(late[10:11] + early[1] - joined)
        scale_l = jnp.exp(late[9:10] - joined)
        return (scale_e * early[0] + scale_l * late, joined, early[2] + late[10:11])

    blank = (jnp.zeros((16, 128), F32), jnp.full((1, 128), FLOOR_LOG, F32), jnp.zeros((1, 128), F32))

    def packed(state):
        mat, level, total = state
        line = lax.broadcasted_iota(jnp.int32, (16, 128), 0)
        return jnp.where(line == 9, level, jnp.where(line == 10, total, mat))

    row_orders = (list(range(nr)), list(reversed(range(nr))))
    z_orders = (list(range(nz)), list(reversed(range(nz))))

    take_queries(0)

    attend(1, 2, (0, 1, 2), start=True)
    take_queries(1)
    take_queries(2)
    attend(2, 3, (0, 1, 2), start=True)
    ring_recv(3, 0)
    for copy in a_copies:
        copy.wait_recv()
    for way in range(2):
        state = blank
        for j in row_orders[way]:
            state = chain(state, agot[j, way])
        rtot[way] = packed(state)
    b_copies = []
    for d in range(1, nz):
        copy = rcopy(rtot.at[(z + d) // nz], pb.at[z], b_ss.at[d], b_rs.at[d], at_z(d))
        copy.start()
        b_copies.append(copy)
    pb[pl.ds(z, 1)] = jnp.zeros((1, 16, 128), F32)
    attend(3, 4, (0, 1, 2), start=True)
    ring_recv(3, 1)
    fill(3, -2)
    fill(4, 2)
    attend(0, half, (3, 4))
    attend(half, 2 * half, (3, 4))
    for copy in b_copies:
        copy.wait_recv()
    for way in range(2):
        state = blank
        for j in z_orders[way]:
            ok = (j < z) if way == 0 else (j > z)
            new = chain(state, pb[j])
            state = tuple(jnp.where(ok, a, b) for a, b in zip(new, state))
        for j in row_orders[way]:
            csend[j, way] = packed(state)
            state = chain(state, agot[j, way])
    c_copies = [
        rcopy(csend.at[lax.rem(me + d, nr)], cgot.at[me], c_ss.at[d], c_rs.at[d], at_row(d)) for d in range(1, nr)
    ]
    for copy in c_copies:
        copy.start()
    cgot[pl.ds(me, 1)] = csend[pl.ds(me, 1)]
    fill(5, -3)
    fill(6, 3)
    ring_recv(far, 0)
    ring_recv(far, 1)
    fill(7, far)
    attend(0, 2 * half, (5, 6, 7), last=True)
    po[pl.ds(me, 1)] = osend[pl.ds(nr - 2, 1)]
    for copy in c_copies:
        copy.wait_recv()
    hsum = jnp.zeros((BLOCK, 128), F32)
    bi = lax.broadcasted_iota(jnp.int32, (128, 128), 0) // 64
    bj = lax.broadcasted_iota(jnp.int32, (128, 128), 1) // 64
    ones_block = (bi == bj).astype(F32)
    low64 = lanes((64, 128)) < 64
    for way in range(2):
        fold = jnp.concatenate([cgot[j, way, pl.ds(0, 8), :] for j in range(nr)], axis=0)
        normal = cgot[0, way, pl.ds(8, 1), :]
        level = cgot[0, way, pl.ds(9, 1), :]
        full = jnp.concatenate([jnp.where(low64, fold, 0.0), jnp.where(low64, 0.0, fold)], axis=0)
        num, den, top, cum = own_parts[way]
        carried_log = cum + level
        joined = jnp.maximum(top, carried_log)
        own = jnp.exp(top - joined)
        carried = jnp.exp(carried_log - joined)
        both = jnp.concatenate([full, ones_block * normal], axis=0)
        in_q = sum(dot_nt(mem_q, a) for a in pieces(both, 2))
        num = num * own + carried * in_q[:, :128]
        den = den * own + carried * in_q[:, 128:]
        hsum = hsum + num / jnp.maximum(jnp.abs(den), jnp.exp(-joined))
    mean = sum(dot(a, ones_block.astype(BF)) for a in pieces(hsum * hsum, 2)) * (1.0 / 64)
    combined = hsum * lax.rsqrt(mean + EPSILON) * mng[pl.ds(y, 1), :]
    mem_rows = (combined * out_gate).astype(BF)
    for j in range(ny):
        fsend[0, j] = mem_rows[64 * j : 64 * j + 64]

    def to_owner(i):
        copies = [
            rcopy(fsend.at[i, lax.rem(y + d, ny)], fx.at[i, y], f_ss.at[i, d], f_rs.at[i, d], at_y(d))
            for d in range(1, ny)
        ]
        for copy in copies:
            copy.start()
        fx[i, pl.ds(y, 1)] = fsend[i, pl.ds(y, 1)]
        return copies

    fm_copies = to_owner(0)
    o_copies = [o_copy(i, t) for i in range(nx) for t in range(2) if i < nx - 1 or t == 1]
    for copy in o_copies:
        copy.wait_recv()
    heads = []
    low_s = lax.broadcasted_iota(jnp.int32, (128, 128), 0) < 64
    low1 = lane2[:128] < 64
    for h in range(2):
        lses = []
        for j in range(nx):
            st = po[2 * j + h, pl.ds(128, 16), :].astype(F32)
            lses.append((st[0:2] + st[2:4]) + st[4:6])
        joined = functools.reduce(jnp.maximum, lses)
        ws = [jnp.exp(v - joined) for v in lses]
        all_w = functools.reduce(jnp.add, ws)
        out_h = jnp.zeros((128, 128), F32)
        for j in range(nx):
            w = ws[j] / all_w
            wide = jnp.where(low_s, jnp.broadcast_to(w[0:1], (128, 128)), jnp.broadcast_to(w[1:2], (128, 128)))
            out_h = out_h + jnp.transpose(wide) * po[2 * j + h, pl.ds(0, 128), :].astype(F32)
        heads.append(out_h)
    att = jnp.concatenate(
        [jnp.where(low1, heads[0], pltpu.roll(heads[1], 64, 1)), jnp.where(low1, pltpu.roll(heads[0], 64, 1), heads[1])],
        axis=0,
    ).astype(BF)
    for j in range(ny):
        fsend[1, j] = att[64 * j : 64 * j + 64]
    fa_copies = to_owner(1)
    loads[10].wait()
    for copy in fm_copies:
        copy.wait_recv()
    for j in range(ny):
        lhs_m[:, 128 * j : 128 * j + 128] = fx[0, j]
    mixed = dot(lhs_m[...], wm[...])
    loads[11].wait()
    for copy in fa_copies:
        copy.wait_recv()
    for j in range(ny):
        lhs_a[:, 128 * j : 128 * j + 128] = fx[1, j]
    out[...] = mixed + dot(lhs_a[...], wa[...])

    for copies in (e_direct, e_onward, n_direct, n_onward, [p_copy], q_copies.values(), a_copies, b_copies, c_copies,
                   o_copies, fm_copies, fa_copies):
        for copy in copies:
            copy.wait_send()
    for copy in list(up.values()) + list(down.values()):
        copy.wait_send()


def body(nz, nx, ny, tokens, input_gain, memory_query, memory_key, memory_value, memory_outgate, memory_gates,
         gate_offset, memory_norm_gain, query_down, query_down_gain, latent_down, latent_gain, rotary_down,
         query_up, latent_up, query_gain, key_gain, memory_output, attention_output):
    args = (
        tokens, input_gain.reshape(1, D), memory_query, memory_key, memory_value, memory_outgate,
        jnp.transpose(memory_gates, (1, 2, 0)).reshape(32, D),
        jnp.transpose(gate_offset, (0, 2, 1)),
        memory_norm_gain.reshape(4, 128), query_down, query_down_gain.reshape(3, 128), latent_down,
        latent_gain.reshape(1, KVR), rotary_down.T,
        jnp.transpose(query_up, (1, 2, 0)).reshape(8 * (NOPE + ROPE), QR),
        latent_up.reshape(KVR * 8, 128), query_gain.reshape(1, 96), key_gain.reshape(1, 96),
        memory_output, attention_output,
    )
    nr = nx * 2
    in_hbm = {2, 3, 4, 5, 6, 9, 11, 13, 14, 15, 18, 19}
    vmem = pl.BlockSpec(memory_space=pltpu.VMEM)
    hbm = pl.BlockSpec(memory_space=pltpu.HBM)
    dma = pltpu.SemaphoreType.DMA
    keys = nz * 512
    far = nz // 2 + 1
    scratch = [
        pltpu.VMEM((D, 128), BF), pltpu.VMEM((D, 128), BF), pltpu.VMEM((D, 128), BF), pltpu.VMEM((D, 128), BF),
        pltpu.VMEM((32, D), BF), pltpu.VMEM((D, QR), BF), pltpu.VMEM((D, KVR), BF), pltpu.VMEM((32, D), BF),
        pltpu.VMEM((768, QR), BF), pltpu.VMEM((KVR * 8, 128), BF), pltpu.VMEM((512, D), BF), pltpu.VMEM((512, D), BF),
        pltpu.VMEM((256, D), BF), pltpu.VMEM((2, 128, QR), BF), pltpu.VMEM((KVR * 8, 128), F32),
        pltpu.VMEM((2, BLOCK, 128), F32),
        pltpu.VMEM((ny, ROWS, D), BF), pltpu.VMEM((ny, ROWS, 768), BF),
        pltpu.VMEM((nz, 2, BLOCK + ROWS, 128), BF), pltpu.VMEM((BLOCK + ROWS, 128), BF),
        pltpu.VMEM((2, BLOCK, 128), BF), pltpu.VMEM((nr, BLOCK, 128), BF),
        pltpu.VMEM((nr, 2, 16, 128), F32), pltpu.VMEM((nr, 2, 16, 128), F32), pltpu.VMEM((2, 16, 128), F32),
        pltpu.VMEM((nz, 16, 128), F32), pltpu.VMEM((nr, 2, 16, 128), F32), pltpu.VMEM((nr, 2, 16, 128), F32),
        pltpu.VMEM((4, BLOCK, 128), BF), pltpu.VMEM((BLOCK, 32), BF),
        pltpu.VMEM((nr, BLOCK, 256), BF), pltpu.VMEM((keys, 256), BF), pltpu.VMEM((keys, 128), BF),
        pltpu.VMEM((nr // 2, 2 * BLOCK, 128), F32), pltpu.VMEM((nr // 2, 2 * BLOCK, 128), F32),
        pltpu.VMEM((nr, 144, 128), BF), pltpu.VMEM((nr, 144, 128), BF),
        pltpu.VMEM((2, ny, ROWS, 128), BF), pltpu.VMEM((2, ny, ROWS, 128), BF),
        pltpu.VMEM((ROWS, 512), BF), pltpu.VMEM((ROWS, 512), BF),
        dma((12,)), dma((6,)), dma((6,)), dma((6,)), dma((6,)), dma, dma,
        dma((nr,)), dma((nr,)), dma((nr,)), dma((nr,)), dma((nz,)), dma((nz,)), dma((nr,)), dma((nr,)),
        dma((far, 2)), dma((far, 2)), dma((far, 2)), dma((far, 2)),
        dma((nr,)), dma((nr,)), dma((2, ny)), dma((2, ny)),
    ]
    mixed = pl.pallas_call(
        functools.partial(kernel, nz, nx, ny),
        out_shape=jax.ShapeDtypeStruct((ROWS, D), F32),
        in_specs=[hbm if i in in_hbm else vmem for i in range(len(args))],
        out_specs=vmem,
        scratch_shapes=scratch,
        compiler_params=pltpu.CompilerParams(
            collective_id=0, has_side_effects=True, vmem_limit_bytes=60 * 1024 * 1024
        ),
        name="mixer",
    )(*args)
    return mixed.astype(BF)


def solution(mesh):
    ny = mesh.shape["tp"]
    nz, nx = 8, 4
    split = Mesh(mesh.devices.reshape(nz, nx, 2, ny), ("sp_0", "sp_1", "sp_2", "tp"))
    rep = P()
    head = P(None, "tp")
    in_specs = (
        P(SP_TP, None), rep, head, head, head, head, rep, P(None, SP, "tp"),
        rep, rep, rep, rep, rep, rep, rep, rep, rep, rep, rep, rep,
    )
    return jax.shard_map(
        functools.partial(body, nz, nx, ny), mesh=split, in_specs=in_specs, out_specs=P(SP_TP, None), check_vma=False
    )
```

```python
import functools

import jax
import jax.numpy as jnp
from jax import lax
from jax.experimental import pallas as pl
from jax.experimental.pallas import tpu as pltpu
from jax.sharding import Mesh
from jax.sharding import PartitionSpec as P

D = 2048
NOPE = 64
ROPE = 32
ROWS = 64
BLOCK = 256
QR = 384
KVR = 256
SP = ("sp_0", "sp_1", "sp_2")
SP_TP = ("sp_0", "sp_1", "sp_2", "tp")
EPSILON = 1e-06
ROPE_BASE = 10000.0
FLOOR_LOG = -1e30
BF = jnp.bfloat16
F32 = jnp.float32
MESH = pl.DeviceIdType.MESH
HI = lax.Precision.HIGHEST
FREQUENCIES = [float(ROPE_BASE ** (-j / 16)) for j in range(16)]


def dot(a, b, precision=None):
    return lax.dot_general(a, b, (((1,), (0,)), ((), ())), precision=precision, preferred_element_type=F32)


def dot_nt(a, b, precision=None):
    return lax.dot_general(a, b, (((1,), (1,)), ((), ())), precision=precision, preferred_element_type=F32)


def pieces(v, n):
    found = []
    for _ in range(n):
        found.append(v.astype(BF))
        v = v - found[-1].astype(F32)
    return found


def lanes(shape):
    return lax.broadcasted_iota(jnp.int32, shape, len(shape) - 1)


def rcopy(src, dst, send_sem, recv_sem, device):
    return pltpu.make_async_remote_copy(
        src_ref=src, dst_ref=dst, send_sem=send_sem, recv_sem=recv_sem, device_id=device, device_id_type=MESH
    )


def rms(v):
    return v * lax.rsqrt(jnp.mean(v * v, axis=-1, keepdims=True) + EPSILON)


def kernel(
    nz, nx, ny,
    tok, gain, hmq, hmk, hmv, hmo, hgt, goff, mng, hqd, qdg, hld, lg, hrt, hqt, hlup,
    qgain, kgain, hwm, hwa,
    out,
    mq, mk, mv, mo, gt, qd, ld, rt, qt, lup, wm, wa,
    rt4, wqt, lupf, trig, normed, ebuf, qbuf, kvg, psend, qsend, qg, asend, agot, rtot, pb, csend, cgot,
    memp, memg, qop, kop, vt, acc_s, top_s, osend, po, fsend, fx, lhs_m, lhs_a,
    w_sem, n_ss, n_rs, e_ss, e_rs, l_ss, l_rs, p_ss, p_rs, q_ss, q_rs, a_ss, a_rs, b_ss, b_rs, c_ss, c_rs,
    u_ss, u_rs, d_ss, d_rs, o_ss, o_rs, f_ss, f_rs,
):
    z = lax.axis_index("sp_0")
    x = lax.axis_index("sp_1")
    c = lax.axis_index("sp_2")
    y = lax.axis_index("tp")
    nr = nx * 2
    me = x * 2 + c

    def at_y(d):
        return {"tp": lax.rem(y + d, ny)}

    def at_row(d):
        j = lax.rem(me + d, nr)
        return {"sp_1": j // 2, "sp_2": lax.rem(j, 2)}

    def at_z(d):
        return {"sp_0": lax.rem(z + d, nz)}

    pairs = ((hld, ld), (hrt, rt), (hqd, qd), (hlup, lup), (hqt, qt), (hmq, mq), (hmk, mk), (hmv, mv),
             (hgt, gt), (hmo, mo), (hwm, wm), (hwa, wa))
    loads = [pltpu.make_async_copy(a, b, w_sem.at[i]) for i, (a, b) in enumerate(pairs)]
    for load in loads:
        load.start()
    barrier = pltpu.get_barrier_semaphore()
    peers = [at_y(d) for d in range(1, ny)] + [at_row(d) for d in range(1, nr)] + [at_z(d) for d in range(1, nz)]
    for peer in peers:
        pl.semaphore_signal(barrier, inc=1, device_id=peer, device_id_type=MESH)

    xt = tok[...].astype(F32)
    normed_local = (rms(xt) * gain[...]).astype(BF)
    normed[pl.ds(y, 1)] = normed_local[None]

    segment = (z * nx + x) * 2 + c
    places = (segment * BLOCK + lax.broadcasted_iota(jnp.int32, (16, BLOCK), 1)).astype(F32)
    line = lax.broadcasted_iota(jnp.int32, (16, BLOCK), 0)
    frequency = jnp.zeros((16, BLOCK), F32)
    for j in range(16):
        frequency = jnp.where(line == j, FREQUENCIES[j], frequency)
    angles = places * frequency
    trig[0] = jnp.transpose(jnp.concatenate([jnp.cos(angles)] * 8, axis=0))
    trig[1] = jnp.transpose(jnp.concatenate([jnp.sin(angles)] * 8, axis=0))

    src = lax.broadcasted_iota(jnp.int32, (96, 128), 0)
    dst = lax.broadcasted_iota(jnp.int32, (96, 128), 1)
    rope_own, rope_swap = 64 + lax.rem(dst, 32), 64 + lax.rem(dst + 16, 32)
    q8 = jnp.broadcast_to(qgain[...], (8, 96))
    k8 = jnp.broadcast_to(kgain[...], (8, 96))
    scale = (NOPE + ROPE) ** (-0.5)
    q_own = dot(q8, (src == dst).astype(F32), HI)[0:1] * scale
    q_swap = dot(q8, (src == rope_swap).astype(F32), HI)[0:1] * scale
    k_own = dot(k8, (src == rope_own).astype(F32), HI)[0:1]
    k_swap = dot(k8, (src == rope_swap).astype(F32), HI)[0:1]
    k_plain = dot(k8, (src == dst).astype(F32), HI)[0:1]
    lane1 = lanes((1, 128))
    sign = jnp.where(lax.rem(lane1, 32) < 16, -1.0, 1.0)
    in_rope = jnp.logical_and(lane1 >= 64, lane1 < 96)

    loads[0].wait()
    la = (rms(dot(normed_local, ld[...])) * lg[...]).astype(BF)
    loads[1].wait()
    for i in range(4):
        rt4[pl.ds(32 * i, 32), :] = rt[...]
        rt4[pl.ds(128 + 32 * i, 16), :] = rt[pl.ds(16, 16), :]
        rt4[pl.ds(128 + 32 * i + 16, 16), :] = rt[pl.ds(0, 16), :]
    ro = dot_nt(normed_local, rt4[...])
    ra, rb = ro[:, :128], ro[:, 128:]
    rscale = lax.rsqrt(jnp.mean(ra * ra, axis=-1, keepdims=True) + EPSILON)
    lane = lanes((ROWS, 128))
    own_rows = pl.ds(pl.multiple_of(y * ROWS, ROWS), ROWS)
    rot = (ra * rscale) * (trig[0, own_rows, :] * k_own) + (rb * rscale) * (trig[1, own_rows, :] * (k_swap * sign))
    rot = jnp.where(lane // ROPE == y, rot, 0.0).astype(BF)
    ebuf[pl.ds(y, 1), :, 0:256] = la[None]
    ebuf[pl.ds(y, 1), :, 256:384] = rot[None]

    pl.semaphore_wait(barrier, len(peers))

    def spread_y(buf, ss, rs):
        lo, hi = pl.ds(0, ROWS // 2), pl.ds(ROWS // 2, ROWS // 2)
        below, above = lax.rem(y + ny - 1, ny), lax.rem(y + 1, ny)

        def one(i, slot, part, d):
            return rcopy(buf.at[slot, part], buf.at[slot, part], ss.at[i], rs.at[i], at_y(d))

        direct = [one(0, y, lo, 1), one(3, y, hi, ny - 1), one(1, y, hi, 1), one(4, y, lo, ny - 1)]
        onward = [one(2, below, lo, 1), one(5, above, hi, ny - 1)]
        return direct, onward

    e_direct, e_onward = spread_y(ebuf, e_ss, e_rs)
    l_direct, l_onward = spread_y(qbuf, l_ss, l_rs)
    n_direct, n_onward = spread_y(normed, n_ss, n_rs)
    for copy in e_direct:
        copy.start()
    loads[2].wait()
    qdg_row = jnp.concatenate([qdg[i : i + 1, :] for i in range(3)], axis=1)
    qbuf[pl.ds(y, 1)] = (rms(dot(normed_local, qd[...])) * qdg_row).astype(BF)[None]
    for copy in l_direct:
        copy.start()
    loads[3].wait()
    lupf[...] = lup[...].astype(F32)
    loads[4].wait()
    for h in range(2):
        base = 96 * (2 * y + h)
        wqt[h, pl.ds(0, 96), :] = qt[pl.ds(pl.multiple_of(base, 32), 96), :]
        wqt[h, pl.ds(96, 16), :] = qt[pl.ds(pl.multiple_of(base + 80, 16), 16), :]
        wqt[h, pl.ds(112, 16), :] = qt[pl.ds(pl.multiple_of(base + 64, 16), 16), :]
    for i in range(2):
        e_direct[i].wait_recv()
        e_onward[i].start()
    for i in range(2):
        l_direct[i].wait_recv()
        l_onward[i].start()
    for copy in n_direct:
        copy.start()
    e_direct[2].wait_recv()
    e_direct[3].wait_recv()
    for copy in e_onward:
        copy.wait_recv()

    lane2 = lanes((BLOCK, 128))
    low = lane2 < 64
    la_all = ebuf[:, :, 0:256].reshape(BLOCK, KVR)
    kv = []
    for h in range(2):
        w = lupf[pl.ds(2 * y + h, KVR, stride=8), :].astype(BF)
        t = dot(la_all, w)
        mp = jnp.sum(jnp.where(low, t * t, 0.0), axis=-1, keepdims=True) * (1.0 / NOPE)
        kv.append((t * jnp.where(low, lax.rsqrt(mp + EPSILON) * k_plain, 1.0)).astype(BF))
    rsum = (
        (ebuf[0, :, 256:384].astype(F32) + ebuf[1, :, 256:384].astype(F32))
        + (ebuf[2, :, 256:384].astype(F32) + ebuf[3, :, 256:384].astype(F32))
    ).astype(BF)
    first = c == 0
    kvg[pl.ds(z, 1), 0, pl.ds(0, BLOCK), :] = jnp.where(first, kv[0], kv[1])[None]
    kvg[pl.ds(z, 1), 0, pl.ds(BLOCK, ROWS), :] = rsum[None]
    psend[pl.ds(0, BLOCK), :] = jnp.where(first, kv[1], kv[0])
    psend[pl.ds(BLOCK, ROWS), :] = rsum
    p_copy = rcopy(psend, kvg.at[z, 1], p_ss, p_rs, {"sp_2": 1 - c})
    p_copy.start()

    up, down = {}, {}
    far = nz // 2

    def ring_send(s, r):
        if s < far or r == 0:
            k = lax.rem(z - (s - 1) + nz, nz)
            up[s, r] = rcopy(kvg.at[k, r], kvg.at[k, r], u_ss.at[s, r], u_rs.at[s, r], at_z(1))
            up[s, r].start()
        if s < far or r == 1:
            k = lax.rem(z + (s - 1), nz)
            down[s, r] = rcopy(kvg.at[k, r], kvg.at[k, r], d_ss.at[s, r], d_rs.at[s, r], at_z(nz - 1))
            down[s, r].start()

    def ring_recv(s, r):
        for way in (up, down):
            if (s, r) in way:
                way[s, r].wait_recv()
        if s < far:
            ring_send(s + 1, r)

    ring_send(1, 0)
    l_direct[2].wait_recv()
    l_direct[3].wait_recv()
    for copy in l_onward:
        copy.wait_recv()
    ql_all = qbuf[...].reshape(BLOCK, QR)
    cos_q = trig[0] * jnp.where(in_rope, q_own, 0.0) + jnp.where(lane1 < 64, q_own, 0.0)
    sin_q = trig[1] * jnp.where(in_rope, q_swap * sign, 0.0)
    for h in range(2):
        q = dot_nt(ql_all, wqt[h])
        q2 = q * q
        mp = jnp.sum(jnp.where(low, q2, 0.0), axis=-1, keepdims=True) * (1.0 / NOPE)
        mr = jnp.sum(jnp.where(lane2 >= 96, q2, 0.0), axis=-1, keepdims=True) * (1.0 / ROPE)
        qn = q * jnp.where(low, lax.rsqrt(mp + EPSILON), lax.rsqrt(mr + EPSILON))
        qsend[h] = (qn * cos_q + pltpu.roll(qn, 96, 1) * sin_q).astype(BF)
    def row_copy(src, dst, ss, rs, i, t):
        device = {"sp_1": lax.rem(x + i + 1, nx), "sp_2": lax.rem(c + t, 2)}
        return rcopy(src, dst, ss.at[2 * i + t], rs.at[2 * i + t], device)

    q_copies = {}
    for i in (nx - 1, 0, nx - 2, 1):
        for t in range(2):
            if i < nx - 1 or t == 1:
                q_copies[i, t] = row_copy(qsend.at[lax.rem(c + t, 2)], qg.at[me], q_ss, q_rs, i, t)
                q_copies[i, t].start()
    qg[pl.ds(me, 1)] = qsend[pl.ds(c, 1)]
    p_copy.wait_recv()
    ring_send(1, 1)

    def fill(slot, d):
        k = lax.rem(z + d + nz, nz)
        for r in range(2):
            base = slot * 512 + r * 256
            kvs = kvg[k, r, pl.ds(0, BLOCK), :]
            kop[pl.ds(base, BLOCK), 0:128] = kvs
            vt[pl.ds(base, BLOCK), :] = jnp.where(low, jnp.ones_like(kvs), kvs)
            rr = kvg[k, r, pl.ds(BLOCK, ROWS), :]
            for j in range(4):
                kop[pl.ds(base + 64 * j, ROWS), 128:256] = jnp.where(lane // ROPE == j, rr, jnp.zeros_like(rr))

    fill(0, 0)
    tile_r = lax.broadcasted_iota(jnp.int32, (128, 128), 0)
    tile_c = lax.broadcasted_iota(jnp.int32, (128, 128), 1)
    tile_m = (tile_r == 64 + lax.rem(tile_c, 32)).astype(BF)

    def take_queries(i):
        xx = lax.rem(x + i + 1, nx)
        back = (2 * nx - i - 2) % nx
        for t in range(2):
            if (back, t) in q_copies:
                q_copies[back, t].wait_recv()
        for t in range(2):
            slab = qg[2 * xx + t]
            qop[2 * xx + t, :, 0:128] = jnp.where(low, slab, jnp.zeros_like(slab))
            qop[2 * xx + t, :, 128:256] = dot(slab, tile_m).astype(BF)

    def o_copy(i, t):
        return row_copy(osend.at[2 * i + t], po.at[me], o_ss, o_rs, i, t)

    def attend(begin, end, slots, start=False, last=False):
        def block(n, carry):
            i = lax.rem(n + nx - 1, nx) if start else n
            xx = lax.rem(x + i + 1, nx)
            cores = [lax.rem(c + t, 2) for t in range(2)]
            qv = jnp.concatenate([qop[2 * xx + cores[t]] for t in range(2)], axis=0)
            if start:
                top = jnp.full((2 * BLOCK, 128), FLOOR_LOG, F32)
                acc = jnp.zeros((2 * BLOCK, 128), F32)
            else:
                top = top_s[i]
                acc = acc_s[i]
            score = dot_nt(qv, kop[pl.ds(slots[0] * 512, 512), :])
            for k in slots:
                after = dot_nt(qv, kop[pl.ds((k + 1) * 512, 512), :]) if k != slots[-1] else None
                new = jnp.maximum(top, jnp.max(score, axis=-1, keepdims=True))
                p = jnp.exp(score - jnp.concatenate([new] * 4, axis=1)).astype(BF)
                acc = acc * jnp.exp(top - new) + dot(p, vt[pl.ds(k * 512, 512), :])
                top = new
                score = after
            if not last:
                top_s[i] = top
                acc_s[i] = acc
                return carry
            den = acc[:, 0:1]
            lse = top + jnp.log(acc)
            share = acc / den
            low1 = lane2[:128] < 64
            for t in range(2):
                d = 2 * i + t
                a0, a1 = share[256 * t : 256 * t + 128], share[256 * t + 128 : 256 * t + 256]
                l0, l1 = lse[256 * t : 256 * t + 128], lse[256 * t + 128 : 256 * t + 256]
                osend[d, pl.ds(0, 128), :] = jnp.where(low1, pltpu.roll(a0, 64, 1), a1).astype(BF)
                rows_l = jnp.transpose(jnp.where(low1, l0, pltpu.roll(l1, 64, 1)))
                three = pieces(jnp.concatenate([rows_l[0:1], rows_l[64:65]], axis=0), 3)
                osend[d, pl.ds(128, 16), :] = jnp.concatenate(three + [jnp.zeros((10, 128), BF)], axis=0)

                @pl.when(jnp.logical_or(i < nx - 1, t == 1))
                def _():
                    o_copy(i, t).start()

            return carry

        lax.fori_loop(begin, end, block, 0)

    half = nr // 4
    for i in range(5, 9):
        loads[i].wait()
    loads[9].wait()

    def project(slot):
        part = normed[slot]
        at = pl.ds(pl.multiple_of(slot * ROWS, ROWS), ROWS)
        memp[0, at, :] = dot(part, mq[...]).astype(BF)
        memp[1, at, :] = (dot(part, mk[...]) * 0.125).astype(BF)
        memp[2, at, :] = dot(part, mv[...]).astype(BF)
        memp[3, at, :] = dot(part, mo[...]).astype(BF)
        memg[at, :] = dot_nt(part, gt[...]).astype(BF)

    for i in range(2):
        n_direct[i].wait_recv()
        n_onward[i].start()
    project(y)
    n_direct[2].wait_recv()
    n_direct[3].wait_recv()
    project(lax.rem(y + 1, ny))
    project(lax.rem(y + ny - 1, ny))
    ring_recv(1, 0)
    take_queries(nx - 1)
    ring_recv(1, 1)
    fill(1, -1)
    fill(2, 1)
    attend(0, 1, (0, 1, 2), start=True)
    for copy in n_onward:
        copy.wait_recv()
    project(lax.rem(y + 2, ny))
    mem_q, mem_k, mem_v = memp[0], memp[1], memp[2]
    row8 = lax.broadcasted_iota(jnp.int32, (8, 32), 0)
    col8 = lax.broadcasted_iota(jnp.int32, (8, 32), 1)
    pick = (col8 == (row8 // 2) * 8 + y * 2 + lax.rem(row8, 2)).astype(BF)
    pre = dot_nt(pick, memg[...]) + jnp.concatenate([goff[i] for i in range(4)], axis=0)
    low_t = lax.broadcasted_iota(jnp.int32, (128, BLOCK), 0) < 64

    def spread(r0, r1):
        wide = jnp.where(low_t, jnp.broadcast_to(r0, (128, BLOCK)), jnp.broadcast_to(r1, (128, BLOCK)))
        return jnp.transpose(wide)

    log_f = jnp.minimum(pre, 0.0) - jnp.log1p(jnp.exp(-jnp.abs(pre)))
    ti = lax.broadcasted_iota(jnp.int32, (BLOCK, BLOCK), 0)
    si = lax.broadcasted_iota(jnp.int32, (BLOCK, BLOCK), 1)
    masks = (si <= ti, si >= ti)
    log_3 = pieces(log_f, 3)
    zero = jnp.zeros_like(mem_q)
    v_f = mem_v.astype(F32)
    parts = []
    line16 = lax.broadcasted_iota(jnp.int32, (8, 128), 0)
    lane8 = lanes((8, 128))
    for way in range(2):
        ones = masks[1 - way].astype(BF)
        cums = (dot(log_3[0], ones) + dot(log_3[1], ones)) + dot(log_3[2], ones)
        cum = cums[4 * way + 2 : 4 * way + 4]
        g = pre[4 * way : 4 * way + 2] - cum
        last = BLOCK - 1 if way == 0 else 0
        total = cum[:, last : last + 1]
        growth = total + g
        level = jnp.max(growth, axis=-1, keepdims=True)
        inflow = jnp.exp(growth - level)
        wide = spread(inflow[0:1], inflow[1:2])
        vw = pieces(wide * v_f, 2)
        mat = sum(
            lax.dot_general(a, mem_k, (((0,), (0,)), ((), ())), preferred_element_type=F32) for a in vw
        )
        fold = jnp.where(lanes((64, 128)) < 64, mat[:64], mat[64:])
        inflow8 = jnp.concatenate([inflow, jnp.zeros((6, BLOCK), F32)], axis=0)
        sums = sum(dot(a, mem_k) for a in pieces(inflow8, 2))
        normal = jnp.where(lane1 < 64, sums[0:1], sums[1:2])

        def by_lane(v):
            return jnp.where(lane8 < 64, jnp.broadcast_to(v[0:1], (8, 128)), jnp.broadcast_to(v[1:2], (8, 128)))

        vecs = jnp.where(line16 == 0, normal, jnp.where(line16 == 1, by_lane(level), by_lane(total)))
        for j in range(nr):
            asend[j, way, pl.ds(0, 8), :] = fold[8 * j : 8 * j + 8]
            asend[j, way, pl.ds(8, 8), :] = vecs
        parts.append((cum, g))
    a_copies = [
        rcopy(asend.at[lax.rem(me + d, nr)], agot.at[me], a_ss.at[d], a_rs.at[d], at_row(d)) for d in range(1, nr)
    ]
    for copy in a_copies:
        copy.start()
    agot[pl.ds(me, 1)] = asend[pl.ds(me, 1)]
    ring_recv(2, 0)
    ring_recv(2, 1)

    def chain(early, late):
        joined = jnp.maximum(late[10:11] + early[1], late[9:10])
        scale_e = jnp.exp(late[10:11] + early[1] - joined)
        scale_l = jnp.exp(late[9:10] - joined)
        return (scale_e * early[0] + scale_l * late, joined, early[2] + late[10:11])

    blank = (jnp.zeros((16, 128), F32), jnp.full((1, 128), FLOOR_LOG, F32), jnp.zeros((1, 128), F32))

    def packed(state):
        mat, level, total = state
        line = lax.broadcasted_iota(jnp.int32, (16, 128), 0)
        return jnp.where(line == 9, level, jnp.where(line == 10, total, mat))

    row_orders = (list(range(nr)), list(reversed(range(nr))))
    z_orders = (list(range(nz)), list(reversed(range(nz))))

    take_queries(0)

    attend(1, 2, (0, 1, 2), start=True)
    take_queries(1)
    take_queries(2)
    attend(2, 3, (0, 1, 2), start=True)
    ring_recv(3, 0)
    for copy in a_copies:
        copy.wait_recv()
    for way in range(2):
        state = blank
        for j in row_orders[way]:
            state = chain(state, agot[j, way])
        rtot[way] = packed(state)
    b_copies = []
    for d in range(1, nz):
        copy = rcopy(rtot.at[(z + d) // nz], pb.at[z], b_ss.at[d], b_rs.at[d], at_z(d))
        copy.start()
        b_copies.append(copy)
    pb[pl.ds(z, 1)] = jnp.zeros((1, 16, 128), F32)
    attend(3, 4, (0, 1, 2), start=True)
    ring_recv(3, 1)
    fill(3, -2)
    fill(4, 2)
    attend(0, half, (3, 4))
    attend(half, 2 * half, (3, 4))
    for copy in b_copies:
        copy.wait_recv()
    for way in range(2):
        state = blank
        for j in z_orders[way]:
            ok = (j < z) if way == 0 else (j > z)
            new = chain(state, pb[j])
            state = tuple(jnp.where(ok, a, b) for a, b in zip(new, state))
        for j in row_orders[way]:
            csend[j, way] = packed(state)
            state = chain(state, agot[j, way])
    c_copies = [
        rcopy(csend.at[lax.rem(me + d, nr)], cgot.at[me], c_ss.at[d], c_rs.at[d], at_row(d)) for d in range(1, nr)
    ]
    for copy in c_copies:
        copy.start()
    cgot[pl.ds(me, 1)] = csend[pl.ds(me, 1)]
    fill(5, -3)
    fill(6, 3)
    ring_recv(far, 0)
    ring_recv(far, 1)
    fill(7, far)
    attend(0, 2 * half, (5, 6, 7), last=True)
    po[pl.ds(me, 1)] = osend[pl.ds(nr - 2, 1)]
    own_parts = []
    s_heads = (dot_nt(jnp.where(low, mem_q, zero), mem_k), dot_nt(jnp.where(low, zero, mem_q), mem_k))
    for way in range(2):
        cum, g_t = parts[way]
        cum = spread(cum[0:1], cum[1:2])
        nums, dens, tops = [], [], []
        for h in range(2):
            decay = cum[:, 64 * h : 64 * h + 1] + g_t[h : h + 1, :]
            decay = jnp.where(masks[way], decay, -jnp.inf)
            top = jnp.max(decay, axis=-1, keepdims=True)
            w = s_heads[h] * jnp.exp(decay - top)
            dens.append(jnp.sum(w, axis=-1, keepdims=True))
            nums.append(dot(w.astype(BF), mem_v))
            tops.append(top)
        own_parts.append((
            jnp.where(low, nums[0], nums[1]), jnp.where(low, dens[0], dens[1]), jnp.where(low, tops[0], tops[1]), cum
        ))
    out_gate = jax.nn.sigmoid(memp[3].astype(F32))
    for copy in c_copies:
        copy.wait_recv()
    hsum = jnp.zeros((BLOCK, 128), F32)
    bi = lax.broadcasted_iota(jnp.int32, (128, 128), 0) // 64
    bj = lax.broadcasted_iota(jnp.int32, (128, 128), 1) // 64
    ones_block = (bi == bj).astype(F32)
    low64 = lanes((64, 128)) < 64
    for way in range(2):
        fold = jnp.concatenate([cgot[j, way, pl.ds(0, 8), :] for j in range(nr)], axis=0)
        normal = cgot[0, way, pl.ds(8, 1), :]
        level = cgot[0, way, pl.ds(9, 1), :]
        full = jnp.concatenate([jnp.where(low64, fold, 0.0), jnp.where(low64, 0.0, fold)], axis=0)
        num, den, top, cum = own_parts[way]
        carried_log = cum + level
        joined = jnp.maximum(top, carried_log)
        own = jnp.exp(top - joined)
        carried = jnp.exp(carried_log - joined)
        both = jnp.concatenate([full, ones_block * normal], axis=0)
        in_q = sum(dot_nt(mem_q, a) for a in pieces(both, 2))
        num = num * own + carried * in_q[:, :128]
        den = den * own + carried * in_q[:, 128:]
        hsum = hsum + num / jnp.maximum(jnp.abs(den), jnp.exp(-joined))
    mean = sum(dot(a, ones_block.astype(BF)) for a in pieces(hsum * hsum, 2)) * (1.0 / 64)
    combined = hsum * lax.rsqrt(mean + EPSILON) * mng[pl.ds(y, 1), :]
    mem_rows = (combined * out_gate).astype(BF)
    for j in range(ny):
        fsend[0, j] = mem_rows[64 * j : 64 * j + 64]

    def to_owner(i):
        copies = [
            rcopy(fsend.at[i, lax.rem(y + d, ny)], fx.at[i, y], f_ss.at[i, d], f_rs.at[i, d], at_y(d))
            for d in range(1, ny)
        ]
        for copy in copies:
            copy.start()
        fx[i, pl.ds(y, 1)] = fsend[i, pl.ds(y, 1)]
        return copies

    fm_copies = to_owner(0)
    o_copies = [o_copy(i, t) for i in range(nx) for t in range(2) if i < nx - 1 or t == 1]
    for copy in o_copies:
        copy.wait_recv()
    heads = []
    low_s = lax.broadcasted_iota(jnp.int32, (128, 128), 0) < 64
    low1 = lane2[:128] < 64
    for h in range(2):
        lses = []
        for j in range(nx):
            st = po[2 * j + h, pl.ds(128, 16), :].astype(F32)
            lses.append((st[0:2] + st[2:4]) + st[4:6])
        joined = functools.reduce(jnp.maximum, lses)
        ws = [jnp.exp(v - joined) for v in lses]
        all_w = functools.reduce(jnp.add, ws)
        out_h = jnp.zeros((128, 128), F32)
        for j in range(nx):
            w = ws[j] / all_w
            wide = jnp.where(low_s, jnp.broadcast_to(w[0:1], (128, 128)), jnp.broadcast_to(w[1:2], (128, 128)))
            out_h = out_h + jnp.transpose(wide) * po[2 * j + h, pl.ds(0, 128), :].astype(F32)
        heads.append(out_h)
    att = jnp.concatenate(
        [jnp.where(low1, heads[0], pltpu.roll(heads[1], 64, 1)), jnp.where(low1, pltpu.roll(heads[0], 64, 1), heads[1])],
        axis=0,
    ).astype(BF)
    for j in range(ny):
        fsend[1, j] = att[64 * j : 64 * j + 64]
    fa_copies = to_owner(1)
    loads[10].wait()
    for copy in fm_copies:
        copy.wait_recv()
    for j in range(ny):
        lhs_m[:, 128 * j : 128 * j + 128] = fx[0, j]
    mixed = dot(lhs_m[...], wm[...])
    loads[11].wait()
    for copy in fa_copies:
        copy.wait_recv()
    for j in range(ny):
        lhs_a[:, 128 * j : 128 * j + 128] = fx[1, j]
    out[...] = (mixed + dot(lhs_a[...], wa[...])).astype(BF)

    for copies in (e_direct, e_onward, l_direct, l_onward, n_direct, n_onward, [p_copy], q_copies.values(), a_copies, b_copies, c_copies,
                   o_copies, fm_copies, fa_copies):
        for copy in copies:
            copy.wait_send()
    for copy in list(up.values()) + list(down.values()):
        copy.wait_send()


def body(nz, nx, ny, tokens, input_gain, memory_query, memory_key, memory_value, memory_outgate, memory_gates,
         gate_offset, memory_norm_gain, query_down, query_down_gain, latent_down, latent_gain, rotary_down,
         query_up, latent_up, query_gain, key_gain, memory_output, attention_output):
    args = (
        tokens, input_gain.reshape(1, D), memory_query, memory_key, memory_value, memory_outgate,
        jnp.transpose(memory_gates, (1, 2, 0)).reshape(32, D),
        jnp.transpose(gate_offset, (0, 2, 1)),
        memory_norm_gain.reshape(4, 128), query_down, query_down_gain.reshape(3, 128), latent_down,
        latent_gain.reshape(1, KVR), rotary_down.T,
        jnp.transpose(query_up, (1, 2, 0)).reshape(8 * (NOPE + ROPE), QR),
        latent_up.reshape(KVR * 8, 128), query_gain.reshape(1, 96), key_gain.reshape(1, 96),
        memory_output, attention_output,
    )
    nr = nx * 2
    in_hbm = {2, 3, 4, 5, 6, 9, 11, 13, 14, 15, 18, 19}
    vmem = pl.BlockSpec(memory_space=pltpu.VMEM)
    hbm = pl.BlockSpec(memory_space=pltpu.HBM)
    dma = pltpu.SemaphoreType.DMA
    keys = nz * 512
    far = nz // 2 + 1
    scratch = [
        pltpu.VMEM((D, 128), BF), pltpu.VMEM((D, 128), BF), pltpu.VMEM((D, 128), BF), pltpu.VMEM((D, 128), BF),
        pltpu.VMEM((32, D), BF), pltpu.VMEM((D, QR), BF), pltpu.VMEM((D, KVR), BF), pltpu.VMEM((32, D), BF),
        pltpu.VMEM((768, QR), BF), pltpu.VMEM((KVR * 8, 128), BF), pltpu.VMEM((512, D), BF), pltpu.VMEM((512, D), BF),
        pltpu.VMEM((256, D), BF), pltpu.VMEM((2, 128, QR), BF), pltpu.VMEM((KVR * 8, 128), F32),
        pltpu.VMEM((2, BLOCK, 128), F32),
        pltpu.VMEM((ny, ROWS, D), BF), pltpu.VMEM((ny, ROWS, 384), BF), pltpu.VMEM((ny, ROWS, QR), BF),
        pltpu.VMEM((nz, 2, BLOCK + ROWS, 128), BF), pltpu.VMEM((BLOCK + ROWS, 128), BF),
        pltpu.VMEM((2, BLOCK, 128), BF), pltpu.VMEM((nr, BLOCK, 128), BF),
        pltpu.VMEM((nr, 2, 16, 128), F32), pltpu.VMEM((nr, 2, 16, 128), F32), pltpu.VMEM((2, 16, 128), F32),
        pltpu.VMEM((nz, 16, 128), F32), pltpu.VMEM((nr, 2, 16, 128), F32), pltpu.VMEM((nr, 2, 16, 128), F32),
        pltpu.VMEM((4, BLOCK, 128), BF), pltpu.VMEM((BLOCK, 32), BF),
        pltpu.VMEM((nr, BLOCK, 256), BF), pltpu.VMEM((keys, 256), BF), pltpu.VMEM((keys, 128), BF),
        pltpu.VMEM((nr // 2, 2 * BLOCK, 128), F32), pltpu.VMEM((nr // 2, 2 * BLOCK, 128), F32),
        pltpu.VMEM((nr, 144, 128), BF), pltpu.VMEM((nr, 144, 128), BF),
        pltpu.VMEM((2, ny, ROWS, 128), BF), pltpu.VMEM((2, ny, ROWS, 128), BF),
        pltpu.VMEM((ROWS, 512), BF), pltpu.VMEM((ROWS, 512), BF),
        dma((12,)), dma((6,)), dma((6,)), dma((6,)), dma((6,)), dma((6,)), dma((6,)), dma, dma,
        dma((nr,)), dma((nr,)), dma((nr,)), dma((nr,)), dma((nz,)), dma((nz,)), dma((nr,)), dma((nr,)),
        dma((far, 2)), dma((far, 2)), dma((far, 2)), dma((far, 2)),
        dma((nr,)), dma((nr,)), dma((2, ny)), dma((2, ny)),
    ]
    return pl.pallas_call(
        functools.partial(kernel, nz, nx, ny),
        out_shape=jax.ShapeDtypeStruct((ROWS, D), BF),
        in_specs=[hbm if i in in_hbm else vmem for i in range(len(args))],
        out_specs=vmem,
        scratch_shapes=scratch,
        compiler_params=pltpu.CompilerParams(
            collective_id=0, has_side_effects=True, vmem_limit_bytes=60 * 1024 * 1024
        ),
        name="mixer",
    )(*args)


def solution(mesh):
    ny = mesh.shape["tp"]
    nz, nx = 8, 4
    split = Mesh(mesh.devices.reshape(nz, nx, 2, ny), ("sp_0", "sp_1", "sp_2", "tp"))
    rep = P()
    head = P(None, "tp")
    in_specs = (
        P(SP_TP, None), rep, head, head, head, head, rep, P(None, SP, "tp"),
        rep, rep, rep, rep, rep, rep, rep, rep, rep, rep, rep, rep,
    )
    return jax.shard_map(
        functools.partial(body, nz, nx, ny), mesh=split, in_specs=in_specs, out_specs=P(SP_TP, None), check_vma=False
    )
```

```python
import functools

import jax
import jax.numpy as jnp
from jax import lax
from jax.experimental import pallas as pl
from jax.experimental.pallas import tpu as pltpu
from jax.sharding import Mesh
from jax.sharding import PartitionSpec as P

D = 2048
NOPE = 64
ROPE = 32
ROWS = 64
BLOCK = 256
QR = 384
KVR = 256
SP = ("sp_0", "sp_1", "sp_2")
SP_TP = ("sp_0", "sp_1", "sp_2", "tp")
EPSILON = 1e-06
ROPE_BASE = 10000.0
FLOOR_LOG = -1e30
BF = jnp.bfloat16
F32 = jnp.float32
MESH = pl.DeviceIdType.MESH
HI = lax.Precision.HIGHEST
FREQUENCIES = [float(ROPE_BASE ** (-j / 16)) for j in range(16)]


def dot(a, b, precision=None):
    return lax.dot_general(a, b, (((1,), (0,)), ((), ())), precision=precision, preferred_element_type=F32)


def dot_nt(a, b, precision=None):
    return lax.dot_general(a, b, (((1,), (1,)), ((), ())), precision=precision, preferred_element_type=F32)


def pieces(v, n):
    found = []
    for _ in range(n):
        found.append(v.astype(BF))
        v = v - found[-1].astype(F32)
    return found


def lanes(shape):
    return lax.broadcasted_iota(jnp.int32, shape, len(shape) - 1)


def rcopy(src, dst, send_sem, recv_sem, device):
    return pltpu.make_async_remote_copy(
        src_ref=src, dst_ref=dst, send_sem=send_sem, recv_sem=recv_sem, device_id=device, device_id_type=MESH
    )


def rms(v):
    return v * lax.rsqrt(jnp.mean(v * v, axis=-1, keepdims=True) + EPSILON)


def kernel(
    nz, nx, ny,
    htok, hgain, hmq, hmk, hmv, hmo, hgt, hgoff, hmng, hqd, hqdg, hld, hlg, hrt, hqt, hlup,
    hqgain, hkgain, hwm, hwa,
    out,
    tok, gain, goff, mng, qdg, lg, qgain, kgain,
    mq, mk, mv, mo, gt, qd, ld, rt, qt, lup, wm, wa,
    rt4, wqt, lupf, trig, normed, ebuf, qbuf, kvg, psend, qsend, qg, asend, agot, rtot, pb, csend, cgot,
    memp, memg, qop, kop, vt, acc_s, top_s, osend, po, fsend, fx, lhs_m, lhs_a,
    w_sem, s_sem, n_ss, n_rs, e_ss, e_rs, l_ss, l_rs, p_ss, p_rs, q_ss, q_rs, a_ss, a_rs, b_ss, b_rs, c_ss, c_rs,
    u_ss, u_rs, d_ss, d_rs, o_ss, o_rs, f_ss, f_rs,
):
    z = lax.axis_index("sp_0")
    x = lax.axis_index("sp_1")
    c = lax.axis_index("sp_2")
    y = lax.axis_index("tp")
    nr = nx * 2
    me = x * 2 + c

    def at_y(d):
        return {"tp": lax.rem(y + d, ny)}

    def at_row(d):
        j = lax.rem(me + d, nr)
        return {"sp_1": j // 2, "sp_2": lax.rem(j, 2)}

    def at_z(d):
        return {"sp_0": lax.rem(z + d, nz)}

    pairs = ((hld, ld), (hrt, rt), (hqd, qd), (hlup, lup), (hqt, qt), (hmq, mq), (hmk, mk), (hmv, mv),
             (hgt, gt), (hmo, mo), (hwm, wm), (hwa, wa))
    smalls = ((htok, tok), (hgain, gain), (hqgain, qgain), (hkgain, kgain), (hlg, lg), (hqdg, qdg), (hgoff, goff),
              (hmng, mng))
    first_loads = [pltpu.make_async_copy(a, b, s_sem.at[i]) for i, (a, b) in enumerate(smalls)]
    loads = [pltpu.make_async_copy(a, b, w_sem.at[i]) for i, (a, b) in enumerate(pairs)]
    for load in first_loads + loads[:2]:
        load.start()
    barrier = pltpu.get_barrier_semaphore()
    peers = [at_y(d) for d in range(1, ny)] + [at_row(d) for d in range(1, nr)] + [at_z(d) for d in range(1, nz)]
    for peer in peers:
        pl.semaphore_signal(barrier, inc=1, device_id=peer, device_id_type=MESH)

    segment = (z * nx + x) * 2 + c
    places = (segment * BLOCK + lax.broadcasted_iota(jnp.int32, (16, BLOCK), 1)).astype(F32)
    line = lax.broadcasted_iota(jnp.int32, (16, BLOCK), 0)
    frequency = jnp.zeros((16, BLOCK), F32)
    for j in range(16):
        frequency = jnp.where(line == j, FREQUENCIES[j], frequency)
    angles = places * frequency
    trig[0] = jnp.transpose(jnp.concatenate([jnp.cos(angles)] * 8, axis=0))
    trig[1] = jnp.transpose(jnp.concatenate([jnp.sin(angles)] * 8, axis=0))

    for load in first_loads:
        load.wait()
    for load in loads[2:]:
        load.start()
    xt = tok[...].astype(F32)
    normed_local = (rms(xt) * gain[...]).astype(BF)
    normed[pl.ds(y, 1)] = normed_local[None]

    src = lax.broadcasted_iota(jnp.int32, (96, 128), 0)
    dst = lax.broadcasted_iota(jnp.int32, (96, 128), 1)
    rope_own, rope_swap = 64 + lax.rem(dst, 32), 64 + lax.rem(dst + 16, 32)
    q8 = jnp.broadcast_to(qgain[...], (8, 96))
    k8 = jnp.broadcast_to(kgain[...], (8, 96))
    scale = (NOPE + ROPE) ** (-0.5)
    q_own = dot(q8, (src == dst).astype(F32), HI)[0:1] * scale
    q_swap = dot(q8, (src == rope_swap).astype(F32), HI)[0:1] * scale
    k_own = dot(k8, (src == rope_own).astype(F32), HI)[0:1]
    k_swap = dot(k8, (src == rope_swap).astype(F32), HI)[0:1]
    k_plain = dot(k8, (src == dst).astype(F32), HI)[0:1]
    lane1 = lanes((1, 128))
    sign = jnp.where(lax.rem(lane1, 32) < 16, -1.0, 1.0)
    in_rope = jnp.logical_and(lane1 >= 64, lane1 < 96)

    loads[0].wait()
    la = (rms(dot(normed_local, ld[...])) * lg[...]).astype(BF)
    loads[1].wait()
    for i in range(4):
        rt4[pl.ds(32 * i, 32), :] = rt[...]
        rt4[pl.ds(128 + 32 * i, 16), :] = rt[pl.ds(16, 16), :]
        rt4[pl.ds(128 + 32 * i + 16, 16), :] = rt[pl.ds(0, 16), :]
    ro = dot_nt(normed_local, rt4[...])
    ra, rb = ro[:, :128], ro[:, 128:]
    rscale = lax.rsqrt(jnp.mean(ra * ra, axis=-1, keepdims=True) + EPSILON)
    lane = lanes((ROWS, 128))
    own_rows = pl.ds(pl.multiple_of(y * ROWS, ROWS), ROWS)
    rot = (ra * rscale) * (trig[0, own_rows, :] * k_own) + (rb * rscale) * (trig[1, own_rows, :] * (k_swap * sign))
    rot = jnp.where(lane // ROPE == y, rot, 0.0).astype(BF)
    ebuf[pl.ds(y, 1), :, 0:256] = la[None]
    ebuf[pl.ds(y, 1), :, 256:384] = rot[None]

    pl.semaphore_wait(barrier, len(peers))

    def spread_y(buf, ss, rs):
        lo, hi = pl.ds(0, ROWS // 2), pl.ds(ROWS // 2, ROWS // 2)
        below, above = lax.rem(y + ny - 1, ny), lax.rem(y + 1, ny)

        def one(i, slot, part, d):
            return rcopy(buf.at[slot, part], buf.at[slot, part], ss.at[i], rs.at[i], at_y(d))

        direct = [one(0, y, lo, 1), one(3, y, hi, ny - 1), one(1, y, hi, 1), one(4, y, lo, ny - 1)]
        onward = [one(2, below, lo, 1), one(5, above, hi, ny - 1)]
        return direct, onward

    e_direct, e_onward = spread_y(ebuf, e_ss, e_rs)
    l_direct, l_onward = spread_y(qbuf, l_ss, l_rs)
    n_direct, n_onward = spread_y(normed, n_ss, n_rs)
    for copy in e_direct:
        copy.start()
    loads[2].wait()
    qdg_row = jnp.concatenate([qdg[i : i + 1, :] for i in range(3)], axis=1)
    qbuf[pl.ds(y, 1)] = (rms(dot(normed_local, qd[...])) * qdg_row).astype(BF)[None]
    for copy in l_direct:
        copy.start()
    loads[3].wait()
    lupf[pl.ds(0, 8 * KVR), :] = lup[...].astype(F32)
    loads[4].wait()
    for h in range(2):
        base = 96 * (2 * y + h)
        wqt[h, pl.ds(0, 96), :] = qt[pl.ds(pl.multiple_of(base, 32), 96), :]
        wqt[h, pl.ds(96, 16), :] = qt[pl.ds(pl.multiple_of(base + 80, 16), 16), :]
        wqt[h, pl.ds(112, 16), :] = qt[pl.ds(pl.multiple_of(base + 64, 16), 16), :]
    for i in range(2):
        e_direct[i].wait_recv()
        e_onward[i].start()
    for i in range(2):
        l_direct[i].wait_recv()
        l_onward[i].start()
    for copy in n_direct:
        copy.start()
    e_direct[2].wait_recv()
    e_direct[3].wait_recv()
    for copy in e_onward:
        copy.wait_recv()

    lane2 = lanes((BLOCK, 128))
    low = lane2 < 64
    la_all = ebuf[:, :, 0:256].reshape(BLOCK, KVR)
    kv = []
    for h in range(2):
        w = lupf[pl.ds(2 * y + h, KVR, stride=8), :].astype(BF)
        t = dot(la_all, w)
        mp = jnp.sum(jnp.where(low, t * t, 0.0), axis=-1, keepdims=True) * (1.0 / NOPE)
        kv.append((t * jnp.where(low, lax.rsqrt(mp + EPSILON) * k_plain, 1.0)).astype(BF))
    rsum = (
        (ebuf[0, :, 256:384].astype(F32) + ebuf[1, :, 256:384].astype(F32))
        + (ebuf[2, :, 256:384].astype(F32) + ebuf[3, :, 256:384].astype(F32))
    ).astype(BF)
    first = c == 0
    kvg[pl.ds(z, 1), 0, pl.ds(0, BLOCK), :] = jnp.where(first, kv[0], kv[1])[None]
    kvg[pl.ds(z, 1), 0, pl.ds(BLOCK, ROWS), :] = rsum[None]
    psend[pl.ds(0, BLOCK), :] = jnp.where(first, kv[1], kv[0])
    psend[pl.ds(BLOCK, ROWS), :] = rsum
    p_copy = rcopy(psend, kvg.at[z, 1], p_ss, p_rs, {"sp_2": 1 - c})
    p_copy.start()

    up, down = {}, {}
    far = nz // 2

    def ring_send(s, r):
        if s < far or r == 0:
            k = lax.rem(z - (s - 1) + nz, nz)
            up[s, r] = rcopy(kvg.at[k, r], kvg.at[k, r], u_ss.at[s, r], u_rs.at[s, r], at_z(1))
            up[s, r].start()
        if s < far or r == 1:
            k = lax.rem(z + (s - 1), nz)
            down[s, r] = rcopy(kvg.at[k, r], kvg.at[k, r], d_ss.at[s, r], d_rs.at[s, r], at_z(nz - 1))
            down[s, r].start()

    def ring_recv(s, r):
        for way in (up, down):
            if (s, r) in way:
                way[s, r].wait_recv()
        if s < far:
            ring_send(s + 1, r)

    ring_send(1, 0)
    l_direct[2].wait_recv()
    l_direct[3].wait_recv()
    for copy in l_onward:
        copy.wait_recv()
    ql_all = qbuf[...].reshape(BLOCK, QR)
    cos_q = trig[0] * jnp.where(in_rope, q_own, 0.0) + jnp.where(lane1 < 64, q_own, 0.0)
    sin_q = trig[1] * jnp.where(in_rope, q_swap * sign, 0.0)
    for h in range(2):
        q = dot_nt(ql_all, wqt[h])
        q2 = q * q
        mp = jnp.sum(jnp.where(low, q2, 0.0), axis=-1, keepdims=True) * (1.0 / NOPE)
        mr = jnp.sum(jnp.where(lane2 >= 96, q2, 0.0), axis=-1, keepdims=True) * (1.0 / ROPE)
        qn = q * jnp.where(low, lax.rsqrt(mp + EPSILON), lax.rsqrt(mr + EPSILON))
        qsend[h] = (qn * cos_q + pltpu.roll(qn, 96, 1) * sin_q).astype(BF)
    def row_copy(src, dst, ss, rs, i, t):
        device = {"sp_1": lax.rem(x + i + 1, nx), "sp_2": lax.rem(c + t, 2)}
        return rcopy(src, dst, ss.at[2 * i + t], rs.at[2 * i + t], device)

    q_copies = {}
    for i in (nx - 1, 0, nx - 2, 1):
        for t in range(2):
            if i < nx - 1 or t == 1:
                q_copies[i, t] = row_copy(qsend.at[lax.rem(c + t, 2)], qg.at[me], q_ss, q_rs, i, t)
                q_copies[i, t].start()
    qg[pl.ds(me, 1)] = qsend[pl.ds(c, 1)]
    p_copy.wait_recv()
    ring_send(1, 1)

    def fill(slot, d):
        k = lax.rem(z + d + nz, nz)
        for r in range(2):
            base = slot * 512 + r * 256
            kvs = kvg[k, r, pl.ds(0, BLOCK), :]
            kop[pl.ds(base, BLOCK), 0:128] = kvs
            vt[pl.ds(base, BLOCK), :] = jnp.where(low, jnp.ones_like(kvs), kvs)
            rr = kvg[k, r, pl.ds(BLOCK, ROWS), :]
            for j in range(4):
                kop[pl.ds(base + 64 * j, ROWS), 128:256] = jnp.where(lane // ROPE == j, rr, jnp.zeros_like(rr))

    fill(0, 0)
    tile_r = lax.broadcasted_iota(jnp.int32, (128, 128), 0)
    tile_c = lax.broadcasted_iota(jnp.int32, (128, 128), 1)
    tile_m = (tile_r == 64 + lax.rem(tile_c, 32)).astype(BF)

    def take_queries(i):
        xx = lax.rem(x + i + 1, nx)
        back = (2 * nx - i - 2) % nx
        for t in range(2):
            if (back, t) in q_copies:
                q_copies[back, t].wait_recv()
        for t in range(2):
            slab = qg[2 * xx + t]
            qop[2 * xx + t, :, 0:128] = jnp.where(low, slab, jnp.zeros_like(slab))
            qop[2 * xx + t, :, 128:256] = dot(slab, tile_m).astype(BF)

    def o_copy(i, t):
        return row_copy(osend.at[2 * i + t], po.at[me], o_ss, o_rs, i, t)

    def attend(begin, end, slots, start=False, last=False):
        def block(n, carry):
            i = lax.rem(n + nx - 1, nx) if start else n
            xx = lax.rem(x + i + 1, nx)
            cores = [lax.rem(c + t, 2) for t in range(2)]
            qv = jnp.concatenate([qop[2 * xx + cores[t]] for t in range(2)], axis=0)
            if start:
                top = jnp.full((2 * BLOCK, 128), FLOOR_LOG, F32)
                acc = jnp.zeros((2 * BLOCK, 128), F32)
            else:
                top = top_s[i]
                acc = acc_s[i]
            score = dot_nt(qv, kop[pl.ds(slots[0] * 512, 512), :])
            for k in slots:
                after = dot_nt(qv, kop[pl.ds((k + 1) * 512, 512), :]) if k != slots[-1] else None
                new = jnp.maximum(top, jnp.max(score, axis=-1, keepdims=True))
                p = jnp.exp(score - jnp.concatenate([new] * 4, axis=1)).astype(BF)
                acc = acc * jnp.exp(top - new) + dot(p, vt[pl.ds(k * 512, 512), :])
                top = new
                score = after
            if not last:
                top_s[i] = top
                acc_s[i] = acc
                return carry
            den = acc[:, 0:1]
            lse = top + jnp.log(acc)
            share = acc / den
            low1 = lane2[:128] < 64
            for t in range(2):
                d = 2 * i + t
                a0, a1 = share[256 * t : 256 * t + 128], share[256 * t + 128 : 256 * t + 256]
                l0, l1 = lse[256 * t : 256 * t + 128], lse[256 * t + 128 : 256 * t + 256]
                osend[d, pl.ds(0, 128), :] = jnp.where(low1, pltpu.roll(a0, 64, 1), a1).astype(BF)
                rows_l = jnp.transpose(jnp.where(low1, l0, pltpu.roll(l1, 64, 1)))
                three = pieces(jnp.concatenate([rows_l[0:1], rows_l[64:65]], axis=0), 3)
                osend[d, pl.ds(128, 16), :] = jnp.concatenate(three + [jnp.zeros((10, 128), BF)], axis=0)

                @pl.when(jnp.logical_or(i < nx - 1, t == 1))
                def _():
                    o_copy(i, t).start()

            return carry

        lax.fori_loop(begin, end, block, 0)

    half = nr // 4
    for i in range(5, 9):
        loads[i].wait()
    loads[9].wait()

    def project(slot):
        part = normed[slot]
        at = pl.ds(pl.multiple_of(slot * ROWS, ROWS), ROWS)
        memp[0, at, :] = dot(part, mq[...]).astype(BF)
        memp[1, at, :] = (dot(part, mk[...]) * 0.125).astype(BF)
        memp[2, at, :] = dot(part, mv[...]).astype(BF)
        memp[3, at, :] = dot(part, mo[...]).astype(BF)
        memg[at, :] = dot_nt(part, gt[...]).astype(BF)

    for i in range(2):
        n_direct[i].wait_recv()
        n_onward[i].start()
    project(y)
    n_direct[2].wait_recv()
    n_direct[3].wait_recv()
    project(lax.rem(y + 1, ny))
    project(lax.rem(y + ny - 1, ny))
    ring_recv(1, 0)
    take_queries(nx - 1)
    ring_recv(1, 1)
    fill(1, -1)
    fill(2, 1)
    attend(0, 1, (0, 1, 2), start=True)
    for copy in n_onward:
        copy.wait_recv()
    project(lax.rem(y + 2, ny))
    mem_q, mem_k, mem_v = memp[0], memp[1], memp[2]
    row8 = lax.broadcasted_iota(jnp.int32, (8, 32), 0)
    col8 = lax.broadcasted_iota(jnp.int32, (8, 32), 1)
    pick = (col8 == (row8 // 2) * 8 + y * 2 + lax.rem(row8, 2)).astype(BF)
    pre = dot_nt(pick, memg[...]) + jnp.concatenate([goff[i] for i in range(4)], axis=0)
    low_t = lax.broadcasted_iota(jnp.int32, (128, BLOCK), 0) < 64

    def spread(r0, r1):
        wide = jnp.where(low_t, jnp.broadcast_to(r0, (128, BLOCK)), jnp.broadcast_to(r1, (128, BLOCK)))
        return jnp.transpose(wide)

    log_f = jnp.minimum(pre, 0.0) - jnp.log1p(jnp.exp(-jnp.abs(pre)))
    ti = lax.broadcasted_iota(jnp.int32, (BLOCK, BLOCK), 0)
    si = lax.broadcasted_iota(jnp.int32, (BLOCK, BLOCK), 1)
    masks = (si <= ti, si >= ti)
    log_3 = pieces(log_f, 3)
    zero = jnp.zeros_like(mem_q)
    v_f = mem_v.astype(F32)
    parts = []
    line16 = lax.broadcasted_iota(jnp.int32, (8, 128), 0)
    lane8 = lanes((8, 128))
    for way in range(2):
        ones = masks[1 - way].astype(BF)
        cums = (dot(log_3[0], ones) + dot(log_3[1], ones)) + dot(log_3[2], ones)
        cum = cums[4 * way + 2 : 4 * way + 4]
        g = pre[4 * way : 4 * way + 2] - cum
        last = BLOCK - 1 if way == 0 else 0
        total = cum[:, last : last + 1]
        growth = total + g
        level = jnp.max(growth, axis=-1, keepdims=True)
        inflow = jnp.exp(growth - level)
        wide = spread(inflow[0:1], inflow[1:2])
        vw = pieces(wide * v_f, 2)
        mat = sum(
            lax.dot_general(a, mem_k, (((0,), (0,)), ((), ())), preferred_element_type=F32) for a in vw
        )
        fold = jnp.where(lanes((64, 128)) < 64, mat[:64], mat[64:])
        inflow8 = jnp.concatenate([inflow, jnp.zeros((6, BLOCK), F32)], axis=0)
        sums = sum(dot(a, mem_k) for a in pieces(inflow8, 2))
        normal = jnp.where(lane1 < 64, sums[0:1], sums[1:2])

        def by_lane(v):
            return jnp.where(lane8 < 64, jnp.broadcast_to(v[0:1], (8, 128)), jnp.broadcast_to(v[1:2], (8, 128)))

        vecs = jnp.where(line16 == 0, normal, jnp.where(line16 == 1, by_lane(level), by_lane(total)))
        for j in range(nr):
            asend[j, way, pl.ds(0, 8), :] = fold[8 * j : 8 * j + 8]
            asend[j, way, pl.ds(8, 8), :] = vecs
        parts.append((cum, g))
    a_copies = [
        rcopy(asend.at[lax.rem(me + d, nr)], agot.at[me], a_ss.at[d], a_rs.at[d], at_row(d)) for d in range(1, nr)
    ]
    for copy in a_copies:
        copy.start()
    agot[pl.ds(me, 1)] = asend[pl.ds(me, 1)]
    ring_recv(2, 0)
    ring_recv(2, 1)

    def chain(early, late):
        joined = jnp.maximum(late[10:11] + early[1], late[9:10])
        scale_e = jnp.exp(late[10:11] + early[1] - joined)
        scale_l = jnp.exp(late[9:10] - joined)
        return (scale_e * early[0] + scale_l * late, joined, early[2] + late[10:11])

    blank = (jnp.zeros((16, 128), F32), jnp.full((1, 128), FLOOR_LOG, F32), jnp.zeros((1, 128), F32))

    def packed(state):
        mat, level, total = state
        line = lax.broadcasted_iota(jnp.int32, (16, 128), 0)
        return jnp.where(line == 9, level, jnp.where(line == 10, total, mat))

    row_orders = (list(range(nr)), list(reversed(range(nr))))
    z_orders = (list(range(nz)), list(reversed(range(nz))))

    take_queries(0)

    attend(1, 2, (0, 1, 2), start=True)
    take_queries(1)
    take_queries(2)
    attend(2, 3, (0, 1, 2), start=True)
    ring_recv(3, 0)
    for copy in a_copies:
        copy.wait_recv()
    for way in range(2):
        state = blank
        for j in row_orders[way]:
            state = chain(state, agot[j, way])
        rtot[way] = packed(state)
    b_copies = []
    for d in range(1, nz):
        copy = rcopy(rtot.at[(z + d) // nz], pb.at[z], b_ss.at[d], b_rs.at[d], at_z(d))
        copy.start()
        b_copies.append(copy)
    pb[pl.ds(z, 1)] = jnp.zeros((1, 16, 128), F32)
    attend(3, 4, (0, 1, 2), start=True)
    ring_recv(3, 1)
    fill(3, -2)
    fill(4, 2)
    attend(0, half, (3, 4))
    attend(half, 2 * half, (3, 4))
    for copy in b_copies:
        copy.wait_recv()
    for way in range(2):
        state = blank
        for j in z_orders[way]:
            ok = (j < z) if way == 0 else (j > z)
            new = chain(state, pb[j])
            state = tuple(jnp.where(ok, a, b) for a, b in zip(new, state))
        for j in row_orders[way]:
            csend[j, way] = packed(state)
            state = chain(state, agot[j, way])
    c_copies = [
        rcopy(csend.at[lax.rem(me + d, nr)], cgot.at[me], c_ss.at[d], c_rs.at[d], at_row(d)) for d in range(1, nr)
    ]
    for copy in c_copies:
        copy.start()
    cgot[pl.ds(me, 1)] = csend[pl.ds(me, 1)]
    fill(5, -3)
    fill(6, 3)
    ring_recv(far, 0)
    ring_recv(far, 1)
    fill(7, far)
    attend(0, 2 * half, (5, 6, 7), last=True)
    po[pl.ds(me, 1)] = osend[pl.ds(nr - 2, 1)]
    own_parts = []
    s_heads = (dot_nt(jnp.where(low, mem_q, zero), mem_k), dot_nt(jnp.where(low, zero, mem_q), mem_k))
    for way in range(2):
        cum, g_t = parts[way]
        cum = spread(cum[0:1], cum[1:2])
        nums, dens, tops = [], [], []
        for h in range(2):
            decay = cum[:, 64 * h : 64 * h + 1] + g_t[h : h + 1, :]
            decay = jnp.where(masks[way], decay, -jnp.inf)
            top = jnp.max(decay, axis=-1, keepdims=True)
            w = s_heads[h] * jnp.exp(decay - top)
            dens.append(jnp.sum(w, axis=-1, keepdims=True))
            nums.append(dot(w.astype(BF), mem_v))
            tops.append(top)
        own_parts.append((
            jnp.where(low, nums[0], nums[1]), jnp.where(low, dens[0], dens[1]), jnp.where(low, tops[0], tops[1]), cum
        ))
    out_gate = jax.nn.sigmoid(memp[3].astype(F32))
    for copy in c_copies:
        copy.wait_recv()
    hsum = jnp.zeros((BLOCK, 128), F32)
    bi = lax.broadcasted_iota(jnp.int32, (128, 128), 0) // 64
    bj = lax.broadcasted_iota(jnp.int32, (128, 128), 1) // 64
    ones_block = (bi == bj).astype(F32)
    low64 = lanes((64, 128)) < 64
    for way in range(2):
        fold = jnp.concatenate([cgot[j, way, pl.ds(0, 8), :] for j in range(nr)], axis=0)
        normal = cgot[0, way, pl.ds(8, 1), :]
        level = cgot[0, way, pl.ds(9, 1), :]
        full = jnp.concatenate([jnp.where(low64, fold, 0.0), jnp.where(low64, 0.0, fold)], axis=0)
        num, den, top, cum = own_parts[way]
        carried_log = cum + level
        joined = jnp.maximum(top, carried_log)
        own = jnp.exp(top - joined)
        carried = jnp.exp(carried_log - joined)
        both = jnp.concatenate([full, ones_block * normal], axis=0)
        in_q = sum(dot_nt(mem_q, a) for a in pieces(both, 2))
        num = num * own + carried * in_q[:, :128]
        den = den * own + carried * in_q[:, 128:]
        hsum = hsum + num / jnp.maximum(jnp.abs(den), jnp.exp(-joined))
    mean = sum(dot(a, ones_block.astype(BF)) for a in pieces(hsum * hsum, 2)) * (1.0 / 64)
    combined = hsum * lax.rsqrt(mean + EPSILON) * mng[pl.ds(y, 1), :]
    mem_rows = (combined * out_gate).astype(BF)
    for j in range(ny):
        fsend[0, j] = mem_rows[64 * j : 64 * j + 64]

    def to_owner(i):
        copies = [
            rcopy(fsend.at[i, lax.rem(y + d, ny)], fx.at[i, y], f_ss.at[i, d], f_rs.at[i, d], at_y(d))
            for d in range(1, ny)
        ]
        for copy in copies:
            copy.start()
        fx[i, pl.ds(y, 1)] = fsend[i, pl.ds(y, 1)]
        return copies

    fm_copies = to_owner(0)
    o_copies = [o_copy(i, t) for i in range(nx) for t in range(2) if i < nx - 1 or t == 1]
    for copy in o_copies:
        copy.wait_recv()
    heads = []
    low_s = lax.broadcasted_iota(jnp.int32, (128, 128), 0) < 64
    low1 = lane2[:128] < 64
    for h in range(2):
        lses = []
        for j in range(nx):
            st = po[2 * j + h, pl.ds(128, 16), :].astype(F32)
            lses.append((st[0:2] + st[2:4]) + st[4:6])
        joined = functools.reduce(jnp.maximum, lses)
        ws = [jnp.exp(v - joined) for v in lses]
        all_w = functools.reduce(jnp.add, ws)
        out_h = jnp.zeros((128, 128), F32)
        for j in range(nx):
            w = ws[j] / all_w
            wide = jnp.where(low_s, jnp.broadcast_to(w[0:1], (128, 128)), jnp.broadcast_to(w[1:2], (128, 128)))
            out_h = out_h + jnp.transpose(wide) * po[2 * j + h, pl.ds(0, 128), :].astype(F32)
        heads.append(out_h)
    att = jnp.concatenate(
        [jnp.where(low1, heads[0], pltpu.roll(heads[1], 64, 1)), jnp.where(low1, pltpu.roll(heads[0], 64, 1), heads[1])],
        axis=0,
    ).astype(BF)
    for j in range(ny):
        fsend[1, j] = att[64 * j : 64 * j + 64]
    fa_copies = to_owner(1)
    loads[10].wait()
    for copy in fm_copies:
        copy.wait_recv()
    for j in range(ny):
        lhs_m[:, 128 * j : 128 * j + 128] = fx[0, j]
    mixed = dot(lhs_m[...], wm[...])
    loads[11].wait()
    for copy in fa_copies:
        copy.wait_recv()
    for j in range(ny):
        lhs_a[:, 128 * j : 128 * j + 128] = fx[1, j]
    out[...] = (mixed + dot(lhs_a[...], wa[...])).astype(BF)

    for copies in (e_direct, e_onward, l_direct, l_onward, n_direct, n_onward, [p_copy], q_copies.values(), a_copies, b_copies, c_copies,
                   o_copies, fm_copies, fa_copies):
        for copy in copies:
            copy.wait_send()
    for copy in list(up.values()) + list(down.values()):
        copy.wait_send()


def body(nz, nx, ny, tokens, input_gain, memory_query, memory_key, memory_value, memory_outgate, memory_gates,
         gate_offset, memory_norm_gain, query_down, query_down_gain, latent_down, latent_gain, rotary_down,
         query_up, latent_up, query_gain, key_gain, memory_output, attention_output):
    args = (
        tokens, input_gain.reshape(1, D), memory_query, memory_key, memory_value, memory_outgate,
        jnp.transpose(memory_gates, (1, 2, 0)).reshape(32, D),
        jnp.transpose(gate_offset, (0, 2, 1)),
        memory_norm_gain.reshape(4, 128), query_down, query_down_gain.reshape(3, 128), latent_down,
        latent_gain.reshape(1, KVR), rotary_down.T,
        jnp.transpose(query_up, (1, 2, 0)).reshape(8 * (NOPE + ROPE), QR),
        latent_up.reshape(KVR * 8, 128), query_gain.reshape(1, 96), key_gain.reshape(1, 96),
        memory_output, attention_output,
    )
    nr = nx * 2
    vmem = pl.BlockSpec(memory_space=pltpu.VMEM)
    hbm = pl.BlockSpec(memory_space=pltpu.HBM)
    dma = pltpu.SemaphoreType.DMA
    keys = nz * 512
    far = nz // 2 + 1
    scratch = [
        pltpu.VMEM((ROWS, D), BF), pltpu.VMEM((1, D), F32), pltpu.VMEM((4, 2, BLOCK), F32), pltpu.VMEM((4, 128), F32),
        pltpu.VMEM((3, 128), F32), pltpu.VMEM((1, KVR), F32), pltpu.VMEM((1, 96), F32), pltpu.VMEM((1, 96), F32),
        pltpu.VMEM((D, 128), BF), pltpu.VMEM((D, 128), BF), pltpu.VMEM((D, 128), BF), pltpu.VMEM((D, 128), BF),
        pltpu.VMEM((32, D), BF), pltpu.VMEM((D, QR), BF), pltpu.VMEM((D, KVR), BF), pltpu.VMEM((32, D), BF),
        pltpu.VMEM((768, QR), BF), pltpu.VMEM((KVR * 8, 128), BF), pltpu.VMEM((512, D), BF), pltpu.VMEM((512, D), BF),
        pltpu.VMEM((256, D), BF), pltpu.VMEM((2, 128, QR), BF), pltpu.VMEM((KVR * 8 + 8, 128), F32),
        pltpu.VMEM((2, BLOCK, 128), F32),
        pltpu.VMEM((ny, ROWS, D), BF), pltpu.VMEM((ny, ROWS, 384), BF), pltpu.VMEM((ny, ROWS, QR), BF),
        pltpu.VMEM((nz, 2, BLOCK + ROWS, 128), BF), pltpu.VMEM((BLOCK + ROWS, 128), BF),
        pltpu.VMEM((2, BLOCK, 128), BF), pltpu.VMEM((nr, BLOCK, 128), BF),
        pltpu.VMEM((nr, 2, 16, 128), F32), pltpu.VMEM((nr, 2, 16, 128), F32), pltpu.VMEM((2, 16, 128), F32),
        pltpu.VMEM((nz, 16, 128), F32), pltpu.VMEM((nr, 2, 16, 128), F32), pltpu.VMEM((nr, 2, 16, 128), F32),
        pltpu.VMEM((4, BLOCK, 128), BF), pltpu.VMEM((BLOCK, 32), BF),
        pltpu.VMEM((nr, BLOCK, 256), BF), pltpu.VMEM((keys, 256), BF), pltpu.VMEM((keys, 128), BF),
        pltpu.VMEM((nr // 2, 2 * BLOCK, 128), F32), pltpu.VMEM((nr // 2, 2 * BLOCK, 128), F32),
        pltpu.VMEM((nr, 144, 128), BF), pltpu.VMEM((nr, 144, 128), BF),
        pltpu.VMEM((2, ny, ROWS, 128), BF), pltpu.VMEM((2, ny, ROWS, 128), BF),
        pltpu.VMEM((ROWS, 512), BF), pltpu.VMEM((ROWS, 512), BF),
        dma((12,)), dma((8,)), dma((6,)), dma((6,)), dma((6,)), dma((6,)), dma((6,)), dma((6,)), dma, dma,
        dma((nr,)), dma((nr,)), dma((nr,)), dma((nr,)), dma((nz,)), dma((nz,)), dma((nr,)), dma((nr,)),
        dma((far, 2)), dma((far, 2)), dma((far, 2)), dma((far, 2)),
        dma((nr,)), dma((nr,)), dma((2, ny)), dma((2, ny)),
    ]
    return pl.pallas_call(
        functools.partial(kernel, nz, nx, ny),
        out_shape=jax.ShapeDtypeStruct((ROWS, D), BF),
        in_specs=[hbm] * len(args),
        out_specs=vmem,
        scratch_shapes=scratch,
        compiler_params=pltpu.CompilerParams(
            collective_id=0, has_side_effects=True, vmem_limit_bytes=60 * 1024 * 1024
        ),
        name="mixer",
    )(*args)


def solution(mesh):
    ny = mesh.shape["tp"]
    nz, nx = 8, 4
    split = Mesh(mesh.devices.reshape(nz, nx, 2, ny), ("sp_0", "sp_1", "sp_2", "tp"))
    rep = P()
    head = P(None, "tp")
    in_specs = (
        P(SP_TP, None), rep, head, head, head, head, rep, P(None, SP, "tp"),
        rep, rep, rep, rep, rep, rep, rep, rep, rep, rep, rep, rep,
    )
    return jax.shard_map(
        functools.partial(body, nz, nx, ny), mesh=split, in_specs=in_specs, out_specs=P(SP_TP, None), check_vma=False
    )
```

```python
import functools

import jax
import jax.numpy as jnp
from jax import lax
from jax.experimental import pallas as pl
from jax.experimental.pallas import tpu as pltpu
from jax.sharding import Mesh
from jax.sharding import PartitionSpec as P

D = 2048
NOPE = 64
ROPE = 32
ROWS = 64
BLOCK = 256
QR = 384
KVR = 256
SP = ("sp_0", "sp_1", "sp_2")
SP_TP = ("sp_0", "sp_1", "sp_2", "tp")
EPSILON = 1e-06
ROPE_BASE = 10000.0
FLOOR_LOG = -1e30
BF = jnp.bfloat16
F32 = jnp.float32
MESH = pl.DeviceIdType.MESH
HI = lax.Precision.HIGHEST
FREQUENCIES = [float(ROPE_BASE ** (-j / 16)) for j in range(16)]


def dot(a, b, precision=None):
    return lax.dot_general(a, b, (((1,), (0,)), ((), ())), precision=precision, preferred_element_type=F32)


def dot_nt(a, b, precision=None):
    return lax.dot_general(a, b, (((1,), (1,)), ((), ())), precision=precision, preferred_element_type=F32)


def pieces(v, n):
    found = []
    for _ in range(n):
        found.append(v.astype(BF))
        v = v - found[-1].astype(F32)
    return found


def lanes(shape):
    return lax.broadcasted_iota(jnp.int32, shape, len(shape) - 1)


def rcopy(src, dst, send_sem, recv_sem, device):
    return pltpu.make_async_remote_copy(
        src_ref=src, dst_ref=dst, send_sem=send_sem, recv_sem=recv_sem, device_id=device, device_id_type=MESH
    )


def rms(v):
    return v * lax.rsqrt(jnp.mean(v * v, axis=-1, keepdims=True) + EPSILON)


def kernel(
    nz, nx, ny,
    htok, hgain, hmq, hmk, hmv, hmo, hgt, hgoff, hmng, hqd, hqdg, hld, hlg, hrt, hqt, hlup,
    hqgain, hkgain, hwm, hwa,
    out,
    tok, gain, goff, mng, qdg, lg, qgain, kgain,
    mq, mk, mv, mo, gt, qd, ld, rt, qt, lup, wm, wa,
    rt4, wqt, lupf, trig, normed, ebuf, qbuf, kvg, psend, qsend, qg, asend, agot, rtot, pb, csend, cgot,
    memp, memg, qop, kop, vt, acc_s, top_s, osend, po, fsend, fx, lhs_m, lhs_a,
    w_sem, s_sem, n_ss, n_rs, e_ss, e_rs, l_ss, l_rs, p_ss, p_rs, q_ss, q_rs, a_ss, a_rs, b_ss, b_rs, c_ss, c_rs,
    u_ss, u_rs, d_ss, d_rs, o_ss, o_rs, f_ss, f_rs,
):
    z = lax.axis_index("sp_0")
    x = lax.axis_index("sp_1")
    c = lax.axis_index("sp_2")
    y = lax.axis_index("tp")
    nr = nx * 2
    me = x * 2 + c

    def at_y(d):
        return {"tp": lax.rem(y + d, ny)}

    def at_row(d):
        j = lax.rem(me + d, nr)
        return {"sp_1": j // 2, "sp_2": lax.rem(j, 2)}

    def at_z(d):
        return {"sp_0": lax.rem(z + d, nz)}

    pairs = ((hld, ld), (hrt, rt), (hqd, qd), (hlup, lup), (hqt, qt), (hmq, mq), (hmk, mk), (hmv, mv),
             (hgt, gt), (hmo, mo), (hwm, wm), (hwa, wa))
    smalls = ((htok, tok), (hgain, gain), (hqgain, qgain), (hkgain, kgain), (hlg, lg), (hqdg, qdg), (hgoff, goff),
              (hmng, mng))
    first_loads = [pltpu.make_async_copy(a, b, s_sem.at[i]) for i, (a, b) in enumerate(smalls)]
    loads = [pltpu.make_async_copy(a, b, w_sem.at[i]) for i, (a, b) in enumerate(pairs)]
    for load in first_loads + loads[:2]:
        load.start()
    barrier = pltpu.get_barrier_semaphore()
    peers = [at_y(d) for d in range(1, ny)] + [at_row(d) for d in range(1, nr)] + [at_z(d) for d in range(1, nz)]
    for peer in peers:
        pl.semaphore_signal(barrier, inc=1, device_id=peer, device_id_type=MESH)

    segment = (z * nx + x) * 2 + c
    places = (segment * BLOCK + lax.broadcasted_iota(jnp.int32, (16, BLOCK), 1)).astype(F32)
    line = lax.broadcasted_iota(jnp.int32, (16, BLOCK), 0)
    frequency = jnp.zeros((16, BLOCK), F32)
    for j in range(16):
        frequency = jnp.where(line == j, FREQUENCIES[j], frequency)
    angles = places * frequency
    trig[0] = jnp.transpose(jnp.concatenate([jnp.cos(angles)] * 8, axis=0))
    trig[1] = jnp.transpose(jnp.concatenate([jnp.sin(angles)] * 8, axis=0))

    for load in first_loads:
        load.wait()
    for load in loads[2:]:
        load.start()
    xt = tok[...].astype(F32)
    normed_local = (rms(xt) * gain[...]).astype(BF)
    normed[pl.ds(y, 1)] = normed_local[None]

    src = lax.broadcasted_iota(jnp.int32, (96, 128), 0)
    dst = lax.broadcasted_iota(jnp.int32, (96, 128), 1)
    rope_own, rope_swap = 64 + lax.rem(dst, 32), 64 + lax.rem(dst + 16, 32)
    q8 = jnp.broadcast_to(qgain[...], (8, 96))
    k8 = jnp.broadcast_to(kgain[...], (8, 96))
    scale = (NOPE + ROPE) ** (-0.5)
    q_own = dot(q8, (src == dst).astype(F32), HI)[0:1] * scale
    q_swap = dot(q8, (src == rope_swap).astype(F32), HI)[0:1] * scale
    k_own = dot(k8, (src == rope_own).astype(F32), HI)[0:1]
    k_swap = dot(k8, (src == rope_swap).astype(F32), HI)[0:1]
    k_plain = dot(k8, (src == dst).astype(F32), HI)[0:1]
    lane1 = lanes((1, 128))
    sign = jnp.where(lax.rem(lane1, 32) < 16, -1.0, 1.0)
    in_rope = jnp.logical_and(lane1 >= 64, lane1 < 96)

    loads[0].wait()
    la = (rms(dot(normed_local, ld[...])) * lg[...]).astype(BF)
    loads[1].wait()
    for i in range(4):
        rt4[pl.ds(32 * i, 32), :] = rt[...]
        rt4[pl.ds(128 + 32 * i, 16), :] = rt[pl.ds(16, 16), :]
        rt4[pl.ds(128 + 32 * i + 16, 16), :] = rt[pl.ds(0, 16), :]
    ro = dot_nt(normed_local, rt4[...])
    ra, rb = ro[:, :128], ro[:, 128:]
    rscale = lax.rsqrt(jnp.mean(ra * ra, axis=-1, keepdims=True) + EPSILON)
    lane = lanes((ROWS, 128))
    own_rows = pl.ds(pl.multiple_of(y * ROWS, ROWS), ROWS)
    rot = (ra * rscale) * (trig[0, own_rows, :] * k_own) + (rb * rscale) * (trig[1, own_rows, :] * (k_swap * sign))
    rot = jnp.where(lane // ROPE == y, rot, 0.0).astype(BF)
    ebuf[pl.ds(y, 1), :, 0:256] = la[None]
    ebuf[pl.ds(y, 1), :, 256:384] = rot[None]

    pl.semaphore_wait(barrier, len(peers))

    def spread_y(buf, ss, rs):
        lo, hi = pl.ds(0, ROWS // 2), pl.ds(ROWS // 2, ROWS // 2)
        below, above = lax.rem(y + ny - 1, ny), lax.rem(y + 1, ny)

        def one(i, slot, part, d):
            return rcopy(buf.at[slot, part], buf.at[slot, part], ss.at[i], rs.at[i], at_y(d))

        direct = [one(0, y, lo, 1), one(3, y, hi, ny - 1), one(1, y, hi, 1), one(4, y, lo, ny - 1)]
        onward = [one(2, below, lo, 1), one(5, above, hi, ny - 1)]
        return direct, onward

    e_direct, e_onward = spread_y(ebuf, e_ss, e_rs)
    l_direct, l_onward = spread_y(qbuf, l_ss, l_rs)
    n_direct, n_onward = spread_y(normed, n_ss, n_rs)
    for copy in e_direct:
        copy.start()
    loads[2].wait()
    qdg_row = jnp.concatenate([qdg[i : i + 1, :] for i in range(3)], axis=1)
    qbuf[pl.ds(y, 1)] = (rms(dot(normed_local, qd[...])) * qdg_row).astype(BF)[None]
    for copy in l_direct:
        copy.start()
    loads[3].wait()
    lupf[pl.ds(0, 8 * KVR), :] = lup[...].astype(F32)
    loads[4].wait()
    for h in range(2):
        base = 96 * (2 * y + h)
        wqt[h, pl.ds(0, 96), :] = qt[pl.ds(pl.multiple_of(base, 32), 96), :]
        wqt[h, pl.ds(96, 16), :] = qt[pl.ds(pl.multiple_of(base + 80, 16), 16), :]
        wqt[h, pl.ds(112, 16), :] = qt[pl.ds(pl.multiple_of(base + 64, 16), 16), :]
    for i in range(2):
        e_direct[i].wait_recv()
        e_onward[i].start()
    for i in range(2):
        l_direct[i].wait_recv()
        l_onward[i].start()
    for copy in n_direct:
        copy.start()
    e_direct[2].wait_recv()
    e_direct[3].wait_recv()
    for copy in e_onward:
        copy.wait_recv()

    lane2 = lanes((BLOCK, 128))
    low = lane2 < 64
    la_all = ebuf[:, :, 0:256].reshape(BLOCK, KVR)
    kv = []
    for h in range(2):
        w = lupf[pl.ds(2 * y + h, KVR, stride=8), :].astype(BF)
        t = dot(la_all, w)
        mp = jnp.sum(jnp.where(low, t * t, 0.0), axis=-1, keepdims=True) * (1.0 / NOPE)
        kv.append((t * jnp.where(low, lax.rsqrt(mp + EPSILON) * k_plain, 1.0)).astype(BF))
    rsum = (
        (ebuf[0, :, 256:384].astype(F32) + ebuf[1, :, 256:384].astype(F32))
        + (ebuf[2, :, 256:384].astype(F32) + ebuf[3, :, 256:384].astype(F32))
    ).astype(BF)
    first = c == 0
    kvg[pl.ds(z, 1), 0, pl.ds(0, BLOCK), :] = jnp.where(first, kv[0], kv[1])[None]
    kvg[pl.ds(z, 1), 0, pl.ds(BLOCK, ROWS), :] = rsum[None]
    psend[pl.ds(0, BLOCK), :] = jnp.where(first, kv[1], kv[0])
    psend[pl.ds(BLOCK, ROWS), :] = rsum
    p_copy = rcopy(psend, kvg.at[z, 1], p_ss, p_rs, {"sp_2": 1 - c})
    p_copy.start()

    up, down = {}, {}
    far = nz // 2

    def ring_send(s, r):
        if s < far or r == 0:
            k = lax.rem(z - (s - 1) + nz, nz)
            up[s, r] = rcopy(kvg.at[k, r], kvg.at[k, r], u_ss.at[s, r], u_rs.at[s, r], at_z(1))
            up[s, r].start()
        if s < far or r == 1:
            k = lax.rem(z + (s - 1), nz)
            down[s, r] = rcopy(kvg.at[k, r], kvg.at[k, r], d_ss.at[s, r], d_rs.at[s, r], at_z(nz - 1))
            down[s, r].start()

    def ring_recv(s, r):
        for way in (up, down):
            if (s, r) in way:
                way[s, r].wait_recv()
        if s < far:
            ring_send(s + 1, r)

    ring_send(1, 0)
    l_direct[2].wait_recv()
    l_direct[3].wait_recv()
    for copy in l_onward:
        copy.wait_recv()
    ql_all = qbuf[...].reshape(BLOCK, QR)
    cos_q = trig[0] * jnp.where(in_rope, q_own, 0.0) + jnp.where(lane1 < 64, q_own, 0.0)
    sin_q = trig[1] * jnp.where(in_rope, q_swap * sign, 0.0)
    for h in range(2):
        q = dot_nt(ql_all, wqt[h])
        q2 = q * q
        mp = jnp.sum(jnp.where(low, q2, 0.0), axis=-1, keepdims=True) * (1.0 / NOPE)
        mr = jnp.sum(jnp.where(lane2 >= 96, q2, 0.0), axis=-1, keepdims=True) * (1.0 / ROPE)
        qn = q * jnp.where(low, lax.rsqrt(mp + EPSILON), lax.rsqrt(mr + EPSILON))
        qsend[h] = (qn * cos_q + pltpu.roll(qn, 96, 1) * sin_q).astype(BF)
    def row_copy(src, dst, ss, rs, i, t):
        device = {"sp_1": lax.rem(x + i + 1, nx), "sp_2": lax.rem(c + t, 2)}
        return rcopy(src, dst, ss.at[2 * i + t], rs.at[2 * i + t], device)

    q_copies = {}
    for i in (nx - 1, 0, nx - 2, 1):
        for t in range(2):
            if i < nx - 1 or t == 1:
                q_copies[i, t] = row_copy(qsend.at[lax.rem(c + t, 2)], qg.at[me], q_ss, q_rs, i, t)
                q_copies[i, t].start()
    qg[pl.ds(me, 1)] = qsend[pl.ds(c, 1)]
    p_copy.wait_recv()
    ring_send(1, 1)

    def fill(slot, d):
        k = lax.rem(z + d + nz, nz)
        for r in range(2):
            base = slot * 512 + r * 256
            kvs = kvg[k, r, pl.ds(0, BLOCK), :]
            kop[pl.ds(base, BLOCK), 0:128] = kvs
            vt[pl.ds(base, BLOCK), :] = jnp.where(low, jnp.ones_like(kvs), kvs)
            rr = kvg[k, r, pl.ds(BLOCK, ROWS), :]
            for j in range(4):
                kop[pl.ds(base + 64 * j, ROWS), 128:256] = jnp.where(lane // ROPE == j, rr, jnp.zeros_like(rr))

    fill(0, 0)
    tile_r = lax.broadcasted_iota(jnp.int32, (128, 128), 0)
    tile_c = lax.broadcasted_iota(jnp.int32, (128, 128), 1)
    tile_m = (tile_r == 64 + lax.rem(tile_c, 32)).astype(BF)

    def take_queries(i):
        xx = lax.rem(x + i + 1, nx)
        back = (2 * nx - i - 2) % nx
        for t in range(2):
            if (back, t) in q_copies:
                q_copies[back, t].wait_recv()
        for t in range(2):
            slab = qg[2 * xx + t]
            qop[2 * xx + t, :, 0:128] = jnp.where(low, slab, jnp.zeros_like(slab))
            qop[2 * xx + t, :, 128:256] = dot(slab, tile_m).astype(BF)

    def o_copy(i, t):
        return row_copy(osend.at[2 * i + t], po.at[me], o_ss, o_rs, i, t)

    def attend(begin, end, slots, start=False, last=False):
        def block(n, carry):
            i = lax.rem(n + nx - 1, nx) if start else n
            if last:
                i = jnp.where(n < 2, 1 - n, n)
            xx = lax.rem(x + i + 1, nx)
            cores = [lax.rem(c + t, 2) for t in range(2)]
            qv = jnp.concatenate([qop[2 * xx + cores[t]] for t in range(2)], axis=0)
            if start:
                top = jnp.full((2 * BLOCK, 128), FLOOR_LOG, F32)
                acc = jnp.zeros((2 * BLOCK, 128), F32)
            else:
                top = top_s[i]
                acc = acc_s[i]
            score = dot_nt(qv, kop[pl.ds(slots[0] * 512, 512), :])
            for k in slots:
                after = dot_nt(qv, kop[pl.ds((k + 1) * 512, 512), :]) if k != slots[-1] else None
                new = jnp.maximum(top, jnp.max(score, axis=-1, keepdims=True))
                p = jnp.exp(score - jnp.concatenate([new] * 4, axis=1)).astype(BF)
                acc = acc * jnp.exp(top - new) + dot(p, vt[pl.ds(k * 512, 512), :])
                top = new
                score = after
            if not last:
                top_s[i] = top
                acc_s[i] = acc
                return carry
            den = acc[:, 0:1]
            lse = top + jnp.log(acc)
            share = acc / den
            low1 = lane2[:128] < 64
            for t in range(2):
                d = 2 * i + t
                a0, a1 = share[256 * t : 256 * t + 128], share[256 * t + 128 : 256 * t + 256]
                l0, l1 = lse[256 * t : 256 * t + 128], lse[256 * t + 128 : 256 * t + 256]
                osend[d, pl.ds(0, 128), :] = jnp.where(low1, pltpu.roll(a0, 64, 1), a1).astype(BF)
                rows_l = jnp.transpose(jnp.where(low1, l0, pltpu.roll(l1, 64, 1)))
                three = pieces(jnp.concatenate([rows_l[0:1], rows_l[64:65]], axis=0), 3)
                osend[d, pl.ds(128, 16), :] = jnp.concatenate(three + [jnp.zeros((10, 128), BF)], axis=0)

                @pl.when(jnp.logical_or(i < nx - 1, t == 1))
                def _():
                    o_copy(i, t).start()

            return carry

        lax.fori_loop(begin, end, block, 0)

    half = nr // 4
    for i in range(5, 9):
        loads[i].wait()
    loads[9].wait()

    def project_gate(slot):
        at = pl.ds(pl.multiple_of(slot * ROWS, ROWS), ROWS)
        memp[3, at, :] = dot(normed[slot], mo[...]).astype(BF)

    def project(slot):
        part = normed[slot]
        at = pl.ds(pl.multiple_of(slot * ROWS, ROWS), ROWS)
        memp[0, at, :] = dot(part, mq[...]).astype(BF)
        memp[1, at, :] = (dot(part, mk[...]) * 0.125).astype(BF)
        memp[2, at, :] = dot(part, mv[...]).astype(BF)
        memg[at, :] = dot_nt(part, gt[...]).astype(BF)

    for i in range(2):
        n_direct[i].wait_recv()
        n_onward[i].start()
    project(y)
    project_gate(y)
    n_direct[2].wait_recv()
    n_direct[3].wait_recv()
    project(lax.rem(y + 1, ny))
    project(lax.rem(y + ny - 1, ny))
    project_gate(lax.rem(y + 1, ny))
    project_gate(lax.rem(y + ny - 1, ny))
    ring_recv(1, 0)
    take_queries(nx - 1)
    ring_recv(1, 1)
    fill(1, -1)
    fill(2, 1)
    attend(0, 1, (0, 1, 2), start=True)
    for copy in n_onward:
        copy.wait_recv()
    project(lax.rem(y + 2, ny))
    mem_q, mem_k, mem_v = memp[0], memp[1], memp[2]
    row8 = lax.broadcasted_iota(jnp.int32, (8, 32), 0)
    col8 = lax.broadcasted_iota(jnp.int32, (8, 32), 1)
    pick = (col8 == (row8 // 2) * 8 + y * 2 + lax.rem(row8, 2)).astype(BF)
    pre = dot_nt(pick, memg[...]) + jnp.concatenate([goff[i] for i in range(4)], axis=0)
    low_t = lax.broadcasted_iota(jnp.int32, (128, BLOCK), 0) < 64

    def spread(r0, r1):
        wide = jnp.where(low_t, jnp.broadcast_to(r0, (128, BLOCK)), jnp.broadcast_to(r1, (128, BLOCK)))
        return jnp.transpose(wide)

    log_f = jnp.minimum(pre, 0.0) - jnp.log1p(jnp.exp(-jnp.abs(pre)))
    ti = lax.broadcasted_iota(jnp.int32, (BLOCK, BLOCK), 0)
    si = lax.broadcasted_iota(jnp.int32, (BLOCK, BLOCK), 1)
    masks = (si <= ti, si >= ti)
    log_3 = pieces(log_f, 3)
    zero = jnp.zeros_like(mem_q)
    v_f = mem_v.astype(F32)
    parts = []
    line16 = lax.broadcasted_iota(jnp.int32, (8, 128), 0)
    lane8 = lanes((8, 128))
    for way in range(2):
        ones = masks[1 - way].astype(BF)
        cums = (dot(log_3[0], ones) + dot(log_3[1], ones)) + dot(log_3[2], ones)
        cum = cums[4 * way + 2 : 4 * way + 4]
        g = pre[4 * way : 4 * way + 2] - cum
        last = BLOCK - 1 if way == 0 else 0
        total = cum[:, last : last + 1]
        growth = total + g
        level = jnp.max(growth, axis=-1, keepdims=True)
        inflow = jnp.exp(growth - level)
        wide = spread(inflow[0:1], inflow[1:2])
        vw = pieces(wide * v_f, 2)
        mat = sum(
            lax.dot_general(a, mem_k, (((0,), (0,)), ((), ())), preferred_element_type=F32) for a in vw
        )
        fold = jnp.where(lanes((64, 128)) < 64, mat[:64], mat[64:])
        inflow8 = jnp.concatenate([inflow, jnp.zeros((6, BLOCK), F32)], axis=0)
        sums = sum(dot(a, mem_k) for a in pieces(inflow8, 2))
        normal = jnp.where(lane1 < 64, sums[0:1], sums[1:2])

        def by_lane(v):
            return jnp.where(lane8 < 64, jnp.broadcast_to(v[0:1], (8, 128)), jnp.broadcast_to(v[1:2], (8, 128)))

        vecs = jnp.where(line16 == 0, normal, jnp.where(line16 == 1, by_lane(level), by_lane(total)))
        for j in range(nr):
            asend[j, way, pl.ds(0, 8), :] = fold[8 * j : 8 * j + 8]
            asend[j, way, pl.ds(8, 8), :] = vecs
        parts.append((cum, g))
    a_copies = [
        rcopy(asend.at[lax.rem(me + d, nr)], agot.at[me], a_ss.at[d], a_rs.at[d], at_row(d)) for d in range(1, nr)
    ]
    for copy in a_copies:
        copy.start()
    agot[pl.ds(me, 1)] = asend[pl.ds(me, 1)]
    ring_recv(2, 0)
    ring_recv(2, 1)

    def chain(early, late):
        joined = jnp.maximum(late[10:11] + early[1], late[9:10])
        scale_e = jnp.exp(late[10:11] + early[1] - joined)
        scale_l = jnp.exp(late[9:10] - joined)
        return (scale_e * early[0] + scale_l * late, joined, early[2] + late[10:11])

    blank = (jnp.zeros((16, 128), F32), jnp.full((1, 128), FLOOR_LOG, F32), jnp.zeros((1, 128), F32))

    def packed(state):
        mat, level, total = state
        line = lax.broadcasted_iota(jnp.int32, (16, 128), 0)
        return jnp.where(line == 9, level, jnp.where(line == 10, total, mat))

    row_orders = (list(range(nr)), list(reversed(range(nr))))
    z_orders = (list(range(nz)), list(reversed(range(nz))))

    take_queries(0)

    attend(1, 2, (0, 1, 2), start=True)
    take_queries(1)
    take_queries(2)
    attend(2, 3, (0, 1, 2), start=True)
    ring_recv(3, 0)
    for copy in a_copies:
        copy.wait_recv()
    for way in range(2):
        state = blank
        for j in row_orders[way]:
            state = chain(state, agot[j, way])
        rtot[way] = packed(state)
    b_copies = []
    for d in range(1, nz):
        copy = rcopy(rtot.at[(z + d) // nz], pb.at[z], b_ss.at[d], b_rs.at[d], at_z(d))
        copy.start()
        b_copies.append(copy)
    pb[pl.ds(z, 1)] = jnp.zeros((1, 16, 128), F32)
    attend(3, 4, (0, 1, 2), start=True)
    ring_recv(3, 1)
    fill(3, -2)
    fill(4, 2)
    attend(0, half, (3, 4))
    attend(half, 2 * half, (3, 4))
    for copy in b_copies:
        copy.wait_recv()
    for way in range(2):
        state = blank
        for j in z_orders[way]:
            ok = (j < z) if way == 0 else (j > z)
            new = chain(state, pb[j])
            state = tuple(jnp.where(ok, a, b) for a, b in zip(new, state))
        for j in row_orders[way]:
            csend[j, way] = packed(state)
            state = chain(state, agot[j, way])
    c_copies = [
        rcopy(csend.at[lax.rem(me + d, nr)], cgot.at[me], c_ss.at[d], c_rs.at[d], at_row(d)) for d in range(1, nr)
    ]
    for copy in c_copies:
        copy.start()
    cgot[pl.ds(me, 1)] = csend[pl.ds(me, 1)]
    fill(5, -3)
    fill(6, 3)
    ring_recv(far, 0)
    ring_recv(far, 1)
    fill(7, far)
    attend(0, 2 * half, (5, 6, 7), last=True)
    po[pl.ds(me, 1)] = osend[pl.ds(nr - 2, 1)]
    own_parts = []
    s_heads = (dot_nt(jnp.where(low, mem_q, zero), mem_k), dot_nt(jnp.where(low, zero, mem_q), mem_k))
    for way in range(2):
        cum, g_t = parts[way]
        cum = spread(cum[0:1], cum[1:2])
        nums, dens, tops = [], [], []
        for h in range(2):
            decay = cum[:, 64 * h : 64 * h + 1] + g_t[h : h + 1, :]
            decay = jnp.where(masks[way], decay, -jnp.inf)
            top = jnp.max(decay, axis=-1, keepdims=True)
            w = s_heads[h] * jnp.exp(decay - top)
            dens.append(jnp.sum(w, axis=-1, keepdims=True))
            nums.append(dot(w.astype(BF), mem_v))
            tops.append(top)
        own_parts.append((
            jnp.where(low, nums[0], nums[1]), jnp.where(low, dens[0], dens[1]), jnp.where(low, tops[0], tops[1]), cum
        ))
    project_gate(lax.rem(y + 2, ny))
    out_gate = jax.nn.sigmoid(memp[3].astype(F32))
    for copy in c_copies:
        copy.wait_recv()
    hsum = jnp.zeros((BLOCK, 128), F32)
    bi = lax.broadcasted_iota(jnp.int32, (128, 128), 0) // 64
    bj = lax.broadcasted_iota(jnp.int32, (128, 128), 1) // 64
    ones_block = (bi == bj).astype(F32)
    low64 = lanes((64, 128)) < 64
    for way in range(2):
        fold = jnp.concatenate([cgot[j, way, pl.ds(0, 8), :] for j in range(nr)], axis=0)
        normal = cgot[0, way, pl.ds(8, 1), :]
        level = cgot[0, way, pl.ds(9, 1), :]
        full = jnp.concatenate([jnp.where(low64, fold, 0.0), jnp.where(low64, 0.0, fold)], axis=0)
        num, den, top, cum = own_parts[way]
        carried_log = cum + level
        joined = jnp.maximum(top, carried_log)
        own = jnp.exp(top - joined)
        carried = jnp.exp(carried_log - joined)
        both = jnp.concatenate([full, ones_block * normal], axis=0)
        in_q = sum(dot_nt(mem_q, a) for a in pieces(both, 2))
        num = num * own + carried * in_q[:, :128]
        den = den * own + carried * in_q[:, 128:]
        hsum = hsum + num / jnp.maximum(jnp.abs(den), jnp.exp(-joined))
    mean = sum(dot(a, ones_block.astype(BF)) for a in pieces(hsum * hsum, 2)) * (1.0 / 64)
    combined = hsum * lax.rsqrt(mean + EPSILON) * mng[pl.ds(y, 1), :]
    mem_rows = (combined * out_gate).astype(BF)
    for j in range(ny):
        fsend[0, j] = mem_rows[64 * j : 64 * j + 64]

    def to_owner(i):
        copies = [
            rcopy(fsend.at[i, lax.rem(y + d, ny)], fx.at[i, y], f_ss.at[i, d], f_rs.at[i, d], at_y(d))
            for d in range(1, ny)
        ]
        for copy in copies:
            copy.start()
        fx[i, pl.ds(y, 1)] = fsend[i, pl.ds(y, 1)]
        return copies

    fm_copies = to_owner(0)
    o_copies = [o_copy(i, t) for i in range(nx) for t in range(2) if i < nx - 1 or t == 1]
    for copy in o_copies:
        copy.wait_recv()
    heads = []
    low_s = lax.broadcasted_iota(jnp.int32, (128, 128), 0) < 64
    low1 = lane2[:128] < 64
    for h in range(2):
        lses = []
        for j in range(nx):
            st = po[2 * j + h, pl.ds(128, 16), :].astype(F32)
            lses.append((st[0:2] + st[2:4]) + st[4:6])
        joined = functools.reduce(jnp.maximum, lses)
        ws = [jnp.exp(v - joined) for v in lses]
        all_w = functools.reduce(jnp.add, ws)
        out_h = jnp.zeros((128, 128), F32)
        for j in range(nx):
            w = ws[j] / all_w
            wide = jnp.where(low_s, jnp.broadcast_to(w[0:1], (128, 128)), jnp.broadcast_to(w[1:2], (128, 128)))
            out_h = out_h + jnp.transpose(wide) * po[2 * j + h, pl.ds(0, 128), :].astype(F32)
        heads.append(out_h)
    att = jnp.concatenate(
        [jnp.where(low1, heads[0], pltpu.roll(heads[1], 64, 1)), jnp.where(low1, pltpu.roll(heads[0], 64, 1), heads[1])],
        axis=0,
    ).astype(BF)
    for j in range(ny):
        fsend[1, j] = att[64 * j : 64 * j + 64]
    fa_copies = to_owner(1)
    loads[10].wait()
    for copy in fm_copies:
        copy.wait_recv()
    for j in range(ny):
        lhs_m[:, 128 * j : 128 * j + 128] = fx[0, j]
    mixed = dot(lhs_m[...], wm[...])
    loads[11].wait()
    for copy in fa_copies:
        copy.wait_recv()
    for j in range(ny):
        lhs_a[:, 128 * j : 128 * j + 128] = fx[1, j]
    out[...] = (mixed + dot(lhs_a[...], wa[...])).astype(BF)

    for copies in (e_direct, e_onward, l_direct, l_onward, n_direct, n_onward, [p_copy], q_copies.values(), a_copies, b_copies, c_copies,
                   o_copies, fm_copies, fa_copies):
        for copy in copies:
            copy.wait_send()
    for copy in list(up.values()) + list(down.values()):
        copy.wait_send()


def body(nz, nx, ny, tokens, input_gain, memory_query, memory_key, memory_value, memory_outgate, memory_gates,
         gate_offset, memory_norm_gain, query_down, query_down_gain, latent_down, latent_gain, rotary_down,
         query_up, latent_up, query_gain, key_gain, memory_output, attention_output):
    args = (
        tokens, input_gain.reshape(1, D), memory_query, memory_key, memory_value, memory_outgate,
        jnp.transpose(memory_gates, (1, 2, 0)).reshape(32, D),
        jnp.transpose(gate_offset, (0, 2, 1)),
        memory_norm_gain.reshape(4, 128), query_down, query_down_gain.reshape(3, 128), latent_down,
        latent_gain.reshape(1, KVR), rotary_down.T,
        jnp.transpose(query_up, (1, 2, 0)).reshape(8 * (NOPE + ROPE), QR),
        latent_up.reshape(KVR * 8, 128), query_gain.reshape(1, 96), key_gain.reshape(1, 96),
        memory_output, attention_output,
    )
    nr = nx * 2
    vmem = pl.BlockSpec(memory_space=pltpu.VMEM)
    hbm = pl.BlockSpec(memory_space=pltpu.HBM)
    dma = pltpu.SemaphoreType.DMA
    keys = nz * 512
    far = nz // 2 + 1
    scratch = [
        pltpu.VMEM((ROWS, D), BF), pltpu.VMEM((1, D), F32), pltpu.VMEM((4, 2, BLOCK), F32), pltpu.VMEM((4, 128), F32),
        pltpu.VMEM((3, 128), F32), pltpu.VMEM((1, KVR), F32), pltpu.VMEM((1, 96), F32), pltpu.VMEM((1, 96), F32),
        pltpu.VMEM((D, 128), BF), pltpu.VMEM((D, 128), BF), pltpu.VMEM((D, 128), BF), pltpu.VMEM((D, 128), BF),
        pltpu.VMEM((32, D), BF), pltpu.VMEM((D, QR), BF), pltpu.VMEM((D, KVR), BF), pltpu.VMEM((32, D), BF),
        pltpu.VMEM((768, QR), BF), pltpu.VMEM((KVR * 8, 128), BF), pltpu.VMEM((512, D), BF), pltpu.VMEM((512, D), BF),
        pltpu.VMEM((256, D), BF), pltpu.VMEM((2, 128, QR), BF), pltpu.VMEM((KVR * 8 + 8, 128), F32),
        pltpu.VMEM((2, BLOCK, 128), F32),
        pltpu.VMEM((ny, ROWS, D), BF), pltpu.VMEM((ny, ROWS, 384), BF), pltpu.VMEM((ny, ROWS, QR), BF),
        pltpu.VMEM((nz, 2, BLOCK + ROWS, 128), BF), pltpu.VMEM((BLOCK + ROWS, 128), BF),
        pltpu.VMEM((2, BLOCK, 128), BF), pltpu.VMEM((nr, BLOCK, 128), BF),
        pltpu.VMEM((nr, 2, 16, 128), F32), pltpu.VMEM((nr, 2, 16, 128), F32), pltpu.VMEM((2, 16, 128), F32),
        pltpu.VMEM((nz, 16, 128), F32), pltpu.VMEM((nr, 2, 16, 128), F32), pltpu.VMEM((nr, 2, 16, 128), F32),
        pltpu.VMEM((4, BLOCK, 128), BF), pltpu.VMEM((BLOCK, 32), BF),
        pltpu.VMEM((nr, BLOCK, 256), BF), pltpu.VMEM((keys, 256), BF), pltpu.VMEM((keys, 128), BF),
        pltpu.VMEM((nr // 2, 2 * BLOCK, 128), F32), pltpu.VMEM((nr // 2, 2 * BLOCK, 128), F32),
        pltpu.VMEM((nr, 144, 128), BF), pltpu.VMEM((nr, 144, 128), BF),
        pltpu.VMEM((2, ny, ROWS, 128), BF), pltpu.VMEM((2, ny, ROWS, 128), BF),
        pltpu.VMEM((ROWS, 512), BF), pltpu.VMEM((ROWS, 512), BF),
        dma((12,)), dma((8,)), dma((6,)), dma((6,)), dma((6,)), dma((6,)), dma((6,)), dma((6,)), dma, dma,
        dma((nr,)), dma((nr,)), dma((nr,)), dma((nr,)), dma((nz,)), dma((nz,)), dma((nr,)), dma((nr,)),
        dma((far, 2)), dma((far, 2)), dma((far, 2)), dma((far, 2)),
        dma((nr,)), dma((nr,)), dma((2, ny)), dma((2, ny)),
    ]
    return pl.pallas_call(
        functools.partial(kernel, nz, nx, ny),
        out_shape=jax.ShapeDtypeStruct((ROWS, D), BF),
        in_specs=[hbm] * len(args),
        out_specs=vmem,
        scratch_shapes=scratch,
        compiler_params=pltpu.CompilerParams(
            collective_id=0, has_side_effects=True, vmem_limit_bytes=60 * 1024 * 1024
        ),
        name="mixer",
    )(*args)


def solution(mesh):
    ny = mesh.shape["tp"]
    nz, nx = 8, 4
    split = Mesh(mesh.devices.reshape(nz, nx, 2, ny), ("sp_0", "sp_1", "sp_2", "tp"))
    rep = P()
    head = P(None, "tp")
    in_specs = (
        P(SP_TP, None), rep, head, head, head, head, rep, P(None, SP, "tp"),
        rep, rep, rep, rep, rep, rep, rep, rep, rep, rep, rep, rep,
    )
    return jax.shard_map(
        functools.partial(body, nz, nx, ny), mesh=split, in_specs=in_specs, out_specs=P(SP_TP, None), check_vma=False
    )
```
